512 devices in a mesh: fs: 64 (over z, y), rep: 4 (over x), tp: 2 (over core).
Axes of the slice: x: 4, y: 8, z: 8, core: 2. Of those that a mesh axis runs over, the one named last changes fastest.
Arguments:
- attention_input: bfloat16 [196608, 2048], P(('fs', 'rep')), may hold values from -6 to 6
- query_cotangent: bfloat16 [196608, 1024], P(('fs', 'rep'), 'tp'), may hold values from -15 to 15
- gate_cotangent: float32 [16, 196608], P('tp', ('fs', 'rep')), may hold values from -6 to 6
- gate_totals: float32 [16, 196608], P('tp', ('fs', 'rep')), may hold values from -2304 to 0, as said below
- projector: bfloat16 [2048, 256], P('fs'), may hold values from -1 to 1
- query_master: float32 [2048, 1024], P('fs', 'tp'), may hold values from -0.125 to 0.125
- lowrank_mean: float32 [256, 1024], P('rep', 'tp'), may hold values from -32 to 32
- lowrank_square: float32 [256, 1024], P('rep', 'tp'), may hold values from 0.05 to 2
- gating_mean: float32 [16, 2048], P('tp'), may hold values from -1.8 to 1.8
- gating_square: float32 [16, 2048], P('tp'), may hold values from 0.01 to 1
Outputs:
- query_update: float32 [2048, 1024], P('fs', 'tp')
- query_renewed: float32 [2048, 1024], P('fs', 'tp')
- query_copy: bfloat16 [2048, 1024], P('fs', 'tp')
- mean_after: float32 [256, 1024], P('rep', 'tp')
- square_after: float32 [256, 1024], P('rep', 'tp')
- gating_update: float32 [16, 2048], P('tp')
- gating_average: float32 [16, 2048], P('tp')
- gating_energy: float32 [16, 2048], P('tp')
The draws below stay inside these ranges and needn't reach their ends.
Inputs may be any that keep to these rules, and one draw needn't show every extreme that they name: `gate_totals`: within each sequence of 768 positions, a running sum of negative log gates, so successive differences are negative.
All inputs are finite; a program needn't handle non-finite values.
Results may differ from the reference program's by a relative error of at most 0.0044.
The reference program's roundings to bfloat16 on the way (of `blended` and `gate_signal`) count: a program that leaves them out, or rounds other values in their place, can miss the bound.
Values may be sent and summed in bfloat16 or wider, within the bound.
No kernel may reach another device: no remote copies, remote signals or barrier semaphores. Data moves between devices by JAX's collectives and lax.ppermute only.
A program may use at most 64 MiB of HBM per device.

```python
import math
import jax
import jax.numpy as jnp
from jax import lax

D = 2048
HEADS = 16
A = 1024
RANK = 256
DEVICE_TOKENS = 768
TOTAL_TOKENS = 196608


def rising(key, count, spread):
    jitter = jax.random.uniform(key, (count,), jnp.float32)
    steps_up = (jnp.arange(count, dtype=jnp.float32) + jitter) / count
    return jnp.exp(jnp.log(spread) * steps_up)


def draw_query_cotangent(key, part):
    column_key = jax.random.fold_in(key, 11)
    value_key = jax.random.fold_in(key, 12)
    scales = 0.3 * rising(column_key, A, 10.0)
    values = jnp.clip(jax.random.normal(value_key, (TOTAL_TOKENS, A), jnp.float32), -5.0, 5.0)
    return (values * scales[None, :]).astype(jnp.bfloat16)


def draw_projector(key, part):
    column_key = jax.random.fold_in(key, 21)
    value_key = jax.random.fold_in(key, 22)
    scales = rising(column_key, RANK, 3.0)
    values = jnp.clip(jax.random.normal(value_key, (D, RANK), jnp.float32), -5.0, 5.0)
    return (values * scales[None, :] / jnp.sqrt(jnp.float32(D))).astype(jnp.bfloat16)


def draw_lowrank_mean(key, part):
    row_key = jax.random.fold_in(key, 31)
    column_key = jax.random.fold_in(key, 32)
    value_key = jax.random.fold_in(key, 33)
    row_scales = rising(row_key, RANK, 4.0)
    column_scales = rising(column_key, A, 4.0)
    values = jnp.clip(jax.random.normal(value_key, (RANK, A), jnp.float32), -4.0, 4.0)
    return 0.5 * values * row_scales[:, None] * column_scales[None, :]


def draw_gate_totals(key, part):
    order = jax.random.permutation(jax.random.fold_in(key, 41), HEADS)
    fast_count = max(HEADS // 2, 1)
    quick_path = order < fast_count
    sequences = TOTAL_TOKENS // DEVICE_TOKENS
    base = jnp.where(quick_path, jnp.log(40.0), jnp.log(jnp.float32(DEVICE_TOKENS)))
    noise = jnp.clip(jax.random.normal(jax.random.fold_in(key, 42), (HEADS, TOTAL_TOKENS), jnp.float32), -4.0, 4.0)
    gate_logarithm = jax.nn.log_sigmoid(base[:, None] + noise)
    block_factor = jnp.exp(jax.random.uniform(jax.random.fold_in(key, 43), (sequences,), jnp.float32, -0.7, 0.7))
    gate_logarithm = gate_logarithm * jnp.repeat(block_factor, DEVICE_TOKENS)[None, :]
    token_groups = jax.random.uniform(jax.random.fold_in(key, 44), (TOTAL_TOKENS,), jnp.float32) < 3.0 / DEVICE_TOKENS
    layer_level = jnp.log(jax.random.uniform(jax.random.fold_in(key, 45), (HEADS, TOTAL_TOKENS), jnp.float32, 0.5, 0.8))
    gate_logarithm = gate_logarithm + jnp.where(jnp.logical_and(token_groups[None, :], jnp.logical_not(quick_path)[:, None]), layer_level, 0.0)
    totals = jnp.cumsum(gate_logarithm.reshape(HEADS, sequences, DEVICE_TOKENS), axis=2)
    return totals.reshape(HEADS, TOTAL_TOKENS)


def block_levels(rng, dims, shards, least, largest):
    loudness, own = 1.0, jax.random.fold_in(rng, 6)
    for position, parts in shards:
        draws = jnp.exp(jax.random.uniform(jax.random.fold_in(own, position), (parts,), jnp.float32, least / len(shards), largest / len(shards)))
        loudness = loudness * jnp.repeat(draws, dims[position] // parts).reshape([-1 if axis == position else 1 for axis in range(len(dims))])
    return loudness


def scatter_about(key, dims, scale, most, pieces=(), kind=jnp.bfloat16):
    result = jax.random.normal(key, dims, jnp.float32) * scale
    if len(pieces) > 0:
        result = block_levels(key, dims, pieces, -0.22, 0.18) * result
    return jnp.clip(result, min=-most, max=most).astype(kind)


def setup_inputs(seed: int = 0) -> dict:
    key_list = jax.random.split(jax.random.key(seed), 11)
    return {
        "attention_input": scatter_about(key_list[0], (TOTAL_TOKENS, D), 1.0, 6.0, ((0, 256),)),
        "query_cotangent": draw_query_cotangent(jax.random.fold_in(key_list[10], 71), 0),
        "gate_cotangent": scatter_about(key_list[2], (HEADS, TOTAL_TOKENS), 1.0, 6.0, ((0, 2), (1, 256)), jnp.float32),
        "gate_totals": draw_gate_totals(jax.random.fold_in(key_list[10], 71), 0),
        "projector": draw_projector(jax.random.fold_in(key_list[10], 71), 0),
        "query_master": scatter_about(key_list[5], (D, A), D ** -0.5, 0.125, ((0, 64), (1, 2)), jnp.float32),
        "lowrank_mean": draw_lowrank_mean(jax.random.fold_in(key_list[10], 71), 0),
        "lowrank_square": jnp.clip(jnp.exp(math.log(2.0) - 3.6888794 * jax.random.uniform(key_list[7], (RANK, A), jnp.float32) ** block_levels(key_list[7], (RANK, A), ((0, 4), (1, 2)), -0.2, 0.2)), 0.05, 2.0),
        "gating_mean": scatter_about(key_list[8], (HEADS, D), 0.3, 1.8, ((0, 2),), jnp.float32),
        "gating_square": jnp.clip(jnp.exp(math.log(1.0) - 4.6051702 * jax.random.uniform(key_list[9], (HEADS, D), jnp.float32) ** block_levels(key_list[9], (HEADS, D), ((0, 2),), -0.2, 0.2)), 0.01, 1.0),
    }


BETA_ONE = 0.9
BETA_TWO = 0.95
STEP_RATE = 0.01
EPSILON = 1e-08
NORM_FLOOR = 1e-06

def reference(attention_input, query_cotangent, gate_cotangent, gate_totals, projector, query_master, lowrank_mean, lowrank_square, gating_mean, gating_square):
    norming = 1.0 / TOTAL_TOKENS ** 0.5
    contract = (((0,), (0,)), ((), ()))
    gradient = lax.dot_general(attention_input, query_cotangent, contract, preferred_element_type=jnp.float32) * norming
    factor = projector.astype(jnp.float32)
    projected = lax.dot_general(factor, gradient, contract, precision=lax.Precision.HIGHEST, preferred_element_type=jnp.float32)
    mean_after = BETA_ONE * lowrank_mean + (1.0 - BETA_ONE) * projected
    square_after = BETA_TWO * lowrank_square + (1.0 - BETA_TWO) * projected * projected
    direction = mean_after / (jnp.sqrt(square_after) + EPSILON)
    balance = jnp.sqrt(jnp.sum(direction * direction) / (jnp.sum(projected * projected) + NORM_FLOOR))
    blended = (direction - balance * projected).astype(jnp.bfloat16)
    query_update = jnp.dot(projector, blended, preferred_element_type=jnp.float32) + balance * gradient
    query_renewed = query_master - STEP_RATE * query_update
    query_copy = query_renewed.astype(jnp.bfloat16)
    sequences = TOTAL_TOKENS // DEVICE_TOKENS
    totals = gate_totals.reshape(HEADS, sequences, DEVICE_TOKENS)
    earlier = jnp.concatenate([jnp.zeros((HEADS, sequences, 1), jnp.float32), totals[:, :, :-1]], axis=2)
    gate_logarithm = totals - earlier
    trailing = lax.cumsum(gate_cotangent.reshape(HEADS, sequences, DEVICE_TOKENS), axis=2, reverse=True)
    gate_signal = (trailing * -jnp.expm1(gate_logarithm)).astype(jnp.bfloat16).reshape(HEADS, TOTAL_TOKENS)
    forget_gradient = jnp.dot(gate_signal, attention_input, preferred_element_type=jnp.float32) * norming
    gating_average = BETA_ONE * gating_mean + (1.0 - BETA_ONE) * forget_gradient
    gating_energy = BETA_TWO * gating_square + (1.0 - BETA_TWO) * forget_gradient * forget_gradient
    gating_update = gating_average / (jnp.sqrt(gating_energy) + EPSILON)
    return (query_update, query_renewed, query_copy, mean_after, square_after, gating_update, gating_average, gating_energy)
```

```python
import jax
import jax.numpy as jnp
from jax import lax
from jax.sharding import Mesh
from jax.sharding import PartitionSpec as P

FS = ("zh", "zl", "yh", "yl")
NEAR = ("zl", "yl", "x")
FAR = ("zh", "yh")
PAIR = ("x", "c")

BETA_ONE = 0.9
BETA_TWO = 0.95
STEP_RATE = 0.01
EPSILON = 1e-08
NORM_FLOOR = 1e-06
BF = jnp.bfloat16
F32 = jnp.float32


def swap(pieces, axes):
    return lax.all_to_all(pieces, axes, 0, 0, tiled=True)


def rounded(v):
    return lax.reduce_precision(v, 8, 7)


def split_two(v):
    high = rounded(v)
    return high.astype(BF), (v - high).astype(BF)


def dot_two(a, b):
    high, low = split_two(b)
    return jnp.dot(a, high, preferred_element_type=F32) + jnp.dot(a, low, preferred_element_type=F32)


def per_device(
    attention_input,
    query_cotangent,
    gate_cotangent,
    gate_totals,
    projector,
    query_master,
    lowrank_mean,
    lowrank_square,
    gating_mean,
    gating_square,
):
    nz, ny, nzl, nyl, nx, nc = (lax.axis_size(a) for a in ("zh", "yh", "zl", "yl", "x", "c"))
    far, near = nz * ny, nzl * nyl * nx
    tokens, width = attention_input.shape
    columns = query_cotangent.shape[1]
    heads = gate_cotangent.shape[0]
    own, rank = projector.shape
    lanes = columns // nx
    block = rank // nx
    rows = block // far
    tokens_all = tokens * far * near
    norming = 1.0 / tokens_all**0.5
    contract = (((0,), (0,)), ((), ()))

    factor = swap(jnp.broadcast_to(projector[None], (far, own, rank)), FAR).reshape(far * own, rank)

    partial = lax.dot_general(attention_input, query_cotangent, contract, preferred_element_type=F32)
    partial = partial.astype(BF).reshape(nz, nzl, ny, nyl, own, nx, lanes)
    partial = partial.transpose(1, 3, 5, 0, 2, 4, 6).reshape(near, far * own, lanes)
    near_sum = jnp.sum(swap(partial, NEAR).astype(F32), axis=0)

    earlier = jnp.concatenate([jnp.zeros((heads, 1), F32), gate_totals[:, :-1]], axis=1)
    later = lax.broadcasted_iota(jnp.int32, (tokens, tokens), 0) >= lax.broadcasted_iota(
        jnp.int32, (tokens, tokens), 1
    )
    trailing = jnp.dot(
        gate_cotangent, later.astype(F32), precision=lax.Precision.HIGHEST, preferred_element_type=F32
    )
    gate_signal = (trailing * -jnp.expm1(gate_totals - earlier)).astype(BF)
    gate_partial = jnp.dot(gate_signal, attention_input, preferred_element_type=F32)

    rank_partial = lax.dot_general(factor, rounded(near_sum).astype(BF), contract, preferred_element_type=F32)
    rank_partial = rank_partial.reshape(nx, far, rows, lanes).transpose(1, 0, 2, 3).reshape(far, nx * rows, lanes)
    second = jnp.concatenate(
        [
            near_sum.astype(BF).reshape(far, own, lanes),
            rank_partial.astype(BF),
            gate_partial.astype(BF).reshape(heads, far, width // far).transpose(1, 0, 2),
        ],
        axis=1,
    )
    second = jnp.sum(swap(second, FAR).astype(F32), axis=0) * norming
    gradient, rank_part, gate_part = jnp.split(second, [own, own + nx * rows])

    third = jnp.concatenate(
        [
            rank_part.reshape(nx, rows, lanes),
            jnp.zeros((nx, 8 - rows, lanes), F32),
            jnp.broadcast_to(gate_part[None], (nx, *gate_part.shape)),
        ],
        axis=1,
    )
    third = jnp.broadcast_to(third[None], (nzl * nyl, *third.shape)).reshape(near, *third.shape[1:])
    third = jnp.sum(swap(third, NEAR).reshape(nzl * nyl, nx, -1, lanes), axis=0)
    fourth = jnp.concatenate(
        [third[:, :rows].reshape(nx * rows, lanes), jnp.sum(third[:, 8:], axis=0)], axis=0
    )
    fourth = swap(jnp.broadcast_to(fourth[None], (far, *fourth.shape)), FAR)
    projected = (
        fourth[:, : nx * rows].reshape(far, nx, rows, lanes).transpose(0, 2, 1, 3).reshape(block, columns)
    )
    forget_gradient = fourth[:, nx * rows :].transpose(1, 0, 2).reshape(heads, width)

    mean_after = BETA_ONE * lowrank_mean + (1.0 - BETA_ONE) * projected
    square_after = BETA_TWO * lowrank_square + (1.0 - BETA_TWO) * projected * projected
    direction = mean_after / (jnp.sqrt(square_after) + EPSILON)
    place = lax.axis_index("x")
    own_factor = lax.dynamic_slice_in_dim(projector, place * block, block, 1)
    lifted_direction = dot_two(own_factor, direction)
    lifted_projected = dot_two(own_factor, projected).reshape(own, nx, lanes)
    mine = lax.broadcasted_iota(jnp.int32, (1, nx, 1), 1) == place
    lifted_projected = lifted_projected - jnp.where(mine, gradient[:, None, :], 0.0)
    sums = jnp.stack([jnp.sum(direction * direction), jnp.sum(projected * projected)])
    first_part = rounded(sums)
    second_part = rounded(sums - first_part)
    third_part = rounded(sums - first_part - second_part)
    scalars = jnp.stack([first_part, second_part, third_part]).reshape(6, 1)
    scalars = jnp.broadcast_to(jnp.pad(scalars, ((0, 2), (0, 0))), (8, lanes))
    fifth = jnp.concatenate(
        [
            lifted_direction.reshape(own, nx, lanes).transpose(1, 0, 2).reshape(nx * own, lanes),
            lifted_projected.transpose(1, 0, 2).reshape(nx * own, lanes),
            scalars,
        ],
        axis=0,
    ).astype(BF)
    fifth = swap(jnp.broadcast_to(fifth[None], (nx * nc, *fifth.shape)), PAIR).reshape(nx, nc, -1, lanes)
    scalars = jnp.sum(fifth[:, :, 2 * nx * own :, 0].astype(F32), axis=(0, 1))
    direction_squares = scalars[0] + scalars[2] + scalars[4]
    projected_squares = scalars[1] + scalars[3] + scalars[5]
    balance = jnp.sqrt(direction_squares / (projected_squares + NORM_FLOOR))
    lifts = lax.dynamic_index_in_dim(fifth, lax.axis_index("c"), 1, False)[:, : 2 * nx * own]
    lifts = jnp.sum(lifts.astype(F32), axis=0).reshape(2, nx, own, lanes)
    query_update = lifts[0] - balance * lifts[1]
    query_update = query_update.transpose(1, 0, 2).reshape(own, columns)
    query_renewed = query_master - STEP_RATE * query_update
    query_copy = query_renewed.astype(BF)
    gating_average = BETA_ONE * gating_mean + (1.0 - BETA_ONE) * forget_gradient
    gating_energy = BETA_TWO * gating_square + (1.0 - BETA_TWO) * forget_gradient * forget_gradient
    gating_update = gating_average / (jnp.sqrt(gating_energy) + EPSILON)
    return (
        query_update,
        query_renewed,
        query_copy,
        mean_after,
        square_after,
        gating_update,
        gating_average,
        gating_energy,
    )


def solution(mesh):
    split = Mesh(
        mesh.devices.reshape(4, 2, 4, 2, mesh.shape["rep"], mesh.shape["tp"]),
        ("zh", "zl", "yh", "yl", "x", "c"),
    )
    in_specs = (
        P((*FS, "x"), None),
        P((*FS, "x"), "c"),
        P("c", (*FS, "x")),
        P("c", (*FS, "x")),
        P(FS, None),
        P(FS, "c"),
        P("x", "c"),
        P("x", "c"),
        P("c", None),
        P("c", None),
    )
    out_specs = (
        P(FS, "c"),
        P(FS, "c"),
        P(FS, "c"),
        P("x", "c"),
        P("x", "c"),
        P("c", None),
        P("c", None),
        P("c", None),
    )
    return jax.shard_map(
        per_device, mesh=split, in_specs=in_specs, out_specs=out_specs, check_vma=False
    )
```

```python
import functools

import jax
import jax.numpy as jnp
from jax import lax
from jax.experimental import pallas as pl
from jax.experimental.pallas import tpu as pltpu
from jax.sharding import Mesh
from jax.sharding import PartitionSpec as P

FS = ("zh", "zl", "yh", "yl")
NEAR = ("zl", "yl", "x")
FAR = ("zh", "yh")
PAIR = ("x", "c")

BETA_ONE = 0.9
BETA_TWO = 0.95
STEP_RATE = 0.01
EPSILON = 1e-08
NORM_FLOOR = 1e-06
BF = jnp.bfloat16
F32 = jnp.float32
FIRST = (((0,), (0,)), ((), ()))
LANES = 128
VMEM = pl.BlockSpec(memory_space=pltpu.VMEM)
SMEM = pl.BlockSpec(memory_space=pltpu.SMEM)


def swap(pieces, axes):
    return lax.all_to_all(pieces, axes, 0, 0, tiled=True)


def shifted(value, axis, step):
    length = lax.axis_size(axis)
    return lax.ppermute(value, axis, [(i, (i + step) % length) for i in range(length)])


def turned(value, axis):
    steps = range(1, lax.axis_size(axis))
    return jnp.stack([value, *(shifted(value, axis, s) for s in steps)])


def split_two(v):
    high = v.astype(BF)
    return high, (v - high.astype(F32)).astype(BF)


def dot(a, b, dims=(((1,), (0,)), ((), ()))):
    return lax.dot_general(a, b, dims, preferred_element_type=F32)


def one_less_exp(v):
    series = 1.0 + v * 0.125
    for k in range(7, 1, -1):
        series = 1.0 + v * (1.0 / k) * series
    return jnp.where(v > -0.3, -v * series, 1.0 - jnp.exp(v))


def first_kernel(sizes, x_ref, q_ref, cot_ref, tot_ref, out_ref, signal):
    nzl, ny, nyl, nx, own = sizes
    step = pl.program_id(0)

    @pl.when(step == 0)
    def _():
        cot = cot_ref[...]
        heads, tokens = cot.shape
        later = lax.broadcasted_iota(jnp.int32, (tokens, tokens), 0) >= lax.broadcasted_iota(
            jnp.int32, (tokens, tokens), 1
        )
        later = jnp.where(later, 1.0, 0.0).astype(BF)
        one = cot.astype(BF)
        rest = cot - one.astype(F32)
        two = rest.astype(BF)
        three = (rest - two.astype(F32)).astype(BF)
        trailing = dot(three, later) + dot(two, later) + dot(one, later)
        totals = tot_ref[...]
        earlier = pltpu.roll(totals, 1, 1)
        lane = lax.broadcasted_iota(jnp.int32, totals.shape, 1)
        gate = totals - jnp.where(lane == 0, 0.0, earlier)
        signal[...] = (trailing * one_less_exp(gate)).astype(BF)

    block = x_ref[...]
    part = dot(block, q_ref[...], FIRST).astype(BF)
    zh, zl = step // nzl, lax.rem(step, nzl)
    for yh in range(ny):
        for yl in range(nyl):
            row = (yh * nyl + yl) * own
            for q in range(nx):
                out_ref[(zl * nyl + yl) * nx + q, pl.ds((zh * ny + yh) * own, own), :] = part[
                    row : row + own, q * LANES : (q + 1) * LANES
                ]
    gates = dot(signal[...], block).astype(BF)
    far_rows = out_ref.shape[1] - gates.shape[0]
    per_step = gates.shape[1] // LANES
    for k in range(per_step):
        out_ref[step * per_step + k, far_rows:, :] = gates[:, k * LANES : (k + 1) * LANES]


def second_kernel(sizes, at_ref, p_ref, in_ref, out_ref, total):
    nz, ny, own, rank_rows, heads = sizes
    summed = in_ref[0].astype(F32)
    for k in range(1, in_ref.shape[0]):
        summed = summed + in_ref[k].astype(F32)
    total[...] = summed
    rows = nz * ny * own
    rank = None
    for b in range(ny):
        for a in range(nz):
            zh = lax.rem(at_ref[0] + nz - a, nz)
            yh = lax.rem(at_ref[1] + ny - b, ny)
            high, low = split_two(total[pl.ds((zh * ny + yh) * own, own), :])
            factor = p_ref[b, a]
            term = dot(factor, high, FIRST) + dot(factor, low, FIRST)
            rank = term if rank is None else rank + term
    gates = total[rows:, :].astype(BF)
    for k in range(nz * ny):
        out_ref[k, :own, :] = total[k * own : (k + 1) * own, :].astype(BF)
        high, low = split_two(rank[k * rank_rows : (k + 1) * rank_rows, :])
        out_ref[k, own : own + rank_rows, :] = high
        out_ref[k, own + rank_rows : own + 2 * rank_rows, :] = low
        out_ref[k, own + 2 * rank_rows :, :] = gates


def third_kernel(sizes, norming, in_ref, gradient_ref, out_ref, gate_ref):
    own, rank_rows = sizes
    summed = in_ref[0].astype(F32)
    for k in range(1, in_ref.shape[0]):
        summed = summed + in_ref[k].astype(F32)
    summed = summed * norming
    gradient_ref[...] = summed[:own]
    rank = (summed[own : own + rank_rows] + summed[own + rank_rows : own + 2 * rank_rows]).astype(BF)
    for k in range(out_ref.shape[0]):
        out_ref[k] = rank
    gate_ref[...] = summed[own + 2 * rank_rows :]


def fourth_kernel(sizes, at_ref, in_ref, moments_ref, p_ref, gradient_ref, out_ref, projected, direction):
    nz, nzl, ny, nyl, nx, nc, rank_rows = sizes
    for zh in range(nz):
        for yh in range(ny):
            piece = None
            for zl in range(nzl):
                for yl in range(nyl):
                    term = in_ref[((zh * nzl + zl) * ny + yh) * nyl + yl].astype(F32)
                    piece = term if piece is None else piece + term
            k = zh * ny + yh
            projected[k * rank_rows : (k + 1) * rank_rows, :] = piece
    block = projected.shape[0] // nx
    squares = jnp.zeros((2, LANES), F32)
    for s in range(nx):
        where = lax.rem(at_ref[2] + nx - s, nx) * block
        p = projected[pl.ds(where, block), :]
        mean = BETA_ONE * moments_ref[s, :block] + (1.0 - BETA_ONE) * p
        square = BETA_TWO * moments_ref[s, block:] + (1.0 - BETA_TWO) * p * p
        d = mean / (jnp.sqrt(square) + EPSILON)
        direction[pl.ds(where, block), :] = d
        squares = squares + jnp.concatenate(
            [jnp.sum(d * d, axis=0, keepdims=True), jnp.sum(p * p, axis=0, keepdims=True)], axis=0
        )
    factor = p_ref[...]
    own = factor.shape[0]
    high, low = split_two(direction[...])
    lifted_direction = dot(factor, high) + dot(factor, low)
    high, low = split_two(projected[...])
    lifted_projected = dot(factor, high) + dot(factor, low) - gradient_ref[...]
    squares = jnp.concatenate([squares, jnp.zeros((6, LANES), F32)], axis=0)
    for x in range(nx):
        for c in range(nc):
            k = x * nc + c
            out_ref[k, :own] = lifted_direction
            out_ref[k, own : 2 * own] = lifted_projected
            out_ref[k, 2 * own : 2 * own + block] = projected[x * block : (x + 1) * block, :]
            out_ref[k, 2 * own + block :] = squares


def last_kernel(
    sizes, at_ref, in_ref, master_ref, mean_ref, square_ref, update_ref, new_ref, copy_ref, mean_out, square_out
):
    nx, nc, own, block = sizes
    squares = in_ref[0, 2 * own + block :]
    for k in range(1, nx * nc):
        squares = squares + in_ref[k, 2 * own + block :]
    direction_squares = jnp.sum(squares[0:1], axis=1, keepdims=True)
    projected_squares = jnp.sum(squares[1:2], axis=1, keepdims=True)
    balance = jnp.sqrt(direction_squares / (projected_squares + NORM_FLOOR))
    for x in range(nx):
        k = x * nc + at_ref[3]
        cut = slice(x * LANES, (x + 1) * LANES)
        update = in_ref[k, :own] - balance * in_ref[k, own : 2 * own]
        update_ref[:, cut] = update
        new = master_ref[:, cut] - STEP_RATE * update
        new_ref[:, cut] = new
        copy_ref[:, cut] = new.astype(BF)
        p = in_ref[k, 2 * own : 2 * own + block]
        mean_out[:, cut] = BETA_ONE * mean_ref[:, cut] + (1.0 - BETA_ONE) * p
        square_out[:, cut] = BETA_TWO * square_ref[:, cut] + (1.0 - BETA_TWO) * p * p


def gate_kernel(sizes, at_ref, in_ref, mean_ref, square_ref, update_ref, average_ref, energy_ref):
    nzl, nyl, nx = sizes
    for a in range(nzl):
        for b in range(nyl):
            for s in range(nx):
                zl = lax.rem(at_ref[4] + nzl - a, nzl)
                yl = lax.rem(at_ref[5] + nyl - b, nyl)
                x = lax.rem(at_ref[2] + nx - s, nx)
                cut = pl.ds(((zl * nyl + yl) * nx + x) * LANES, LANES)
                g = in_ref[a, b, s]
                average = BETA_ONE * mean_ref[:, cut] + (1.0 - BETA_ONE) * g
                energy = BETA_TWO * square_ref[:, cut] + (1.0 - BETA_TWO) * g * g
                average_ref[:, cut] = average
                energy_ref[:, cut] = energy
                update_ref[:, cut] = average / (jnp.sqrt(energy) + EPSILON)


def per_device(
    attention_input,
    query_cotangent,
    gate_cotangent,
    gate_totals,
    projector,
    query_master,
    lowrank_mean,
    lowrank_square,
    gating_mean,
    gating_square,
):
    nz, ny, nzl, nyl, nx, nc = (lax.axis_size(a) for a in ("zh", "yh", "zl", "yl", "x", "c"))
    far, near = nz * ny, nzl * nyl * nx
    tokens, width = attention_input.shape
    columns = query_cotangent.shape[1]
    heads = gate_cotangent.shape[0]
    own, rank = projector.shape
    block = rank // nx
    rank_rows = rank // far
    norming = 1.0 / (tokens * far * near) ** 0.5
    shape = jax.ShapeDtypeStruct
    at = jnp.stack([lax.axis_index(a) for a in ("zh", "yh", "x", "c", "zl", "yl")]).astype(jnp.int32)

    factors = turned(turned(projector, "zh"), "yh")

    cut = ny * nyl * own
    first = pl.pallas_call(
        functools.partial(first_kernel, (nzl, ny, nyl, nx, own)),
        out_shape=shape((near, far * own + heads, LANES), BF),
        grid=(nz * nzl,),
        in_specs=[
            pl.BlockSpec((tokens, cut), lambda z: (0, z)),
            pl.BlockSpec((tokens, columns), lambda z: (0, 0)),
            pl.BlockSpec((heads, tokens), lambda z: (0, 0)),
            pl.BlockSpec((heads, tokens), lambda z: (0, 0)),
        ],
        out_specs=pl.BlockSpec((near, far * own + heads, LANES), lambda z: (0, 0, 0)),
        scratch_shapes=[pltpu.VMEM((heads, tokens), BF)],
        name="first",
    )(attention_input, query_cotangent, gate_cotangent, gate_totals)
    first = swap(first, NEAR)

    mine = jnp.concatenate(
        [lowrank_mean.reshape(block, nx, LANES), lowrank_square.reshape(block, nx, LANES)]
    ).transpose(1, 0, 2)
    first, mine = lax.optimization_barrier((first, mine))
    second = pl.pallas_call(
        functools.partial(second_kernel, (nz, ny, own, rank_rows, heads)),
        out_shape=shape((far, own + 2 * rank_rows + heads, LANES), BF),
        in_specs=[SMEM, VMEM, VMEM],
        out_specs=VMEM,
        scratch_shapes=[pltpu.VMEM((far * own + heads, LANES), F32)],
        name="second",
    )(at, factors, first)
    second = swap(second, FAR)

    moments = [lax.dynamic_index_in_dim(mine, at[2], 0, False)]
    for s in range(1, nx):
        piece = lax.dynamic_index_in_dim(mine, lax.rem(at[2] + s, nx), 0, False)
        moments.append(shifted(piece, "x", s))
    moments = jnp.stack(moments)
    second, moments = lax.optimization_barrier((second, moments))

    gradient, third, gates = pl.pallas_call(
        functools.partial(third_kernel, (own, rank_rows), norming),
        out_shape=(
            shape((own, LANES), F32),
            shape((far * nzl * nyl, rank_rows, LANES), BF),
            shape((heads, LANES), F32),
        ),
        in_specs=[VMEM],
        out_specs=(VMEM, VMEM, VMEM),
        name="third",
    )(second)
    third = swap(third, FS)
    gates = turned(turned(turned(gates, "x"), "yl"), "zl")
    third, gates = lax.optimization_barrier((third, gates))

    fourth = pl.pallas_call(
        functools.partial(fourth_kernel, (nz, nzl, ny, nyl, nx, nc, rank_rows)),
        out_shape=shape((nx * nc, 2 * own + block + 8, LANES), F32),
        in_specs=[SMEM, VMEM, VMEM, VMEM, VMEM],
        out_specs=VMEM,
        scratch_shapes=[pltpu.VMEM((rank, LANES), F32), pltpu.VMEM((rank, LANES), F32)],
        name="fourth",
    )(at, third, moments, projector, gradient)
    fourth = swap(fourth, PAIR)

    gating_update, gating_average, gating_energy = pl.pallas_call(
        functools.partial(gate_kernel, (nzl, nyl, nx)),
        out_shape=(shape((heads, width), F32),) * 3,
        in_specs=[SMEM, VMEM, VMEM, VMEM],
        out_specs=(VMEM,) * 3,
        name="gating",
    )(at, gates, gating_mean, gating_square)

    query_update, query_renewed, query_copy, mean_after, square_after = pl.pallas_call(
        functools.partial(last_kernel, (nx, nc, own, block)),
        out_shape=(
            shape((own, columns), F32),
            shape((own, columns), F32),
            shape((own, columns), BF),
            shape((block, columns), F32),
            shape((block, columns), F32),
        ),
        in_specs=[SMEM, VMEM, VMEM, VMEM, VMEM],
        out_specs=(VMEM,) * 5,
        name="last",
    )(at, fourth, query_master, lowrank_mean, lowrank_square)
    return (
        query_update,
        query_renewed,
        query_copy,
        mean_after,
        square_after,
        gating_update,
        gating_average,
        gating_energy,
    )


def solution(mesh):
    split = Mesh(
        mesh.devices.reshape(4, 2, 4, 2, mesh.shape["rep"], mesh.shape["tp"]),
        ("zh", "zl", "yh", "yl", "x", "c"),
    )
    in_specs = (
        P((*FS, "x"), None),
        P((*FS, "x"), "c"),
        P("c", (*FS, "x")),
        P("c", (*FS, "x")),
        P(FS, None),
        P(FS, "c"),
        P("x", "c"),
        P("x", "c"),
        P("c", None),
        P("c", None),
    )
    out_specs = (
        P(FS, "c"),
        P(FS, "c"),
        P(FS, "c"),
        P("x", "c"),
        P("x", "c"),
        P("c", None),
        P("c", None),
        P("c", None),
    )
    return jax.shard_map(
        per_device, mesh=split, in_specs=in_specs, out_specs=out_specs, check_vma=False
    )
```

```python
import functools

import jax
import jax.numpy as jnp
from jax import lax
from jax.experimental import pallas as pl
from jax.experimental.pallas import tpu as pltpu
from jax.sharding import Mesh
from jax.sharding import PartitionSpec as P

FS = ("zh", "zl", "yh", "yl")
NEAR = ("zl", "yl", "x")
FAR = ("zh", "yh")
PAIR = ("x", "c")

BETA_ONE = 0.9
BETA_TWO = 0.95
STEP_RATE = 0.01
EPSILON = 1e-08
NORM_FLOOR = 1e-06
BF = jnp.bfloat16
F32 = jnp.float32
FIRST = (((0,), (0,)), ((), ()))
LANES = 128
VMEM = pl.BlockSpec(memory_space=pltpu.VMEM)
ANY = pl.BlockSpec(memory_space=pltpu.HBM)
SMEM = pl.BlockSpec(memory_space=pltpu.SMEM)


def swap(pieces, axes):
    return lax.all_to_all(pieces, axes, 0, 0, tiled=True)


def shifted(value, axis, step):
    length = lax.axis_size(axis)
    return lax.ppermute(value, axis, [(i, (i + step) % length) for i in range(length)])


def turned(value, axis):
    steps = range(1, lax.axis_size(axis))
    return jnp.stack([value, *(shifted(value, axis, s) for s in steps)])


def split_two(v):
    high = v.astype(BF)
    return high, (v - high.astype(F32)).astype(BF)


def dot(a, b, dims=(((1,), (0,)), ((), ()))):
    return lax.dot_general(a, b, dims, preferred_element_type=F32)


def one_less_exp(v):
    series = 1.0 + v * 0.125
    for k in range(7, 1, -1):
        series = 1.0 + v * (1.0 / k) * series
    return jnp.where(v > -0.3, -v * series, 1.0 - jnp.exp(v))


def gate_signals(cot, totals):
    heads, tokens = cot.shape
    later = lax.broadcasted_iota(jnp.int32, (tokens, tokens), 0) >= lax.broadcasted_iota(
        jnp.int32, (tokens, tokens), 1
    )
    later = jnp.where(later, 1.0, 0.0).astype(BF)
    one = cot.astype(BF).astype(F32)
    rest = cot - one
    two = rest.astype(BF).astype(F32)
    parts = jnp.concatenate([one, two, rest - two, jnp.zeros_like(one)], axis=0).astype(BF)
    trailing = dot(parts, later)
    trailing = trailing[2 * heads : 3 * heads] + trailing[heads : 2 * heads] + trailing[:heads]
    lane = lax.broadcasted_iota(jnp.int32, totals.shape, 1)
    gate = totals - jnp.where(lane == 0, 0.0, pltpu.roll(totals, 1, 1))
    return (trailing * one_less_exp(gate)).astype(BF)


def first_kernel(
    sizes, x_ref, q_ref, cot_ref, tot_ref, out_ref, x_held, q_held, out_held, gate_held, x_sem, q_sem, out_sem
):
    nz, nzl, ny, nyl, nx, own = sizes
    wide = x_held.shape[2]
    heads, steps = gate_held.shape[1], nz * nzl
    copies = []
    q_copy = pltpu.make_async_copy(q_ref, q_held, q_sem)
    q_copy.start()
    for z in range(steps):
        copy = pltpu.make_async_copy(x_ref.at[:, z * wide : (z + 1) * wide], x_held.at[z], x_sem.at[z])
        copy.start()
        copies.append(copy)
    signal = gate_signals(cot_ref[...], tot_ref[...])
    q_copy.wait()
    sends = []
    for z in range(steps):
        copies[z].wait()
        block = x_held[z]
        part = dot(block, q_held[...], FIRST).astype(BF)
        zh, zl = divmod(z, nzl)
        for yh in range(ny):
            for yl in range(nyl):
                row = (yh * nyl + yl) * own
                for q in range(nx):
                    out_held[z, yl * nx + q, yh * own : (yh + 1) * own, :] = part[
                        row : row + own, q * LANES : (q + 1) * LANES
                    ]
        target = out_ref.at[
            zl * nyl * nx : (zl + 1) * nyl * nx, zh * ny * own : (zh + 1) * ny * own, :
        ]
        send = pltpu.make_async_copy(out_held.at[z], target, out_sem.at[z])
        send.start()
        sends.append(send)
        gates = dot(signal, block).astype(BF)
        for k in range(wide // LANES):
            gate_held[z * (wide // LANES) + k] = gates[:, k * LANES : (k + 1) * LANES]
    target = out_ref.at[:, nz * ny * own : nz * ny * own + heads, :]
    send = pltpu.make_async_copy(gate_held, target, out_sem.at[steps])
    send.start()
    sends.append(send)
    for send in sends:
        send.wait()


def second_kernel(own, in_ref, out_ref):
    far, rows = out_ref.shape[:2]
    for k in range(far + 1):
        cut = slice(k * own, (k + 1) * own) if k < far else slice(far * own, in_ref.shape[1])
        summed = in_ref[0, cut].astype(F32)
        for i in range(1, in_ref.shape[0]):
            summed = summed + in_ref[i, cut].astype(F32)
        if k < far:
            out_ref[k, :own, :] = summed.astype(BF)
        else:
            for j in range(far):
                out_ref[j, own:, :] = summed.astype(BF)


def third_kernel(norming, in_ref, p_ref, gradient_ref, out_ref, gate_ref):
    own = p_ref.shape[0]
    summed = in_ref[0].astype(F32)
    for k in range(1, in_ref.shape[0]):
        summed = summed + in_ref[k].astype(F32)
    summed = summed * norming
    gate_ref[...] = summed[own:]
    gradient = summed[:own]
    gradient_ref[...] = gradient
    factor = p_ref[...]
    high, low = split_two(gradient)
    rank = dot(factor, high, FIRST) + dot(factor, low, FIRST)
    top = lax.broadcasted_iota(jnp.int32, (8, LANES), 0) < 4
    for g in range(out_ref.shape[0] // 2):
        value = rank[8 * g : 8 * g + 8]
        high = value.astype(BF).astype(F32)
        low = value - high
        out_ref[2 * g] = jnp.where(top, high, pltpu.roll(low, 4, 0)).astype(BF)
        out_ref[2 * g + 1] = jnp.where(top, pltpu.roll(high, 4, 0), low).astype(BF)


def rank_kernel(in_ref, out_ref):
    summed = in_ref[0].astype(F32)
    for k in range(1, in_ref.shape[0]):
        summed = summed + in_ref[k].astype(F32)
    summed = summed + pltpu.roll(summed, 4, 0)
    high = summed.astype(BF).astype(F32)
    top = lax.broadcasted_iota(jnp.int32, (8, LANES), 0) < 4
    piece = jnp.where(top, high, summed - high).astype(BF)
    for k in range(out_ref.shape[0]):
        out_ref[k] = piece


def fourth_kernel(
    sizes, at_ref, in_ref, moments_ref, p_ref, gradient_ref, gates_ref, out_ref, projected, direction
):
    nx, nc = sizes
    top = lax.broadcasted_iota(jnp.int32, (8, LANES), 0) < 4
    for g in range(in_ref.shape[0] // 2):
        even, odd = in_ref[2 * g].astype(F32), in_ref[2 * g + 1].astype(F32)
        even = even + pltpu.roll(even, 4, 0)
        odd = odd + pltpu.roll(odd, 4, 0)
        projected[8 * g : 8 * g + 8, :] = jnp.where(top, even, odd)
    block = projected.shape[0] // nx
    squares = jnp.zeros((2, LANES), F32)
    for s in range(nx):
        where = pl.multiple_of(lax.rem(at_ref[0] + nx - s, nx) * block, block)
        p = projected[pl.ds(where, block), :]
        mean = BETA_ONE * moments_ref[s, :block] + (1.0 - BETA_ONE) * p
        square = BETA_TWO * moments_ref[s, block:] + (1.0 - BETA_TWO) * p * p
        d = mean / (jnp.sqrt(square) + EPSILON)
        direction[pl.ds(where, block), :] = d
        squares = squares + jnp.concatenate(
            [jnp.sum(d * d, axis=0, keepdims=True), jnp.sum(p * p, axis=0, keepdims=True)], axis=0
        )
    factor = p_ref[...]
    own = factor.shape[0]
    high, low = split_two(direction[...])
    lifted_direction = dot(factor, high) + dot(factor, low)
    high, low = split_two(projected[...])
    lifted_projected = dot(factor, high) + dot(factor, low) - gradient_ref[...]
    squares = jnp.concatenate([squares, jnp.zeros((6, LANES), F32)], axis=0)
    gates = gates_ref[...].reshape(-1, LANES)
    for x in range(nx):
        for c in range(nc):
            k = x * nc + c
            out_ref[k, :own] = lifted_direction
            out_ref[k, own : 2 * own] = lifted_projected
            out_ref[k, 2 * own : 2 * own + block] = projected[x * block : (x + 1) * block, :]
            out_ref[k, 2 * own + block : 2 * own + block + 8] = squares
            out_ref[k, 2 * own + block + 8 :] = gates


def last_kernel(
    sizes,
    at_ref,
    in_ref,
    master_ref,
    mean_ref,
    square_ref,
    gate_mean_ref,
    gate_square_ref,
    update_ref,
    new_ref,
    copy_ref,
    mean_out,
    square_out,
    gate_update_ref,
    average_ref,
    energy_ref,
):
    nzl, nyl, nx, nc, own, block = sizes
    heads = gate_mean_ref.shape[0]
    after = 2 * own + block + 8
    squares = in_ref[0, 2 * own + block : after]
    for k in range(1, nx * nc):
        squares = squares + in_ref[k, 2 * own + block : after]
    direction_squares = jnp.sum(squares[0:1], axis=1, keepdims=True)
    projected_squares = jnp.sum(squares[1:2], axis=1, keepdims=True)
    balance = jnp.sqrt(direction_squares / (projected_squares + NORM_FLOOR))
    for x in range(nx):
        k = x * nc + at_ref[1]
        cut = slice(x * LANES, (x + 1) * LANES)
        update = in_ref[k, :own] - balance * in_ref[k, own : 2 * own]
        update_ref[:, cut] = update
        new = master_ref[:, cut] - STEP_RATE * update
        new_ref[:, cut] = new
        copy_ref[:, cut] = new.astype(BF)
        p = in_ref[k, 2 * own : 2 * own + block]
        mean_out[:, cut] = BETA_ONE * mean_ref[:, cut] + (1.0 - BETA_ONE) * p
        square_out[:, cut] = BETA_TWO * square_ref[:, cut] + (1.0 - BETA_TWO) * p * p
        for a in range(nzl):
            for b in range(nyl):
                zl = lax.rem(at_ref[2] + nzl - a, nzl)
                yl = lax.rem(at_ref[3] + nyl - b, nyl)
                place = pl.ds(pl.multiple_of(((zl * nyl + yl) * nx + x) * LANES, LANES), LANES)
                row = after + (a * nyl + b) * heads
                g = in_ref[k, row : row + heads]
                average = BETA_ONE * gate_mean_ref[:, place] + (1.0 - BETA_ONE) * g
                energy = BETA_TWO * gate_square_ref[:, place] + (1.0 - BETA_TWO) * g * g
                average_ref[:, place] = average
                energy_ref[:, place] = energy
                gate_update_ref[:, place] = average / (jnp.sqrt(energy) + EPSILON)


def near_memory(value):
    return pltpu.with_memory_space_constraint(value, pltpu.VMEM)


def per_device(
    attention_input,
    query_cotangent,
    gate_cotangent,
    gate_totals,
    projector,
    query_master,
    lowrank_mean,
    lowrank_square,
    gating_mean,
    gating_square,
):
    nz, ny, nzl, nyl, nx, nc = (lax.axis_size(a) for a in ("zh", "yh", "zl", "yl", "x", "c"))
    far, near = nz * ny, nzl * nyl * nx
    every = far * nzl * nyl
    tokens, width = attention_input.shape
    columns = query_cotangent.shape[1]
    heads = gate_cotangent.shape[0]
    own, rank = projector.shape
    block = rank // nx
    norming = 1.0 / (tokens * far * near) ** 0.5
    shape = jax.ShapeDtypeStruct
    at = jnp.stack([lax.axis_index(a) for a in ("x", "c", "zl", "yl")]).astype(jnp.int32)

    wide = ny * nyl * own
    first = pl.pallas_call(
        functools.partial(first_kernel, (nz, nzl, ny, nyl, nx, own)),
        out_shape=shape((near, far * own + heads, LANES), BF),
        in_specs=[ANY, ANY, VMEM, VMEM],
        out_specs=ANY,
        scratch_shapes=[
            pltpu.VMEM((nz * nzl, tokens, wide), BF),
            pltpu.VMEM((tokens, columns), BF),
            pltpu.VMEM((nz * nzl, nyl * nx, ny * own, LANES), BF),
            pltpu.VMEM((near, heads, LANES), BF),
            pltpu.SemaphoreType.DMA((nz * nzl,)),
            pltpu.SemaphoreType.DMA,
            pltpu.SemaphoreType.DMA((nz * nzl + 1,)),
        ],
        name="first",
    )(attention_input, query_cotangent, gate_cotangent, gate_totals)
    first = swap(first, NEAR)

    second = pl.pallas_call(
        functools.partial(second_kernel, own),
        out_shape=pltpu.VMEM((far, own + heads, LANES), BF),
        in_specs=[VMEM],
        out_specs=VMEM,
        name="second",
    )(near_memory(first))
    mine = jnp.concatenate(
        [lowrank_mean.reshape(block, nx, LANES), lowrank_square.reshape(block, nx, LANES)]
    ).transpose(1, 0, 2)
    place = lax.axis_index("x")
    pieces = [lax.dynamic_index_in_dim(mine, lax.rem(place + s, nx), 0, False) for s in range(nx)]
    first, pieces = lax.optimization_barrier((first, pieces))
    second = swap(second, FAR)
    moments = jnp.stack([pieces[0], *(shifted(pieces[s], "x", s) for s in range(1, nx))])
    second, moments = lax.optimization_barrier((second, moments))

    gradient, third, gates = pl.pallas_call(
        functools.partial(third_kernel, norming),
        out_shape=(
            pltpu.VMEM((own, LANES), F32),
            pltpu.VMEM((every, 8, LANES), BF),
            pltpu.VMEM((heads, LANES), F32),
        ),
        in_specs=[VMEM, VMEM],
        out_specs=(VMEM, VMEM, VMEM),
        name="third",
    )(near_memory(second), projector)
    third = swap(third, FS)
    gates = turned(gates, "yl")
    third, gates = lax.optimization_barrier((third, gates))

    ranked = pl.pallas_call(
        rank_kernel,
        out_shape=pltpu.VMEM((every, 8, LANES), BF),
        in_specs=[VMEM],
        out_specs=VMEM,
        name="ranked",
    )(near_memory(third))
    ranked = swap(ranked, FS)
    gates = turned(gates, "zl")
    ranked, gates = lax.optimization_barrier((ranked, gates))

    fourth = pl.pallas_call(
        functools.partial(fourth_kernel, (nx, nc)),
        out_shape=pltpu.VMEM((nx * nc, 2 * own + block + 8 + nzl * nyl * heads, LANES), F32),
        in_specs=[SMEM, VMEM, VMEM, VMEM, VMEM, VMEM],
        out_specs=VMEM,
        scratch_shapes=[pltpu.VMEM((rank, LANES), F32), pltpu.VMEM((rank, LANES), F32)],
        name="fourth",
    )(at, near_memory(ranked), near_memory(moments), projector, gradient, near_memory(gates))
    fourth = swap(fourth, PAIR)

    return pl.pallas_call(
        functools.partial(last_kernel, (nzl, nyl, nx, nc, own, block)),
        out_shape=(
            shape((own, columns), F32),
            shape((own, columns), F32),
            shape((own, columns), BF),
            shape((block, columns), F32),
            shape((block, columns), F32),
            shape((heads, width), F32),
            shape((heads, width), F32),
            shape((heads, width), F32),
        ),
        in_specs=[SMEM, *[VMEM] * 6],
        out_specs=(VMEM,) * 8,
        name="last",
    )(at, near_memory(fourth), query_master, lowrank_mean, lowrank_square, gating_mean, gating_square)


def solution(mesh):
    split = Mesh(
        mesh.devices.reshape(4, 2, 4, 2, mesh.shape["rep"], mesh.shape["tp"]),
        ("zh", "zl", "yh", "yl", "x", "c"),
    )
    in_specs = (
        P((*FS, "x"), None),
        P((*FS, "x"), "c"),
        P("c", (*FS, "x")),
        P("c", (*FS, "x")),
        P(FS, None),
        P(FS, "c"),
        P("x", "c"),
        P("x", "c"),
        P("c", None),
        P("c", None),
    )
    out_specs = (
        P(FS, "c"),
        P(FS, "c"),
        P(FS, "c"),
        P("x", "c"),
        P("x", "c"),
        P("c", None),
        P("c", None),
        P("c", None),
    )
    return jax.shard_map(
        per_device, mesh=split, in_specs=in_specs, out_specs=out_specs, check_vma=False
    )
```

```python
import functools

import jax
import jax.numpy as jnp
from jax import lax
from jax.experimental import pallas as pl
from jax.experimental.pallas import tpu as pltpu
from jax.sharding import Mesh
from jax.sharding import PartitionSpec as P

FS = ("zh", "zl", "yh", "yl")
NEAR = ("zl", "yl", "x")
FAR = ("zh", "yh")
PAIR = ("x", "c")

BETA_ONE = 0.9
BETA_TWO = 0.95
STEP_RATE = 0.01
EPSILON = 1e-08
NORM_FLOOR = 1e-06
BF = jnp.bfloat16
F32 = jnp.float32
FIRST = (((0,), (0,)), ((), ()))
LANES = 128
VMEM = pl.BlockSpec(memory_space=pltpu.VMEM)
ANY = pl.BlockSpec(memory_space=pltpu.HBM)
SMEM = pl.BlockSpec(memory_space=pltpu.SMEM)


def swap(pieces, axes):
    return lax.all_to_all(pieces, axes, 0, 0, tiled=True)


def shifted(value, axis, step):
    length = lax.axis_size(axis)
    return lax.ppermute(value, axis, [(i, (i + step) % length) for i in range(length)])


def split_two(v):
    high = v.astype(BF)
    return high, (v - high.astype(F32)).astype(BF)


def dot(a, b, dims=(((1,), (0,)), ((), ()))):
    return lax.dot_general(a, b, dims, preferred_element_type=F32)


def one_less_exp(v):
    series = 1.0 + v * 0.125
    for k in range(7, 1, -1):
        series = 1.0 + v * (1.0 / k) * series
    return jnp.where(v > -0.3, -v * series, 1.0 - jnp.exp(v))


def gate_signals(cot, totals):
    heads, tokens = cot.shape
    later = lax.broadcasted_iota(jnp.int32, (tokens, tokens), 0) >= lax.broadcasted_iota(
        jnp.int32, (tokens, tokens), 1
    )
    later = jnp.where(later, 1.0, 0.0).astype(BF)
    one = cot.astype(BF).astype(F32)
    rest = cot - one
    two = rest.astype(BF).astype(F32)
    parts = jnp.concatenate([one, two, rest - two, jnp.zeros_like(one)], axis=0).astype(BF)
    trailing = dot(parts, later)
    trailing = trailing[2 * heads : 3 * heads] + trailing[heads : 2 * heads] + trailing[:heads]
    lane = lax.broadcasted_iota(jnp.int32, totals.shape, 1)
    gate = totals - jnp.where(lane == 0, 0.0, pltpu.roll(totals, 1, 1))
    return (trailing * one_less_exp(gate)).astype(BF)


def first_kernel(
    sizes, x_ref, q_ref, cot_ref, tot_ref, out_ref, x_held, q_held, out_held, gate_held, x_sem, q_sem, out_sem
):
    nz, nzl, ny, nyl, nx, own = sizes
    wide = x_held.shape[2]
    heads, steps = gate_held.shape[1], nz * nzl
    copies = []
    q_copy = pltpu.make_async_copy(q_ref, q_held, q_sem)
    q_copy.start()
    for z in range(steps):
        copy = pltpu.make_async_copy(x_ref.at[:, z * wide : (z + 1) * wide], x_held.at[z], x_sem.at[z])
        copy.start()
        copies.append(copy)
    signal = gate_signals(cot_ref[...], tot_ref[...])
    q_copy.wait()
    sends = []
    for z in range(steps):
        copies[z].wait()
        block = x_held[z]
        part = dot(block, q_held[...], FIRST).astype(BF)
        zh, zl = divmod(z, nzl)
        for yh in range(ny):
            for yl in range(nyl):
                row = (yh * nyl + yl) * own
                for q in range(nx):
                    out_held[z, yl * nx + q, yh * own : (yh + 1) * own, :] = part[
                        row : row + own, q * LANES : (q + 1) * LANES
                    ]
        target = out_ref.at[
            zl * nyl * nx : (zl + 1) * nyl * nx, zh * ny * own : (zh + 1) * ny * own, :
        ]
        send = pltpu.make_async_copy(out_held.at[z], target, out_sem.at[z])
        send.start()
        sends.append(send)
        gates = dot(signal, block).astype(BF)
        for k in range(wide // LANES):
            gate_held[z * (wide // LANES) + k] = gates[:, k * LANES : (k + 1) * LANES]
    target = out_ref.at[:, nz * ny * own : nz * ny * own + heads, :]
    send = pltpu.make_async_copy(gate_held, target, out_sem.at[steps])
    send.start()
    sends.append(send)
    for send in sends:
        send.wait()


def second_kernel(own, in_ref, out_ref):
    far, rows = out_ref.shape[:2]
    for k in range(far + 1):
        cut = slice(k * own, (k + 1) * own) if k < far else slice(far * own, in_ref.shape[1])
        summed = in_ref[0, cut].astype(F32)
        for i in range(1, in_ref.shape[0]):
            summed = summed + in_ref[i, cut].astype(F32)
        if k < far:
            out_ref[k, :own, :] = summed.astype(BF)
        else:
            for j in range(far):
                out_ref[j, own:, :] = summed.astype(BF)


def third_kernel(norming, in_ref, p_ref, gradient_ref, out_ref, gate_ref):
    own = p_ref.shape[0]
    summed = in_ref[0].astype(F32)
    for k in range(1, in_ref.shape[0]):
        summed = summed + in_ref[k].astype(F32)
    summed = summed * norming
    gate_ref[...] = summed[own:]
    gradient = summed[:own]
    gradient_ref[...] = gradient
    factor = p_ref[...]
    high, low = split_two(gradient)
    rank = dot(factor, high, FIRST) + dot(factor, low, FIRST)
    top = lax.broadcasted_iota(jnp.int32, (8, LANES), 0) < 4
    for g in range(out_ref.shape[0] // 2):
        value = rank[8 * g : 8 * g + 8]
        high = value.astype(BF).astype(F32)
        low = value - high
        out_ref[2 * g] = jnp.where(top, high, pltpu.roll(low, 4, 0)).astype(BF)
        out_ref[2 * g + 1] = jnp.where(top, pltpu.roll(high, 4, 0), low).astype(BF)


def rank_kernel(at_ref, in_ref, gates_ref, out_ref, held):
    summed = in_ref[0].astype(F32)
    for k in range(1, in_ref.shape[0]):
        summed = summed + in_ref[k].astype(F32)
    summed = summed + pltpu.roll(summed, 4, 0)
    gates = gates_ref[...]
    high = gates.astype(BF).astype(F32)
    low = gates - high
    held[0] = pltpu.roll(high, 4, 0)
    held[1] = high
    held[2] = pltpu.roll(low, 4, 0)
    held[3] = low
    top = lax.broadcasted_iota(jnp.int32, (8, LANES), 0) < 4
    piece = jnp.where(top, summed, held[lax.rem(at_ref[4], 4)]).astype(BF)
    for k in range(out_ref.shape[0]):
        out_ref[k] = piece


def fourth_kernel(
    sizes, at_ref, in_ref, moments_ref, p_ref, gradient_ref, out_ref, projected, direction, gates
):
    nzl, ny, nyl, nx, nc = sizes
    top = lax.broadcasted_iota(jnp.int32, (8, LANES), 0) < 4
    for g in range(in_ref.shape[0] // 2):
        even, odd = in_ref[2 * g].astype(F32), in_ref[2 * g + 1].astype(F32)
        projected[8 * g : 8 * g + 8, :] = jnp.where(top, even, pltpu.roll(odd, 4, 0))
    for zl in range(nzl):
        for yl in range(nyl):
            one, two, three, four = (
                in_ref[(zl * ny + yh) * nyl + yl].astype(F32) for yh in range(4)
            )
            gates[8 * (zl * nyl + yl) : 8 * (zl * nyl + yl) + 8, :] = jnp.where(
                top, pltpu.roll(one, 4, 0) + pltpu.roll(three, 4, 0), two + four
            )
    block = projected.shape[0] // nx
    squares = jnp.zeros((2, LANES), F32)
    for s in range(nx):
        where = pl.multiple_of(lax.rem(at_ref[0] + nx - s, nx) * block, block)
        p = projected[pl.ds(where, block), :]
        mean = BETA_ONE * moments_ref[s, :block] + (1.0 - BETA_ONE) * p
        square = BETA_TWO * moments_ref[s, block:] + (1.0 - BETA_TWO) * p * p
        d = mean / (jnp.sqrt(square) + EPSILON)
        direction[pl.ds(where, block), :] = d
        squares = squares + jnp.concatenate(
            [jnp.sum(d * d, axis=0, keepdims=True), jnp.sum(p * p, axis=0, keepdims=True)], axis=0
        )
    factor = p_ref[...]
    own = factor.shape[0]
    high, low = split_two(direction[...])
    lifted_direction = dot(factor, high) + dot(factor, low)
    high, low = split_two(projected[...])
    lifted_projected = dot(factor, high) + dot(factor, low) - gradient_ref[...]
    squares = jnp.concatenate([squares, jnp.zeros((6, LANES), F32)], axis=0)
    for x in range(nx):
        for c in range(nc):
            k = x * nc + c
            out_ref[k, :own] = lifted_direction
            out_ref[k, own : 2 * own] = lifted_projected
            out_ref[k, 2 * own : 2 * own + block] = projected[x * block : (x + 1) * block, :]
            out_ref[k, 2 * own + block : 2 * own + block + 8] = squares
            out_ref[k, 2 * own + block + 8 :] = gates[...]


def last_kernel(
    sizes,
    at_ref,
    in_ref,
    master_ref,
    mean_ref,
    square_ref,
    gate_mean_ref,
    gate_square_ref,
    update_ref,
    new_ref,
    copy_ref,
    mean_out,
    square_out,
    gate_update_ref,
    average_ref,
    energy_ref,
):
    nzl, nyl, nx, nc, own, block = sizes
    heads = gate_mean_ref.shape[0]
    after = 2 * own + block + 8
    squares = in_ref[0, 2 * own + block : after]
    for k in range(1, nx * nc):
        squares = squares + in_ref[k, 2 * own + block : after]
    direction_squares = jnp.sum(squares[0:1], axis=1, keepdims=True)
    projected_squares = jnp.sum(squares[1:2], axis=1, keepdims=True)
    balance = jnp.sqrt(direction_squares / (projected_squares + NORM_FLOOR))
    for x in range(nx):
        k = x * nc + at_ref[1]
        cut = slice(x * LANES, (x + 1) * LANES)
        update = in_ref[k, :own] - balance * in_ref[k, own : 2 * own]
        update_ref[:, cut] = update
        new = master_ref[:, cut] - STEP_RATE * update
        new_ref[:, cut] = new
        copy_ref[:, cut] = new.astype(BF)
        p = in_ref[k, 2 * own : 2 * own + block]
        mean_out[:, cut] = BETA_ONE * mean_ref[:, cut] + (1.0 - BETA_ONE) * p
        square_out[:, cut] = BETA_TWO * square_ref[:, cut] + (1.0 - BETA_TWO) * p * p
        for a in range(nzl):
            for b in range(nyl):
                start = ((a * nyl + b) * nx + x) * LANES
                place = slice(start, start + LANES)
                row = after + (a * nyl + b) * heads
                g = in_ref[k, row : row + heads]
                average = BETA_ONE * gate_mean_ref[:, place] + (1.0 - BETA_ONE) * g
                energy = BETA_TWO * gate_square_ref[:, place] + (1.0 - BETA_TWO) * g * g
                average_ref[:, place] = average
                energy_ref[:, place] = energy
                gate_update_ref[:, place] = average / (jnp.sqrt(energy) + EPSILON)


def near_memory(value):
    return pltpu.with_memory_space_constraint(value, pltpu.VMEM)


def per_device(
    attention_input,
    query_cotangent,
    gate_cotangent,
    gate_totals,
    projector,
    query_master,
    lowrank_mean,
    lowrank_square,
    gating_mean,
    gating_square,
):
    nz, ny, nzl, nyl, nx, nc = (lax.axis_size(a) for a in ("zh", "yh", "zl", "yl", "x", "c"))
    far, near = nz * ny, nzl * nyl * nx
    every = far * nzl * nyl
    tokens, width = attention_input.shape
    columns = query_cotangent.shape[1]
    heads = gate_cotangent.shape[0]
    own, rank = projector.shape
    block = rank // nx
    norming = 1.0 / (tokens * far * near) ** 0.5
    shape = jax.ShapeDtypeStruct
    at = jnp.stack([lax.axis_index(a) for a in ("x", "c", "zl", "yl", "yh")]).astype(jnp.int32)

    wide = ny * nyl * own
    first = pl.pallas_call(
        functools.partial(first_kernel, (nz, nzl, ny, nyl, nx, own)),
        out_shape=shape((near, far * own + heads, LANES), BF),
        in_specs=[ANY, ANY, VMEM, VMEM],
        out_specs=ANY,
        scratch_shapes=[
            pltpu.VMEM((nz * nzl, tokens, wide), BF),
            pltpu.VMEM((tokens, columns), BF),
            pltpu.VMEM((nz * nzl, nyl * nx, ny * own, LANES), BF),
            pltpu.VMEM((near, heads, LANES), BF),
            pltpu.SemaphoreType.DMA((nz * nzl,)),
            pltpu.SemaphoreType.DMA,
            pltpu.SemaphoreType.DMA((nz * nzl + 1,)),
        ],
        name="first",
    )(attention_input, query_cotangent, gate_cotangent, gate_totals)
    first = swap(first, NEAR)
    mine = jnp.concatenate(
        [lowrank_mean.reshape(block, nx, LANES), lowrank_square.reshape(block, nx, LANES)]
    ).transpose(1, 0, 2)
    place = lax.axis_index("x")
    pieces = [lax.dynamic_index_in_dim(mine, lax.rem(place + s, nx), 0, False) for s in range(nx)]
    moments = jnp.stack([pieces[0], *(shifted(pieces[s], "x", s) for s in range(1, nx))])
    first, moments = lax.optimization_barrier((first, moments))

    second = pl.pallas_call(
        functools.partial(second_kernel, own),
        out_shape=pltpu.VMEM((far, own + heads, LANES), BF),
        in_specs=[VMEM],
        out_specs=VMEM,
        name="second",
    )(near_memory(first))
    second = swap(second, FAR)

    gradient, third, gates = pl.pallas_call(
        functools.partial(third_kernel, norming),
        out_shape=(
            pltpu.VMEM((own, LANES), F32),
            pltpu.VMEM((every, 8, LANES), BF),
            pltpu.VMEM((heads, LANES), F32),
        ),
        in_specs=[VMEM, VMEM],
        out_specs=(VMEM, VMEM, VMEM),
        name="third",
    )(near_memory(second), projector)
    third = swap(third, FS)

    ranked = pl.pallas_call(
        rank_kernel,
        out_shape=pltpu.VMEM((every, 8, LANES), BF),
        in_specs=[SMEM, VMEM, VMEM],
        out_specs=VMEM,
        scratch_shapes=[pltpu.VMEM((4, heads, LANES), F32)],
        name="ranked",
    )(at, near_memory(third), near_memory(gates))
    ranked = swap(ranked, FS)

    fourth = pl.pallas_call(
        functools.partial(fourth_kernel, (nzl, ny, nyl, nx, nc)),
        out_shape=pltpu.VMEM((nx * nc, 2 * own + block + 8 + nzl * nyl * heads, LANES), F32),
        in_specs=[SMEM, VMEM, VMEM, VMEM, VMEM],
        out_specs=VMEM,
        scratch_shapes=[
            pltpu.VMEM((rank, LANES), F32),
            pltpu.VMEM((rank, LANES), F32),
            pltpu.VMEM((nzl * nyl * heads, LANES), F32),
        ],
        name="fourth",
    )(at, near_memory(ranked), near_memory(moments), projector, near_memory(gradient))
    fourth = swap(fourth, PAIR)

    return pl.pallas_call(
        functools.partial(last_kernel, (nzl, nyl, nx, nc, own, block)),
        out_shape=(
            shape((own, columns), F32),
            shape((own, columns), F32),
            shape((own, columns), BF),
            shape((block, columns), F32),
            shape((block, columns), F32),
            shape((heads, width), F32),
            shape((heads, width), F32),
            shape((heads, width), F32),
        ),
        in_specs=[SMEM, *[VMEM] * 6],
        out_specs=(VMEM,) * 8,
        name="last",
    )(at, near_memory(fourth), query_master, lowrank_mean, lowrank_square, gating_mean, gating_square)


def solution(mesh):
    split = Mesh(
        mesh.devices.reshape(4, 2, 4, 2, mesh.shape["rep"], mesh.shape["tp"]),
        ("zh", "zl", "yh", "yl", "x", "c"),
    )
    in_specs = (
        P((*FS, "x"), None),
        P((*FS, "x"), "c"),
        P("c", (*FS, "x")),
        P("c", (*FS, "x")),
        P(FS, None),
        P(FS, "c"),
        P("x", "c"),
        P("x", "c"),
        P("c", None),
        P("c", None),
    )
    out_specs = (
        P(FS, "c"),
        P(FS, "c"),
        P(FS, "c"),
        P("x", "c"),
        P("x", "c"),
        P("c", None),
        P("c", None),
        P("c", None),
    )
    return jax.shard_map(
        per_device, mesh=split, in_specs=in_specs, out_specs=out_specs, check_vma=False
    )
```

```python
import functools

import jax
import jax.numpy as jnp
from jax import lax
from jax.experimental import pallas as pl
from jax.experimental.pallas import tpu as pltpu
from jax.sharding import Mesh
from jax.sharding import PartitionSpec as P

FS = ("zh", "zl", "yh", "yl")
NEAR = ("zl", "yl", "x")
FAR = ("zh", "yh")
CLOSE = ("zl", "yl")
LAST = ("zl", "yl", "x", "c")

BETA_ONE = 0.9
BETA_TWO = 0.95
STEP_RATE = 0.01
EPSILON = 1e-08
NORM_FLOOR = 1e-06
BF = jnp.bfloat16
F32 = jnp.float32
FIRST = (((0,), (0,)), ((), ()))
LANES = 128
PART = 32
VMEM = pl.BlockSpec(memory_space=pltpu.VMEM)
ANY = pl.BlockSpec(memory_space=pltpu.HBM)
SMEM = pl.BlockSpec(memory_space=pltpu.SMEM)


def swap(pieces, axes):
    return lax.all_to_all(pieces, axes, 0, 0, tiled=True)


def shifted(value, axis, step):
    length = lax.axis_size(axis)
    return lax.ppermute(value, axis, [(i, (i + step) % length) for i in range(length)])


def split_two(v):
    high = v.astype(BF)
    return high, (v - high.astype(F32)).astype(BF)


def dot(a, b, dims=(((1,), (0,)), ((), ()))):
    return lax.dot_general(a, b, dims, preferred_element_type=F32)


def one_less_exp(v):
    series = 1.0 + v * 0.125
    for k in range(7, 1, -1):
        series = 1.0 + v * (1.0 / k) * series
    return jnp.where(v > -0.3, -v * series, 1.0 - jnp.exp(v))


def gate_signals(cot, totals):
    heads, tokens = cot.shape
    later = lax.broadcasted_iota(jnp.int32, (tokens, tokens), 0) >= lax.broadcasted_iota(
        jnp.int32, (tokens, tokens), 1
    )
    later = jnp.where(later, 1.0, 0.0).astype(BF)
    one = cot.astype(BF).astype(F32)
    rest = cot - one
    two = rest.astype(BF).astype(F32)
    parts = jnp.concatenate([one, two, rest - two, jnp.zeros_like(one)], axis=0).astype(BF)
    trailing = dot(parts, later)
    trailing = trailing[2 * heads : 3 * heads] + trailing[heads : 2 * heads] + trailing[:heads]
    lane = lax.broadcasted_iota(jnp.int32, totals.shape, 1)
    gate = totals - jnp.where(lane == 0, 0.0, pltpu.roll(totals, 1, 1))
    return (trailing * one_less_exp(gate)).astype(BF)


def lane_blocks(shape):
    return lax.broadcasted_iota(jnp.int32, shape, len(shape) - 1) // PART


def turn(value, blocks):
    blocks = blocks % (LANES // PART)
    return pltpu.roll(value, blocks * PART, 1) if blocks else value


def turn_by(value, blocks):
    count = LANES // PART
    return pltpu.roll(value, lax.rem(blocks + 2 * count, count) * PART, 1)


def first_kernel(
    sizes, x_ref, q_ref, cot_ref, tot_ref, out_ref, x_held, q_held, out_held, gate_held, x_sem, q_sem, out_sem
):
    nz, nzl, ny, nyl, nx, own = sizes
    wide = x_held.shape[2]
    heads = gate_held.shape[1]
    copies = []
    q_copy = pltpu.make_async_copy(q_ref, q_held, q_sem)
    q_copy.start()
    for z in range(nz):
        copy = pltpu.make_async_copy(x_ref.at[:, z * wide : (z + 1) * wide], x_held.at[z], x_sem.at[z])
        copy.start()
        copies.append(copy)
    signal = gate_signals(cot_ref[...], tot_ref[...])
    q_copy.wait()
    lane = lane_blocks((own, LANES))
    sends = []
    for z in range(nz):
        copies[z].wait()
        block = x_held[z]
        part = dot(block, q_held[...], FIRST)
        for yh in range(ny):
            to = slice(yh * own, (yh + 1) * own)
            for q in range(nx):
                turned = []
                for j in range(nzl * nyl):
                    row = ((j // nyl * ny + yh) * nyl + j % nyl) * own
                    turned.append(turn(part[row : row + own, q * LANES : (q + 1) * LANES], j))
                for t in range(nzl * nyl):
                    piece = turned[0]
                    for j in range(1, nzl * nyl):
                        piece = jnp.where(lane == (t + j) % (nzl * nyl), turned[j], piece)
                    out_held[z, t * nx + q, to, :] = piece.astype(BF)
        target = out_ref.at[:, z * ny * own : (z + 1) * ny * own, :]
        send = pltpu.make_async_copy(out_held.at[z], target, out_sem.at[z])
        send.start()
        sends.append(send)
        gates = dot(signal, block).astype(BF)
        for k in range(wide // LANES):
            gate_held[z * (wide // LANES) + k] = gates[:, k * LANES : (k + 1) * LANES]
    target = out_ref.at[:, nz * ny * own : nz * ny * own + heads, :]
    send = pltpu.make_async_copy(gate_held, target, out_sem.at[nz])
    send.start()
    sends.append(send)
    for send in sends:
        send.wait()


def second_kernel(own, in_ref, out_ref):
    far, rows = out_ref.shape[:2]
    for k in range(far + 1):
        cut = slice(k * own, (k + 1) * own) if k < far else slice(far * own, in_ref.shape[1])
        summed = in_ref[0, cut].astype(F32)
        for i in range(1, in_ref.shape[0]):
            summed = summed + in_ref[i, cut].astype(F32)
        if k < far:
            out_ref[k, :own, :] = summed.astype(BF)
        else:
            for j in range(far):
                out_ref[j, own:, :] = summed.astype(BF)


def four_factors(p_ref, t):
    return jnp.concatenate([p_ref[j ^ t] for j in range(p_ref.shape[0])], axis=0)


def two_halves(value, out_ref):
    top = lax.broadcasted_iota(jnp.int32, (8, LANES), 0) < 4
    for g in range(out_ref.shape[0] // 2):
        rows = value[8 * g : 8 * g + 8]
        high = rows.astype(BF).astype(F32)
        low = rows - high
        out_ref[2 * g] = jnp.where(top, high, pltpu.roll(low, 4, 0)).astype(BF)
        out_ref[2 * g + 1] = jnp.where(top, pltpu.roll(high, 4, 0), low).astype(BF)


def third_kernel(norming, at_ref, in_ref, p_ref, gradient_ref, out_ref, gate_ref):
    own = p_ref.shape[1]
    count = p_ref.shape[0]
    summed = in_ref[0].astype(F32)
    for k in range(1, in_ref.shape[0]):
        summed = summed + in_ref[k].astype(F32)
    summed = summed * norming
    gate_ref[...] = summed[own:]
    gradient = turn_by(summed[:own], -at_ref[2])
    gradient_ref[...] = gradient
    factor = four_factors(p_ref, at_ref[2])
    high, low = split_two(jnp.concatenate([turn(gradient, -j) for j in range(count)], axis=0))
    rank = dot(factor, high, FIRST) + dot(factor, low, FIRST)
    block = rank.shape[0] // count
    lane = lane_blocks((block, LANES))
    packed = rank[:block]
    for u in range(1, count):
        packed = jnp.where(lane == u, turn(rank[u * block : (u + 1) * block], u), packed)
    two_halves(packed, out_ref)


def rank_kernel(in_ref, out_ref):
    summed = in_ref[0].astype(F32)
    for k in range(1, in_ref.shape[0]):
        summed = summed + in_ref[k].astype(F32)
    summed = summed + pltpu.roll(summed, 4, 0)
    high = summed.astype(BF).astype(F32)
    top = lax.broadcasted_iota(jnp.int32, (8, LANES), 0) < 4
    piece = jnp.where(top, high, summed - high).astype(BF)
    for k in range(out_ref.shape[0]):
        out_ref[k] = piece


def fourth_kernel(sizes, at_ref, in_ref, moments_ref, p_ref, gradient_ref, gates_ref, out_ref):
    nx, nc = sizes
    count, own = p_ref.shape[:2]
    top = lax.broadcasted_iota(jnp.int32, (8, LANES), 0) < 4
    rows = []
    for g in range(in_ref.shape[0] // 2):
        even, odd = in_ref[2 * g].astype(F32), in_ref[2 * g + 1].astype(F32)
        even = even + pltpu.roll(even, 4, 0)
        odd = odd + pltpu.roll(odd, 4, 0)
        rows.append(jnp.where(top, even, odd))
    projected = jnp.concatenate(rows, axis=0)
    block = projected.shape[0]
    lane = lane_blocks((2 * block, LANES))
    moments = moments_ref[0]
    for s in range(nx):
        u = lax.rem(at_ref[0] + nx - s, nx)
        moments = jnp.where(lane == u, turn_by(moments_ref[s], u - at_ref[2]), moments)
    mean = BETA_ONE * moments[:block] + (1.0 - BETA_ONE) * projected
    square = BETA_TWO * moments[block:] + (1.0 - BETA_TWO) * projected * projected
    direction = mean / (jnp.sqrt(square) + EPSILON)
    sums = [
        jnp.sum(direction * direction, axis=0, keepdims=True),
        jnp.sum(projected * projected, axis=0, keepdims=True),
    ]
    sums = jnp.concatenate(sums, axis=0)
    one = sums.astype(BF).astype(F32)
    two = (sums - one).astype(BF).astype(F32)
    sums = jnp.concatenate([one, two, sums - one - two, jnp.zeros((2, LANES), F32)], axis=0).astype(BF)
    lane = lane_blocks((block, LANES))
    both = [jnp.where(lane == 0, turn(direction, -u), turn(projected, 1 - u)) for u in range(count)]
    high, low = split_two(jnp.concatenate(both, axis=0))
    factor = four_factors(p_ref, at_ref[2])
    lifted = dot(factor, high) + dot(factor, low)
    lane = lane_blocks((own, LANES))
    gates = gates_ref[...].astype(BF)
    gradient = gradient_ref[...]
    for x in range(nx):
        tail = jnp.where(lane == 2, turn(projected[:own], 2 - x), turn(projected[own:], 3 - x))
        for j in range(count):
            piece = lifted[j * own : (j + 1) * own]
            piece = jnp.where(lane == 1, piece - turn(gradient, 1 - j), piece)
            piece = jnp.where(lane < 2, piece, tail).astype(BF)
            for c in range(nc):
                k = (j * nx + x) * nc + c
                out_ref[k, :own] = piece
                out_ref[k, own : own + 8] = gates
                out_ref[k, own + 8 :] = sums


def last_kernel(
    sizes,
    at_ref,
    in_ref,
    master_ref,
    mean_ref,
    square_ref,
    gate_mean_ref,
    gate_square_ref,
    update_ref,
    new_ref,
    copy_ref,
    mean_out,
    square_out,
    gate_update_ref,
    average_ref,
    energy_ref,
):
    count, nx, nc = sizes
    own = master_ref.shape[0]
    sums = in_ref[0, own + 8 :].astype(F32)
    for k in range(1, in_ref.shape[0]):
        sums = sums + in_ref[k, own + 8 :].astype(F32)
    sums = sums[0:2] + sums[2:4] + sums[4:6]
    direction_squares = jnp.sum(sums[0:1], axis=1, keepdims=True)
    projected_squares = jnp.sum(sums[1:2], axis=1, keepdims=True)
    balance = jnp.sqrt(direction_squares / (projected_squares + NORM_FLOOR))
    lane = lane_blocks((own, LANES))
    for x in range(nx):
        update, upper, lower = None, None, None
        for t in range(count):
            k = (t * nx + x) * nc + at_ref[1]
            piece = in_ref[k, :own].astype(F32)
            term = turn(piece - balance * turn(piece, -1), t)
            above, below = turn(piece, t - 2), turn(piece, t - 3)
            update = term if t == 0 else jnp.where(lane == t, term, update)
            upper = above if t == 0 else jnp.where(lane == t, above, upper)
            lower = below if t == 0 else jnp.where(lane == t, below, lower)
            g = in_ref[k, own : own + 8].astype(F32)
            place = slice((t * nx + x) * LANES, (t * nx + x + 1) * LANES)
            average = BETA_ONE * gate_mean_ref[:, place] + (1.0 - BETA_ONE) * g
            energy = BETA_TWO * gate_square_ref[:, place] + (1.0 - BETA_TWO) * g * g
            average_ref[:, place] = average
            energy_ref[:, place] = energy
            gate_update_ref[:, place] = average / (jnp.sqrt(energy) + EPSILON)
        cut = slice(x * LANES, (x + 1) * LANES)
        update_ref[:, cut] = update
        new = master_ref[:, cut] - STEP_RATE * update
        new_ref[:, cut] = new
        copy_ref[:, cut] = new.astype(BF)
        p = jnp.concatenate([upper, lower], axis=0)
        mean_out[:, cut] = BETA_ONE * mean_ref[:, cut] + (1.0 - BETA_ONE) * p
        square_out[:, cut] = BETA_TWO * square_ref[:, cut] + (1.0 - BETA_TWO) * p * p


def near_memory(value):
    return pltpu.with_memory_space_constraint(value, pltpu.VMEM)


def per_device(
    attention_input,
    query_cotangent,
    gate_cotangent,
    gate_totals,
    projector,
    query_master,
    lowrank_mean,
    lowrank_square,
    gating_mean,
    gating_square,
):
    nz, ny, nzl, nyl, nx, nc = (lax.axis_size(a) for a in ("zh", "yh", "zl", "yl", "x", "c"))
    far, near = nz * ny, nzl * nyl * nx
    count = nzl * nyl
    tokens, width = attention_input.shape
    columns = query_cotangent.shape[1]
    heads = gate_cotangent.shape[0]
    own, rank = projector.shape
    block = rank // nx
    norming = 1.0 / (tokens * far * near) ** 0.5
    shape = jax.ShapeDtypeStruct
    at = jnp.stack([lax.axis_index(a) for a in ("x", "c", CLOSE)]).astype(jnp.int32)

    wide = nzl * ny * nyl * own
    first = pl.pallas_call(
        functools.partial(first_kernel, (nz, nzl, ny, nyl, nx, own)),
        out_shape=shape((near, far * own + heads, LANES), BF),
        in_specs=[ANY, ANY, VMEM, VMEM],
        out_specs=ANY,
        scratch_shapes=[
            pltpu.VMEM((nz, tokens, wide), BF),
            pltpu.VMEM((tokens, columns), BF),
            pltpu.VMEM((nz, near, ny * own, LANES), BF),
            pltpu.VMEM((near, heads, LANES), BF),
            pltpu.SemaphoreType.DMA((nz,)),
            pltpu.SemaphoreType.DMA,
            pltpu.SemaphoreType.DMA((nz + 1,)),
        ],
        name="first",
    )(attention_input, query_cotangent, gate_cotangent, gate_totals)
    first = swap(first, NEAR)
    mine = jnp.concatenate(
        [lowrank_mean.reshape(block, nx, LANES), lowrank_square.reshape(block, nx, LANES)]
    ).transpose(1, 0, 2)
    place = lax.axis_index("x")
    pieces = [lax.dynamic_index_in_dim(mine, lax.rem(place + s, nx), 0, False) for s in range(nx)]
    moments = jnp.stack([pieces[0], *(shifted(pieces[s], "x", s) for s in range(1, nx))])
    neighbours = [lax.ppermute(projector, CLOSE, [(i, i ^ e) for i in range(count)]) for e in range(1, count)]
    factors = jnp.stack([projector, *neighbours])
    first, moments, factors = lax.optimization_barrier((first, moments, factors))

    second = pl.pallas_call(
        functools.partial(second_kernel, own),
        out_shape=pltpu.VMEM((far, own + heads, LANES), BF),
        in_specs=[VMEM],
        out_specs=VMEM,
        name="second",
    )(near_memory(first))
    second = swap(second, FAR)

    gradient, third, gates = pl.pallas_call(
        functools.partial(third_kernel, norming),
        out_shape=(
            pltpu.VMEM((own, LANES), F32),
            pltpu.VMEM((far, 8, LANES), BF),
            pltpu.VMEM((heads, LANES), F32),
        ),
        in_specs=[SMEM, VMEM, VMEM],
        out_specs=(VMEM, VMEM, VMEM),
        name="third",
    )(at, near_memory(second), near_memory(factors))
    third = swap(third, FAR)

    ranked = pl.pallas_call(
        rank_kernel,
        out_shape=pltpu.VMEM((far, 8, LANES), BF),
        in_specs=[VMEM],
        out_specs=VMEM,
        name="ranked",
    )(near_memory(third))
    ranked = swap(ranked, FAR)

    fourth = pl.pallas_call(
        functools.partial(fourth_kernel, (nx, nc)),
        out_shape=pltpu.VMEM((count * nx * nc, own + 16, LANES), BF),
        in_specs=[SMEM, VMEM, VMEM, VMEM, VMEM, VMEM],
        out_specs=VMEM,
        name="fourth",
    )(
        at,
        near_memory(ranked),
        near_memory(moments),
        near_memory(factors),
        near_memory(gradient),
        near_memory(gates),
    )
    fourth = swap(fourth, LAST)

    return pl.pallas_call(
        functools.partial(last_kernel, (count, nx, nc)),
        out_shape=(
            shape((own, columns), F32),
            shape((own, columns), F32),
            shape((own, columns), BF),
            shape((block, columns), F32),
            shape((block, columns), F32),
            shape((heads, width), F32),
            shape((heads, width), F32),
            shape((heads, width), F32),
        ),
        in_specs=[SMEM, *[VMEM] * 6],
        out_specs=(VMEM,) * 8,
        name="last",
    )(at, near_memory(fourth), query_master, lowrank_mean, lowrank_square, gating_mean, gating_square)


def solution(mesh):
    split = Mesh(
        mesh.devices.reshape(4, 2, 4, 2, mesh.shape["rep"], mesh.shape["tp"]),
        ("zh", "zl", "yh", "yl", "x", "c"),
    )
    in_specs = (
        P((*FS, "x"), None),
        P((*FS, "x"), "c"),
        P("c", (*FS, "x")),
        P("c", (*FS, "x")),
        P(FS, None),
        P(FS, "c"),
        P("x", "c"),
        P("x", "c"),
        P("c", None),
        P("c", None),
    )
    out_specs = (
        P(FS, "c"),
        P(FS, "c"),
        P(FS, "c"),
        P("x", "c"),
        P("x", "c"),
        P("c", None),
        P("c", None),
        P("c", None),
    )
    return jax.shard_map(
        per_device, mesh=split, in_specs=in_specs, out_specs=out_specs, check_vma=False
    )
```

```python
import functools

import jax
import jax.numpy as jnp
from jax import lax
from jax.experimental import pallas as pl
from jax.experimental.pallas import tpu as pltpu
from jax.sharding import Mesh
from jax.sharding import PartitionSpec as P

FS = ("zh", "zl", "yh", "yl")
NEAR = ("zl", "yl", "x")
FAR = ("zh", "yh")
CLOSE = ("zl", "yl")
LAST = ("zl", "yl", "x", "c")


BETA_ONE = 0.9
BETA_TWO = 0.95
STEP_RATE = 0.01
EPSILON = 1e-08
NORM_FLOOR = 1e-06
BF = jnp.bfloat16
F32 = jnp.float32
FIRST = (((0,), (0,)), ((), ()))
LANES = 128
PART = 32
VMEM = pl.BlockSpec(memory_space=pltpu.VMEM)
ANY = pl.BlockSpec(memory_space=pltpu.HBM)
SMEM = pl.BlockSpec(memory_space=pltpu.SMEM)


def swap(pieces, axes):
    return lax.all_to_all(pieces, axes, 0, 0, tiled=True)


def shifted(value, axis, step):
    length = lax.axis_size(axis)
    return lax.ppermute(value, axis, [(i, (i + step) % length) for i in range(length)])


def split_two(v):
    high = v.astype(BF)
    return high, (v - high.astype(F32)).astype(BF)


def dot(a, b, dims=(((1,), (0,)), ((), ()))):
    return lax.dot_general(a, b, dims, preferred_element_type=F32)


def one_less_exp(v):
    series = 1.0 + v * 0.125
    for k in range(7, 1, -1):
        series = 1.0 + v * (1.0 / k) * series
    return jnp.where(v > -0.3, -v * series, 1.0 - jnp.exp(v))


def gate_signals(cot, totals):
    heads, tokens = cot.shape
    later = lax.broadcasted_iota(jnp.int32, (tokens, tokens), 0) >= lax.broadcasted_iota(
        jnp.int32, (tokens, tokens), 1
    )
    later = jnp.where(later, 1.0, 0.0).astype(BF)
    one = cot.astype(BF).astype(F32)
    rest = cot - one
    two = rest.astype(BF).astype(F32)
    parts = jnp.concatenate([one, two, rest - two, jnp.zeros_like(one)], axis=0).astype(BF)
    trailing = dot(parts, later)
    trailing = trailing[2 * heads : 3 * heads] + trailing[heads : 2 * heads] + trailing[:heads]
    lane = lax.broadcasted_iota(jnp.int32, totals.shape, 1)
    gate = totals - jnp.where(lane == 0, 0.0, pltpu.roll(totals, 1, 1))
    return (trailing * one_less_exp(gate)).astype(BF)


def lane_blocks(shape):
    return lax.broadcasted_iota(jnp.int32, shape, len(shape) - 1) // PART


def turn(value, blocks):
    blocks = blocks % (LANES // PART)
    return pltpu.roll(value, blocks * PART, 1) if blocks else value


def turn_by(value, blocks):
    count = LANES // PART
    return pltpu.roll(value, lax.rem(blocks + 2 * count, count) * PART, 1)


def first_kernel(
    sizes, x_ref, q_ref, cot_ref, tot_ref, out_ref, x_held, q_held, out_held, gate_held, x_sem, q_sem, out_sem
):
    nz, nzl, ny, nyl, nx, own = sizes
    wide = x_held.shape[2]
    heads = gate_held.shape[1]
    copies = []
    q_copy = pltpu.make_async_copy(q_ref, q_held, q_sem)
    q_copy.start()
    for z in range(nz):
        copy = pltpu.make_async_copy(x_ref.at[:, z * wide : (z + 1) * wide], x_held.at[z], x_sem.at[z])
        copy.start()
        copies.append(copy)
    signal = gate_signals(cot_ref[...], tot_ref[...])
    q_copy.wait()
    lane = lane_blocks((own, LANES))
    sends = []
    for z in range(nz):
        copies[z].wait()
        block = x_held[z]
        part = dot(block, q_held[...], FIRST)
        for yh in range(ny):
            to = slice(yh * own, (yh + 1) * own)
            for q in range(nx):
                turned = []
                for j in range(nzl * nyl):
                    row = ((j // nyl * ny + yh) * nyl + j % nyl) * own
                    turned.append(turn(part[row : row + own, q * LANES : (q + 1) * LANES], j))
                for t in range(nzl * nyl):
                    piece = turned[0]
                    for j in range(1, nzl * nyl):
                        piece = jnp.where(lane == (t + j) % (nzl * nyl), turned[j], piece)
                    out_held[z, t * nx + q, to, :] = piece.astype(BF)
        target = out_ref.at[:, z * ny * own : (z + 1) * ny * own, :]
        send = pltpu.make_async_copy(out_held.at[z], target, out_sem.at[z])
        send.start()
        sends.append(send)
        gates = dot(signal, block).astype(BF)
        for k in range(wide // LANES):
            gate_held[z * (wide // LANES) + k] = gates[:, k * LANES : (k + 1) * LANES]
    target = out_ref.at[:, nz * ny * own : nz * ny * own + heads, :]
    send = pltpu.make_async_copy(gate_held, target, out_sem.at[nz])
    send.start()
    sends.append(send)
    for send in sends:
        send.wait()


def second_kernel(own, in_ref, out_ref):
    far, rows = out_ref.shape[:2]
    for k in range(far + 1):
        cut = slice(k * own, (k + 1) * own) if k < far else slice(far * own, in_ref.shape[1])
        summed = in_ref[0, cut].astype(F32)
        for i in range(1, in_ref.shape[0]):
            summed = summed + in_ref[i, cut].astype(F32)
        if k < far:
            out_ref[k, :own, :] = summed.astype(BF)
        else:
            for j in range(far):
                out_ref[j, own:, :] = summed.astype(BF)


def four_factors(p_ref, t):
    return jnp.concatenate([p_ref[j ^ t] for j in range(p_ref.shape[0])], axis=0)


def third_kernel(norming, at_ref, in_ref, p_ref, gradient_ref, out_ref, gate_ref):
    own = p_ref.shape[1]
    count = p_ref.shape[0]
    summed = in_ref[0].astype(F32)
    for k in range(1, in_ref.shape[0]):
        summed = summed + in_ref[k].astype(F32)
    summed = summed * norming
    gate_ref[...] = summed[own:]
    gradient = turn_by(summed[:own], -at_ref[2])
    gradient_ref[...] = gradient
    factor = four_factors(p_ref, at_ref[2])
    high, low = split_two(jnp.concatenate([turn(gradient, -j) for j in range(count)], axis=0))
    rank = dot(factor, high, FIRST) + dot(factor, low, FIRST)
    block = rank.shape[0] // count
    lane = lane_blocks((block, LANES))
    packed = rank[:block]
    for u in range(1, count):
        packed = jnp.where(lane == u, turn(rank[u * block : (u + 1) * block], u), packed)
    packed = packed.astype(BF)
    for k in range(out_ref.shape[0]):
        out_ref[k] = packed


def moment_kernel(at_ref, mean_ref, square_ref, out_ref):
    own = out_ref.shape[1]
    lane = lane_blocks((own, LANES))
    count = out_ref.shape[0]
    for s in range(count):
        cut = pl.ds(pl.multiple_of(lax.rem(at_ref[0] + s, count) * LANES, LANES), LANES)
        mean, square = mean_ref[:, cut], square_ref[:, cut]
        piece = None
        for k, rows in enumerate((mean[:own], mean[own:], square[:own], square[own:])):
            rows = turn_by(rows, k - at_ref[2])
            piece = rows if k == 0 else jnp.where(lane == k, rows, piece)
        out_ref[s] = piece


def fourth_kernel(sizes, at_ref, in_ref, moments_ref, p_ref, gradient_ref, gates_ref, out_ref):
    nx, nc = sizes
    count, own = p_ref.shape[:2]
    projected = in_ref[0].astype(F32)
    for k in range(1, in_ref.shape[0]):
        projected = projected + in_ref[k].astype(F32)
    block = projected.shape[0]
    lane = lane_blocks((own, LANES))
    moments = [moments_ref[0]] * 4
    for s in range(nx):
        u = lax.rem(at_ref[0] + nx - s, nx)
        piece = moments_ref[s]
        moments = [jnp.where(lane == u, turn_by(piece, u - k), moments[k]) for k in range(4)]
    mean = jnp.concatenate(moments[:2], axis=0)
    square = jnp.concatenate(moments[2:], axis=0)
    mean = BETA_ONE * mean + (1.0 - BETA_ONE) * projected
    square = BETA_TWO * square + (1.0 - BETA_TWO) * projected * projected
    direction = mean / (jnp.sqrt(square) + EPSILON)
    sums = [
        jnp.sum(direction * direction, axis=0, keepdims=True),
        jnp.sum(projected * projected, axis=0, keepdims=True),
    ]
    sums = jnp.concatenate(sums, axis=0)
    one = sums.astype(BF).astype(F32)
    two = (sums - one).astype(BF).astype(F32)
    sums = jnp.concatenate([one, two, sums - one - two, jnp.zeros((2, LANES), F32)], axis=0).astype(BF)
    lane = lane_blocks((block, LANES))
    both = [jnp.where(lane == 0, turn(direction, -u), turn(projected, 1 - u)) for u in range(count)]
    high, low = split_two(jnp.concatenate(both, axis=0))
    factor = four_factors(p_ref, at_ref[2])
    lifted = dot(factor, high) + dot(factor, low)
    lane = lane_blocks((own, LANES))
    gates = gates_ref[...].astype(BF)
    gradient = gradient_ref[...]
    for x in range(nx):
        tail = jnp.where(lane == 2, turn(projected[:own], 2 - x), turn(projected[own:], 3 - x))
        for j in range(count):
            piece = lifted[j * own : (j + 1) * own]
            piece = jnp.where(lane == 1, piece - turn(gradient, 1 - j), piece)
            piece = jnp.where(lane < 2, piece, tail).astype(BF)
            for c in range(nc):
                k = (j * nx + x) * nc + c
                out_ref[k, :own] = piece
                out_ref[k, own : own + 8] = gates
                out_ref[k, own + 8 :] = sums


def last_kernel(
    sizes,
    at_ref,
    in_ref,
    master_ref,
    mean_ref,
    square_ref,
    gate_mean_ref,
    gate_square_ref,
    update_ref,
    new_ref,
    copy_ref,
    mean_out,
    square_out,
    gate_update_ref,
    average_ref,
    energy_ref,
):
    count, nx, nc = sizes
    own = master_ref.shape[0]
    sums = in_ref[0, own + 8 :].astype(F32)
    for k in range(1, in_ref.shape[0]):
        sums = sums + in_ref[k, own + 8 :].astype(F32)
    sums = sums[0:2] + sums[2:4] + sums[4:6]
    direction_squares = jnp.sum(sums[0:1], axis=1, keepdims=True)
    projected_squares = jnp.sum(sums[1:2], axis=1, keepdims=True)
    balance = jnp.sqrt(direction_squares / (projected_squares + NORM_FLOOR))
    lane = lane_blocks((own, LANES))
    for x in range(nx):
        update, upper, lower = None, None, None
        for t in range(count):
            k = (t * nx + x) * nc + at_ref[1]
            piece = in_ref[k, :own].astype(F32)
            term = turn(piece - balance * turn(piece, -1), t)
            above, below = turn(piece, t - 2), turn(piece, t - 3)
            update = term if t == 0 else jnp.where(lane == t, term, update)
            upper = above if t == 0 else jnp.where(lane == t, above, upper)
            lower = below if t == 0 else jnp.where(lane == t, below, lower)
            g = in_ref[k, own : own + 8].astype(F32)
            place = slice((t * nx + x) * LANES, (t * nx + x + 1) * LANES)
            average = BETA_ONE * gate_mean_ref[:, place] + (1.0 - BETA_ONE) * g
            energy = BETA_TWO * gate_square_ref[:, place] + (1.0 - BETA_TWO) * g * g
            average_ref[:, place] = average
            energy_ref[:, place] = energy
            gate_update_ref[:, place] = average / (jnp.sqrt(energy) + EPSILON)
        cut = slice(x * LANES, (x + 1) * LANES)
        update_ref[:, cut] = update
        new = master_ref[:, cut] - STEP_RATE * update
        new_ref[:, cut] = new
        copy_ref[:, cut] = new.astype(BF)
        p = jnp.concatenate([upper, lower], axis=0)
        mean_out[:, cut] = BETA_ONE * mean_ref[:, cut] + (1.0 - BETA_ONE) * p
        square_out[:, cut] = BETA_TWO * square_ref[:, cut] + (1.0 - BETA_TWO) * p * p


def near_memory(value):
    return pltpu.with_memory_space_constraint(value, pltpu.VMEM)


def per_device(
    attention_input,
    query_cotangent,
    gate_cotangent,
    gate_totals,
    projector,
    query_master,
    lowrank_mean,
    lowrank_square,
    gating_mean,
    gating_square,
):
    nz, ny, nzl, nyl, nx, nc = (lax.axis_size(a) for a in ("zh", "yh", "zl", "yl", "x", "c"))
    far, near = nz * ny, nzl * nyl * nx
    count = nzl * nyl
    tokens, width = attention_input.shape
    columns = query_cotangent.shape[1]
    heads = gate_cotangent.shape[0]
    own, rank = projector.shape
    block = rank // nx
    norming = 1.0 / (tokens * far * near) ** 0.5
    shape = jax.ShapeDtypeStruct
    at = jnp.stack([lax.axis_index(a) for a in ("x", "c", CLOSE)]).astype(jnp.int32)

    wide = nzl * ny * nyl * own
    first = pl.pallas_call(
        functools.partial(first_kernel, (nz, nzl, ny, nyl, nx, own)),
        out_shape=shape((near, far * own + heads, LANES), BF),
        in_specs=[ANY, ANY, VMEM, VMEM],
        out_specs=ANY,
        scratch_shapes=[
            pltpu.VMEM((nz, tokens, wide), BF),
            pltpu.VMEM((tokens, columns), BF),
            pltpu.VMEM((nz, near, ny * own, LANES), BF),
            pltpu.VMEM((near, heads, LANES), BF),
            pltpu.SemaphoreType.DMA((nz,)),
            pltpu.SemaphoreType.DMA,
            pltpu.SemaphoreType.DMA((nz + 1,)),
        ],
        name="first",
    )(attention_input, query_cotangent, gate_cotangent, gate_totals)
    first = swap(first, NEAR)
    pieces = pl.pallas_call(
        moment_kernel,
        out_shape=shape((nx, own, LANES), F32),
        in_specs=[SMEM, VMEM, VMEM],
        out_specs=VMEM,
        name="pieces",
    )(at, lowrank_mean, lowrank_square)
    moments = jnp.stack([pieces[0], *(shifted(pieces[s], "x", s) for s in range(1, nx))])
    neighbours = [lax.ppermute(projector, CLOSE, [(i, i ^ e) for i in range(count)]) for e in range(1, count)]
    factors = jnp.stack([projector, *neighbours])
    first, moments, factors = lax.optimization_barrier((first, moments, factors))

    second = pl.pallas_call(
        functools.partial(second_kernel, own),
        out_shape=pltpu.VMEM((far, own + heads, LANES), BF),
        in_specs=[VMEM],
        out_specs=VMEM,
        name="second",
    )(near_memory(first))
    second = swap(second, FAR)

    gradient, third, gates = pl.pallas_call(
        functools.partial(third_kernel, norming),
        out_shape=(
            pltpu.VMEM((own, LANES), F32),
            pltpu.VMEM((far, block, LANES), BF),
            pltpu.VMEM((heads, LANES), F32),
        ),
        in_specs=[SMEM, VMEM, VMEM],
        out_specs=(VMEM, VMEM, VMEM),
        name="third",
    )(at, near_memory(second), near_memory(factors))
    third = swap(third, FAR)

    fourth = pl.pallas_call(
        functools.partial(fourth_kernel, (nx, nc)),
        out_shape=pltpu.VMEM((count * nx * nc, own + 16, LANES), BF),
        in_specs=[SMEM, VMEM, VMEM, VMEM, VMEM, VMEM],
        out_specs=VMEM,
        name="fourth",
    )(
        at,
        near_memory(third),
        near_memory(moments),
        near_memory(factors),
        near_memory(gradient),
        near_memory(gates),
    )
    fourth = swap(fourth, LAST)

    return pl.pallas_call(
        functools.partial(last_kernel, (count, nx, nc)),
        out_shape=(
            shape((own, columns), F32),
            shape((own, columns), F32),
            shape((own, columns), BF),
            shape((block, columns), F32),
            shape((block, columns), F32),
            shape((heads, width), F32),
            shape((heads, width), F32),
            shape((heads, width), F32),
        ),
        in_specs=[SMEM, *[VMEM] * 6],
        out_specs=(VMEM,) * 8,
        name="last",
    )(at, near_memory(fourth), query_master, lowrank_mean, lowrank_square, gating_mean, gating_square)


def solution(mesh):
    split = Mesh(
        mesh.devices.reshape(4, 2, 4, 2, mesh.shape["rep"], mesh.shape["tp"]),
        ("zh", "zl", "yh", "yl", "x", "c"),
    )
    in_specs = (
        P((*FS, "x"), None),
        P((*FS, "x"), "c"),
        P("c", (*FS, "x")),
        P("c", (*FS, "x")),
        P(FS, None),
        P(FS, "c"),
        P("x", "c"),
        P("x", "c"),
        P("c", None),
        P("c", None),
    )
    out_specs = (
        P(FS, "c"),
        P(FS, "c"),
        P(FS, "c"),
        P("x", "c"),
        P("x", "c"),
        P("c", None),
        P("c", None),
        P("c", None),
    )
    return jax.shard_map(
        per_device, mesh=split, in_specs=in_specs, out_specs=out_specs, check_vma=False
    )
```

```python
import functools

import jax
import jax.numpy as jnp
from jax import lax
from jax.experimental import pallas as pl
from jax.experimental.pallas import tpu as pltpu
from jax.sharding import Mesh
from jax.sharding import PartitionSpec as P

FS = ("zh", "zl", "yh", "yl")
NEAR = ("zl", "yl", "x")
FAR = ("zh", "yh")
CLOSE = ("zl", "yl")
LAST = ("zl", "yl", "x", "c")


BETA_ONE = 0.9
BETA_TWO = 0.95
STEP_RATE = 0.01
EPSILON = 1e-08
NORM_FLOOR = 1e-06
BF = jnp.bfloat16
F32 = jnp.float32
FIRST = (((0,), (0,)), ((), ()))
LANES = 128
PART = 32
VMEM = pl.BlockSpec(memory_space=pltpu.VMEM)
ANY = pl.BlockSpec(memory_space=pltpu.HBM)


def swap(pieces, axes):
    return lax.all_to_all(pieces, axes, 0, 0, tiled=True)


def shifted(value, axis, step):
    length = lax.axis_size(axis)
    return lax.ppermute(value, axis, [(i, (i + step) % length) for i in range(length)])


def split_two(v):
    high = v.astype(BF)
    return high, (v - high.astype(F32)).astype(BF)


def dot(a, b, dims=(((1,), (0,)), ((), ()))):
    return lax.dot_general(a, b, dims, preferred_element_type=F32)


def one_less_exp(v):
    series = 1.0 + v * 0.125
    for k in range(7, 1, -1):
        series = 1.0 + v * (1.0 / k) * series
    return jnp.where(v > -0.3, -v * series, 1.0 - jnp.exp(v))


def gate_signals(cot, totals):
    heads, tokens = cot.shape
    later = lax.broadcasted_iota(jnp.int32, (tokens, tokens), 0) >= lax.broadcasted_iota(
        jnp.int32, (tokens, tokens), 1
    )
    later = jnp.where(later, 1.0, 0.0).astype(BF)
    one = cot.astype(BF).astype(F32)
    rest = cot - one
    two = rest.astype(BF).astype(F32)
    parts = jnp.concatenate([one, two, rest - two, jnp.zeros_like(one)], axis=0).astype(BF)
    trailing = dot(parts, later)
    trailing = trailing[2 * heads : 3 * heads] + trailing[heads : 2 * heads] + trailing[:heads]
    lane = lax.broadcasted_iota(jnp.int32, totals.shape, 1)
    gate = totals - jnp.where(lane == 0, 0.0, pltpu.roll(totals, 1, 1))
    return (trailing * one_less_exp(gate)).astype(BF)


def lane_blocks(shape):
    return lax.broadcasted_iota(jnp.int32, shape, len(shape) - 1) // PART


def turn(value, blocks):
    blocks = blocks % (LANES // PART)
    return pltpu.roll(value, blocks * PART, 1) if blocks else value


def turn_by(value, blocks):
    count = LANES // PART
    return pltpu.roll(value, lax.rem(blocks + 2 * count, count) * PART, 1)


def first_kernel(
    sizes,
    x_ref,
    q_ref,
    cot_ref,
    tot_ref,
    out_ref,
    x_held,
    q_held,
    cot_held,
    tot_held,
    out_held,
    gate_held,
    x_sem,
    q_sem,
    small_sem,
    out_sem,
):
    nz, nzl, ny, nyl, nx, own = sizes
    wide = x_held.shape[2]
    heads = gate_held.shape[1]
    small = [
        pltpu.make_async_copy(cot_ref, cot_held, small_sem.at[0]),
        pltpu.make_async_copy(tot_ref, tot_held, small_sem.at[1]),
    ]
    q_copy = pltpu.make_async_copy(q_ref, q_held, q_sem)
    loads = [
        pltpu.make_async_copy(x_ref.at[:, z * wide : (z + 1) * wide], x_held.at[z], x_sem.at[z])
        for z in range(nz)
    ]
    for copy in (*small, q_copy, loads[0]):
        copy.start()
    for copy in small:
        copy.wait()
    for copy in loads[1:]:
        copy.start()
    signal = gate_signals(cot_held[...], tot_held[...])
    lane = lane_blocks((own, LANES))
    q_copy.wait()

    def send_of(z):
        rows = pl.ds(pl.multiple_of(z * ny * own, ny * own), ny * own)
        return pltpu.make_async_copy(out_held.at[z], out_ref.at[:, rows, :], out_sem.at[z])

    def step(z, carry):
        columns = pl.ds(pl.multiple_of(z * wide, wide), wide)
        pltpu.make_async_copy(x_ref.at[:, columns], x_held.at[z], x_sem.at[z]).wait()
        block = x_held[z]
        part = dot(block, q_held[...], FIRST)
        for yh in range(ny):
            to = slice(yh * own, (yh + 1) * own)
            for q in range(nx):
                turned = []
                for j in range(nzl * nyl):
                    row = ((j // nyl * ny + yh) * nyl + j % nyl) * own
                    turned.append(turn(part[row : row + own, q * LANES : (q + 1) * LANES], j))
                for t in range(nzl * nyl):
                    piece = turned[0]
                    for j in range(1, nzl * nyl):
                        piece = jnp.where(lane == (t + j) % (nzl * nyl), turned[j], piece)
                    out_held[z, t * nx + q, to, :] = piece.astype(BF)
        send_of(z).start()
        gates = dot(signal, block).astype(BF)
        for k in range(wide // LANES):
            gate_held[z * (wide // LANES) + k] = gates[:, k * LANES : (k + 1) * LANES]
        return carry

    lax.fori_loop(0, nz, step, 0)
    target = out_ref.at[:, nz * ny * own : nz * ny * own + heads, :]
    gate_send = pltpu.make_async_copy(gate_held, target, out_sem.at[nz])
    gate_send.start()
    for z in range(nz):
        send_of(z).wait()
    gate_send.wait()


def second_kernel(own, in_ref, out_ref):
    far, rows = out_ref.shape[:2]
    for k in range(far + 1):
        cut = slice(k * own, (k + 1) * own) if k < far else slice(far * own, in_ref.shape[1])
        summed = in_ref[0, cut].astype(F32)
        for i in range(1, in_ref.shape[0]):
            summed = summed + in_ref[i, cut].astype(F32)
        if k < far:
            out_ref[k, :own, :] = summed.astype(BF)
        else:
            for j in range(far):
                out_ref[j, own:, :] = summed.astype(BF)


def four_factors(p_ref, t):
    return jnp.concatenate([p_ref[j ^ t] for j in range(p_ref.shape[0])], axis=0)


def third_kernel(norming, in_ref, p_ref, gradient_ref, out_ref, gate_ref):
    own = p_ref.shape[1]
    count = p_ref.shape[0]
    summed = in_ref[0].astype(F32)
    for k in range(1, in_ref.shape[0]):
        summed = summed + in_ref[k].astype(F32)
    summed = summed * norming
    gate_ref[...] = summed[own:]
    gradient = turn_by(summed[:own], -lax.axis_index(CLOSE))
    gradient_ref[...] = gradient
    factor = four_factors(p_ref, lax.axis_index(CLOSE))
    high, low = split_two(jnp.concatenate([turn(gradient, -j) for j in range(count)], axis=0))
    rank = dot(factor, high, FIRST) + dot(factor, low, FIRST)
    block = rank.shape[0] // count
    lane = lane_blocks((block, LANES))
    packed = rank[:block]
    for u in range(1, count):
        packed = jnp.where(lane == u, turn(rank[u * block : (u + 1) * block], u), packed)
    packed = packed.astype(BF)
    for k in range(out_ref.shape[0]):
        out_ref[k] = packed


def moment_kernel(mean_ref, square_ref, out_ref):
    own = out_ref.shape[1]
    lane = lane_blocks((own, LANES))
    count = out_ref.shape[0]
    for s in range(count):
        cut = pl.ds(pl.multiple_of(lax.rem(lax.axis_index("x") + s, count) * LANES, LANES), LANES)
        mean, square = mean_ref[:, cut], square_ref[:, cut]
        piece = None
        for k, rows in enumerate((mean[:own], mean[own:], square[:own], square[own:])):
            rows = turn_by(rows, k - lax.axis_index(CLOSE))
            piece = rows if k == 0 else jnp.where(lane == k, rows, piece)
        out_ref[s] = piece


def fourth_kernel(sizes, in_ref, moments_ref, p_ref, gradient_ref, gates_ref, out_ref):
    nx, nc = sizes
    count, own = p_ref.shape[:2]
    projected = in_ref[0].astype(F32)
    for k in range(1, in_ref.shape[0]):
        projected = projected + in_ref[k].astype(F32)
    block = projected.shape[0]
    lane = lane_blocks((own, LANES))
    moments = [moments_ref[0]] * 4
    for s in range(nx):
        u = lax.rem(lax.axis_index("x") + nx - s, nx)
        piece = moments_ref[s]
        moments = [jnp.where(lane == u, turn_by(piece, u - k), moments[k]) for k in range(4)]
    mean = jnp.concatenate(moments[:2], axis=0)
    square = jnp.concatenate(moments[2:], axis=0)
    mean = BETA_ONE * mean + (1.0 - BETA_ONE) * projected
    square = BETA_TWO * square + (1.0 - BETA_TWO) * projected * projected
    direction = mean / (jnp.sqrt(square) + EPSILON)
    sums = [
        jnp.sum(direction * direction, axis=0, keepdims=True),
        jnp.sum(projected * projected, axis=0, keepdims=True),
    ]
    sums = jnp.concatenate(sums, axis=0)
    one = sums.astype(BF).astype(F32)
    two = (sums - one).astype(BF).astype(F32)
    sums = jnp.concatenate([one, two, sums - one - two, jnp.zeros((2, LANES), F32)], axis=0).astype(BF)
    lane = lane_blocks((block, LANES))
    both = [jnp.where(lane == 0, turn(direction, -u), turn(projected, 1 - u)) for u in range(count)]
    high, low = split_two(jnp.concatenate(both, axis=0))
    factor = four_factors(p_ref, lax.axis_index(CLOSE))
    lifted = dot(factor, high) + dot(factor, low)
    lane = lane_blocks((own, LANES))
    gates = gates_ref[...].astype(BF)
    gradient = gradient_ref[...]
    for x in range(nx):
        tail = jnp.where(lane == 2, turn(projected[:own], 2 - x), turn(projected[own:], 3 - x))
        for j in range(count):
            piece = lifted[j * own : (j + 1) * own]
            piece = jnp.where(lane == 1, piece - turn(gradient, 1 - j), piece)
            piece = jnp.where(lane < 2, piece, tail).astype(BF)
            for c in range(nc):
                k = (j * nx + x) * nc + c
                out_ref[k, :own] = piece
                out_ref[k, own : own + 8] = gates
                out_ref[k, own + 8 :] = sums


def last_kernel(
    sizes,
    in_ref,
    master_ref,
    mean_ref,
    square_ref,
    gate_mean_ref,
    gate_square_ref,
    update_ref,
    new_ref,
    copy_ref,
    mean_out,
    square_out,
    gate_update_ref,
    average_ref,
    energy_ref,
):
    count, nx, nc = sizes
    own = master_ref.shape[0]
    sums = in_ref[0, own + 8 :].astype(F32)
    for k in range(1, in_ref.shape[0]):
        sums = sums + in_ref[k, own + 8 :].astype(F32)
    sums = sums[0:2] + sums[2:4] + sums[4:6]
    direction_squares = jnp.sum(sums[0:1], axis=1, keepdims=True)
    projected_squares = jnp.sum(sums[1:2], axis=1, keepdims=True)
    balance = jnp.sqrt(direction_squares / (projected_squares + NORM_FLOOR))
    lane = lane_blocks((own, LANES))
    for x in range(nx):
        update, upper, lower = None, None, None
        for t in range(count):
            k = (t * nx + x) * nc + lax.axis_index("c")
            piece = in_ref[k, :own].astype(F32)
            term = turn(piece - balance * turn(piece, -1), t)
            above, below = turn(piece, t - 2), turn(piece, t - 3)
            update = term if t == 0 else jnp.where(lane == t, term, update)
            upper = above if t == 0 else jnp.where(lane == t, above, upper)
            lower = below if t == 0 else jnp.where(lane == t, below, lower)
            g = in_ref[k, own : own + 8].astype(F32)
            place = slice((t * nx + x) * LANES, (t * nx + x + 1) * LANES)
            average = BETA_ONE * gate_mean_ref[:, place] + (1.0 - BETA_ONE) * g
            energy = BETA_TWO * gate_square_ref[:, place] + (1.0 - BETA_TWO) * g * g
            average_ref[:, place] = average
            energy_ref[:, place] = energy
            gate_update_ref[:, place] = average / (jnp.sqrt(energy) + EPSILON)
        cut = slice(x * LANES, (x + 1) * LANES)
        update_ref[:, cut] = update
        new = master_ref[:, cut] - STEP_RATE * update
        new_ref[:, cut] = new
        copy_ref[:, cut] = new.astype(BF)
        p = jnp.concatenate([upper, lower], axis=0)
        mean_out[:, cut] = BETA_ONE * mean_ref[:, cut] + (1.0 - BETA_ONE) * p
        square_out[:, cut] = BETA_TWO * square_ref[:, cut] + (1.0 - BETA_TWO) * p * p


def near_memory(value):
    return pltpu.with_memory_space_constraint(value, pltpu.VMEM)


def per_device(
    attention_input,
    query_cotangent,
    gate_cotangent,
    gate_totals,
    projector,
    query_master,
    lowrank_mean,
    lowrank_square,
    gating_mean,
    gating_square,
):
    nz, ny, nzl, nyl, nx, nc = (lax.axis_size(a) for a in ("zh", "yh", "zl", "yl", "x", "c"))
    far, near = nz * ny, nzl * nyl * nx
    count = nzl * nyl
    tokens, width = attention_input.shape
    columns = query_cotangent.shape[1]
    heads = gate_cotangent.shape[0]
    own, rank = projector.shape
    block = rank // nx
    norming = 1.0 / (tokens * far * near) ** 0.5
    shape = jax.ShapeDtypeStruct

    wide = nzl * ny * nyl * own
    first = pl.pallas_call(
        functools.partial(first_kernel, (nz, nzl, ny, nyl, nx, own)),
        out_shape=shape((near, far * own + heads, LANES), BF),
        in_specs=[ANY] * 4,
        out_specs=ANY,
        scratch_shapes=[
            pltpu.VMEM((nz, tokens, wide), BF),
            pltpu.VMEM((tokens, columns), BF),
            pltpu.VMEM((heads, tokens), F32),
            pltpu.VMEM((heads, tokens), F32),
            pltpu.VMEM((nz, near, ny * own, LANES), BF),
            pltpu.VMEM((near, heads, LANES), BF),
            pltpu.SemaphoreType.DMA((nz,)),
            pltpu.SemaphoreType.DMA,
            pltpu.SemaphoreType.DMA((2,)),
            pltpu.SemaphoreType.DMA((nz + 1,)),
        ],
        name="first",
    )(attention_input, query_cotangent, gate_cotangent, gate_totals)
    first = swap(first, NEAR)
    pieces = pl.pallas_call(
        moment_kernel,
        out_shape=shape((nx, own, LANES), F32),
        in_specs=[VMEM, VMEM],
        out_specs=VMEM,
        name="pieces",
    )(lowrank_mean, lowrank_square)
    moments = jnp.stack([pieces[0], *(shifted(pieces[s], "x", s) for s in range(1, nx))])
    neighbours = [lax.ppermute(projector, CLOSE, [(i, i ^ e) for i in range(count)]) for e in range(1, count)]
    factors = jnp.stack([projector, *neighbours])
    first, moments, factors = lax.optimization_barrier((first, moments, factors))

    second = pl.pallas_call(
        functools.partial(second_kernel, own),
        out_shape=pltpu.VMEM((far, own + heads, LANES), BF),
        in_specs=[VMEM],
        out_specs=VMEM,
        name="second",
    )(near_memory(first))
    second = swap(second, FAR)

    gradient, third, gates = pl.pallas_call(
        functools.partial(third_kernel, norming),
        out_shape=(
            pltpu.VMEM((own, LANES), F32),
            pltpu.VMEM((far, block, LANES), BF),
            pltpu.VMEM((heads, LANES), F32),
        ),
        in_specs=[VMEM, VMEM],
        out_specs=(VMEM, VMEM, VMEM),
        name="third",
    )(near_memory(second), near_memory(factors))
    third = swap(third, FAR)

    fourth = pl.pallas_call(
        functools.partial(fourth_kernel, (nx, nc)),
        out_shape=pltpu.VMEM((count * nx * nc, own + 16, LANES), BF),
        in_specs=[VMEM, VMEM, VMEM, VMEM, VMEM],
        out_specs=VMEM,
        name="fourth",
    )(
        near_memory(third),
        near_memory(moments),
        near_memory(factors),
        near_memory(gradient),
        near_memory(gates),
    )
    fourth = swap(fourth, LAST)

    return pl.pallas_call(
        functools.partial(last_kernel, (count, nx, nc)),
        out_shape=(
            shape((own, columns), F32),
            shape((own, columns), F32),
            shape((own, columns), BF),
            shape((block, columns), F32),
            shape((block, columns), F32),
            shape((heads, width), F32),
            shape((heads, width), F32),
            shape((heads, width), F32),
        ),
        in_specs=[VMEM] * 6,
        out_specs=(VMEM,) * 8,
        name="last",
    )(
        near_memory(fourth),
        near_memory(query_master),
        near_memory(lowrank_mean),
        near_memory(lowrank_square),
        near_memory(gating_mean),
        near_memory(gating_square),
    )


def solution(mesh):
    split = Mesh(
        mesh.devices.reshape(4, 2, 4, 2, mesh.shape["rep"], mesh.shape["tp"]),
        ("zh", "zl", "yh", "yl", "x", "c"),
    )
    in_specs = (
        P((*FS, "x"), None),
        P((*FS, "x"), "c"),
        P("c", (*FS, "x")),
        P("c", (*FS, "x")),
        P(FS, None),
        P(FS, "c"),
        P("x", "c"),
        P("x", "c"),
        P("c", None),
        P("c", None),
    )
    out_specs = (
        P(FS, "c"),
        P(FS, "c"),
        P(FS, "c"),
        P("x", "c"),
        P("x", "c"),
        P("c", None),
        P("c", None),
        P("c", None),
    )
    return jax.shard_map(
        per_device, mesh=split, in_specs=in_specs, out_specs=out_specs, check_vma=False
    )
```

```python
import functools

import jax
import jax.numpy as jnp
from jax import lax
from jax.experimental import pallas as pl
from jax.experimental.pallas import tpu as pltpu
from jax.sharding import Mesh
from jax.sharding import PartitionSpec as P

FS = ("zh", "zl", "yh", "yl")
NEAR = ("zl", "yl", "x")
FAR = ("zh", "yh")
CLOSE = ("zl", "yl")
LAST = ("zl", "yl", "x", "c")


BETA_ONE = 0.9
BETA_TWO = 0.95
STEP_RATE = 0.01
EPSILON = 1e-08
NORM_FLOOR = 1e-06
BF = jnp.bfloat16
F32 = jnp.float32
FIRST = (((0,), (0,)), ((), ()))
LANES = 128
PART = 32
VMEM = pl.BlockSpec(memory_space=pltpu.VMEM)
ANY = pl.BlockSpec(memory_space=pltpu.HBM)


def swap(pieces, axes):
    return lax.all_to_all(pieces, axes, 0, 0, tiled=True)


def shifted(value, axis, step):
    length = lax.axis_size(axis)
    return lax.ppermute(value, axis, [(i, (i + step) % length) for i in range(length)])


def split_two(v):
    high = v.astype(BF)
    return high, (v - high.astype(F32)).astype(BF)


def dot(a, b, dims=(((1,), (0,)), ((), ()))):
    return lax.dot_general(a, b, dims, preferred_element_type=F32)


def one_less_exp(v):
    series = 1.0 + v * 0.125
    for k in range(7, 1, -1):
        series = 1.0 + v * (1.0 / k) * series
    return jnp.where(v > -0.3, -v * series, 1.0 - jnp.exp(v))


def gate_signals(cot, totals):
    heads, tokens = cot.shape
    later = lax.broadcasted_iota(jnp.int32, (tokens, tokens), 0) >= lax.broadcasted_iota(
        jnp.int32, (tokens, tokens), 1
    )
    later = jnp.where(later, 1.0, 0.0).astype(BF)
    one = cot.astype(BF).astype(F32)
    rest = cot - one
    two = rest.astype(BF).astype(F32)
    parts = jnp.concatenate([one, two, rest - two, jnp.zeros_like(one)], axis=0).astype(BF)
    trailing = dot(parts, later)
    trailing = trailing[2 * heads : 3 * heads] + trailing[heads : 2 * heads] + trailing[:heads]
    lane = lax.broadcasted_iota(jnp.int32, totals.shape, 1)
    gate = totals - jnp.where(lane == 0, 0.0, pltpu.roll(totals, 1, 1))
    return (trailing * one_less_exp(gate)).astype(BF)


def lane_blocks(shape):
    return lax.broadcasted_iota(jnp.int32, shape, len(shape) - 1) // PART


def turn(value, blocks):
    blocks = blocks % (LANES // PART)
    return pltpu.roll(value, blocks * PART, 1) if blocks else value


def turn_by(value, blocks):
    count = LANES // PART
    return pltpu.roll(value, lax.rem(blocks + 2 * count, count) * PART, 1)


def first_kernel(
    sizes,
    x_ref,
    q_ref,
    cot_ref,
    tot_ref,
    out_ref,
    x_held,
    q_held,
    cot_held,
    tot_held,
    out_held,
    gate_held,
    x_sem,
    q_sem,
    small_sem,
    out_sem,
):
    nz, nzl, ny, nyl, nx, own = sizes
    wide = x_held.shape[2]
    heads = gate_held.shape[1]
    small = [
        pltpu.make_async_copy(cot_ref, cot_held, small_sem.at[0]),
        pltpu.make_async_copy(tot_ref, tot_held, small_sem.at[1]),
    ]
    q_copy = pltpu.make_async_copy(q_ref, q_held, q_sem)
    loads = [
        pltpu.make_async_copy(x_ref.at[:, z * wide : (z + 1) * wide], x_held.at[z], x_sem.at[z])
        for z in range(nz)
    ]
    for copy in (*small, q_copy, loads[0]):
        copy.start()
    for copy in small:
        copy.wait()
    for copy in loads[1:]:
        copy.start()
    signal = gate_signals(cot_held[...], tot_held[...])
    lane = lane_blocks((own, LANES))
    q_copy.wait()

    def send_of(z):
        rows = pl.ds(pl.multiple_of(z * ny * own, ny * own), ny * own)
        return pltpu.make_async_copy(out_held.at[z], out_ref.at[:, rows, :], out_sem.at[z])

    def step(z, carry):
        columns = pl.ds(pl.multiple_of(z * wide, wide), wide)
        pltpu.make_async_copy(x_ref.at[:, columns], x_held.at[z], x_sem.at[z]).wait()
        block = x_held[z]
        part = dot(block, q_held[...], FIRST)
        for yh in range(ny):
            to = slice(yh * own, (yh + 1) * own)
            for q in range(nx):
                turned = []
                for j in range(nzl * nyl):
                    row = ((j // nyl * ny + yh) * nyl + j % nyl) * own
                    turned.append(turn(part[row : row + own, q * LANES : (q + 1) * LANES], j))
                for t in range(nzl * nyl):
                    piece = turned[0]
                    for j in range(1, nzl * nyl):
                        piece = jnp.where(lane == (t + j) % (nzl * nyl), turned[j], piece)
                    out_held[z, t * nx + q, to, :] = piece.astype(BF)
        send_of(z).start()
        gates = dot(signal, block).astype(BF)
        for k in range(wide // LANES):
            gate_held[z * (wide // LANES) + k] = gates[:, k * LANES : (k + 1) * LANES]
        return carry

    lax.fori_loop(0, nz, step, 0)
    target = out_ref.at[:, nz * ny * own : nz * ny * own + heads, :]
    gate_send = pltpu.make_async_copy(gate_held, target, out_sem.at[nz])
    gate_send.start()
    for z in range(nz):
        send_of(z).wait()
    gate_send.wait()


def second_kernel(own, in_ref, out_ref):
    far, rows = out_ref.shape[:2]
    for k in range(far + 1):
        cut = slice(k * own, (k + 1) * own) if k < far else slice(far * own, in_ref.shape[1])
        summed = in_ref[0, cut].astype(F32)
        for i in range(1, in_ref.shape[0]):
            summed = summed + in_ref[i, cut].astype(F32)
        if k < far:
            out_ref[k, :own, :] = summed.astype(BF)
        else:
            for j in range(far):
                out_ref[j, own:, :] = summed.astype(BF)


def four_factors(p_ref, t):
    return jnp.concatenate([p_ref[j ^ t] for j in range(p_ref.shape[0])], axis=0)


def third_kernel(norming, in_ref, p_ref, gradient_ref, out_ref, gate_ref):
    own = p_ref.shape[1]
    count = p_ref.shape[0]
    summed = in_ref[0].astype(F32)
    for k in range(1, in_ref.shape[0]):
        summed = summed + in_ref[k].astype(F32)
    summed = summed * norming
    gate_ref[...] = summed[own:]
    gradient = turn_by(summed[:own], -lax.axis_index(CLOSE))
    gradient_ref[...] = gradient
    factor = four_factors(p_ref, lax.axis_index(CLOSE))
    high, low = split_two(jnp.concatenate([turn(gradient, -j) for j in range(count)], axis=0))
    rank = dot(factor, high, FIRST) + dot(factor, low, FIRST)
    block = rank.shape[0] // count
    lane = lane_blocks((block, LANES))
    packed = rank[:block]
    for u in range(1, count):
        packed = jnp.where(lane == u, turn(rank[u * block : (u + 1) * block], u), packed)
    packed = packed.astype(BF)
    for k in range(out_ref.shape[0]):
        out_ref[k] = packed


def moment_kernel(mean_ref, square_ref, out_ref):
    own = out_ref.shape[1]
    lane = lane_blocks((own, LANES))
    count = out_ref.shape[0]
    for s in range(count):
        cut = pl.ds(pl.multiple_of(lax.rem(lax.axis_index("x") + s, count) * LANES, LANES), LANES)
        mean, square = mean_ref[:, cut], square_ref[:, cut]
        piece = None
        for k, rows in enumerate((mean[:own], mean[own:], square[:own], square[own:])):
            rows = turn_by(rows, k - lax.axis_index(CLOSE))
            piece = rows if k == 0 else jnp.where(lane == k, rows, piece)
        out_ref[s] = piece


def fourth_kernel(sizes, in_ref, moments_ref, p_ref, gradient_ref, gates_ref, out_ref):
    nx, nc = sizes
    count, own = p_ref.shape[:2]
    projected = in_ref[0].astype(F32)
    for k in range(1, in_ref.shape[0]):
        projected = projected + in_ref[k].astype(F32)
    block = projected.shape[0]
    lane = lane_blocks((own, LANES))
    moments = [moments_ref[0]] * 4
    for s in range(nx):
        u = lax.rem(lax.axis_index("x") + nx - s, nx)
        piece = moments_ref[s]
        moments = [jnp.where(lane == u, turn_by(piece, u - k), moments[k]) for k in range(4)]
    mean = jnp.concatenate(moments[:2], axis=0)
    square = jnp.concatenate(moments[2:], axis=0)
    mean = BETA_ONE * mean + (1.0 - BETA_ONE) * projected
    square = BETA_TWO * square + (1.0 - BETA_TWO) * projected * projected
    direction = mean / (jnp.sqrt(square) + EPSILON)
    sums = [
        jnp.sum(direction * direction, axis=0, keepdims=True),
        jnp.sum(projected * projected, axis=0, keepdims=True),
    ]
    sums = jnp.concatenate(sums, axis=0)
    one = sums.astype(BF).astype(F32)
    two = (sums - one).astype(BF).astype(F32)
    sums = jnp.concatenate([one, two, sums - one - two, jnp.zeros((2, LANES), F32)], axis=0).astype(BF)
    lane = lane_blocks((block, LANES))
    both = [jnp.where(lane == 0, turn(direction, -u), turn(projected, 1 - u)) for u in range(count)]
    high, low = split_two(jnp.concatenate(both, axis=0))
    factor = four_factors(p_ref, lax.axis_index(CLOSE))
    lifted = dot(factor, high) + dot(factor, low)
    lane = lane_blocks((own, LANES))
    gates = gates_ref[...].astype(BF)
    gradient = gradient_ref[...]
    for x in range(nx):
        tail = jnp.where(lane == 2, turn(projected[:own], 2 - x), turn(projected[own:], 3 - x))
        for j in range(count):
            piece = lifted[j * own : (j + 1) * own]
            piece = jnp.where(lane == 1, piece - turn(gradient, 1 - j), piece)
            low = piece - piece.astype(BF).astype(F32)
            low = jnp.where(lane[: own // 2] < 2, low[: own // 2], turn(low[own // 2 :], 2)).astype(BF)
            piece = jnp.where(lane < 2, piece, tail).astype(BF)
            for c in range(nc):
                k = (j * nx + x) * nc + c
                out_ref[k, :own] = piece
                out_ref[k, own : own + own // 2] = low
                out_ref[k, own + own // 2 : own + own // 2 + 8] = gates
                out_ref[k, own + own // 2 + 8 :] = sums


def last_kernel(
    sizes,
    in_ref,
    master_ref,
    mean_ref,
    square_ref,
    gate_mean_ref,
    gate_square_ref,
    update_ref,
    new_ref,
    copy_ref,
    mean_out,
    square_out,
    gate_update_ref,
    average_ref,
    energy_ref,
):
    count, nx, nc = sizes
    own = master_ref.shape[0]
    after = own + own // 2
    sums = in_ref[0, after + 8 :].astype(F32)
    for k in range(1, in_ref.shape[0]):
        sums = sums + in_ref[k, after + 8 :].astype(F32)
    sums = sums[0:2] + sums[2:4] + sums[4:6]
    direction_squares = jnp.sum(sums[0:1], axis=1, keepdims=True)
    projected_squares = jnp.sum(sums[1:2], axis=1, keepdims=True)
    balance = jnp.sqrt(direction_squares / (projected_squares + NORM_FLOOR))
    lane = lane_blocks((own, LANES))
    for x in range(nx):
        update, upper, lower = None, None, None
        for t in range(count):
            k = (t * nx + x) * nc + lax.axis_index("c")
            piece = in_ref[k, :own].astype(F32)
            low = in_ref[k, own:after].astype(F32)
            full = piece + jnp.concatenate([low, turn(low, -2)], axis=0)
            term = turn(full - balance * turn(full, -1), t)
            above, below = turn(piece, t - 2), turn(piece, t - 3)
            update = term if t == 0 else jnp.where(lane == t, term, update)
            upper = above if t == 0 else jnp.where(lane == t, above, upper)
            lower = below if t == 0 else jnp.where(lane == t, below, lower)
            g = in_ref[k, after : after + 8].astype(F32)
            place = slice((t * nx + x) * LANES, (t * nx + x + 1) * LANES)
            average = BETA_ONE * gate_mean_ref[:, place] + (1.0 - BETA_ONE) * g
            energy = BETA_TWO * gate_square_ref[:, place] + (1.0 - BETA_TWO) * g * g
            average_ref[:, place] = average
            energy_ref[:, place] = energy
            gate_update_ref[:, place] = average / (jnp.sqrt(energy) + EPSILON)
        cut = slice(x * LANES, (x + 1) * LANES)
        update_ref[:, cut] = update
        new = master_ref[:, cut] - STEP_RATE * update
        new_ref[:, cut] = new
        copy_ref[:, cut] = new.astype(BF)
        p = jnp.concatenate([upper, lower], axis=0)
        mean_out[:, cut] = BETA_ONE * mean_ref[:, cut] + (1.0 - BETA_ONE) * p
        square_out[:, cut] = BETA_TWO * square_ref[:, cut] + (1.0 - BETA_TWO) * p * p


def near_memory(value):
    return pltpu.with_memory_space_constraint(value, pltpu.VMEM)


def per_device(
    attention_input,
    query_cotangent,
    gate_cotangent,
    gate_totals,
    projector,
    query_master,
    lowrank_mean,
    lowrank_square,
    gating_mean,
    gating_square,
):
    nz, ny, nzl, nyl, nx, nc = (lax.axis_size(a) for a in ("zh", "yh", "zl", "yl", "x", "c"))
    far, near = nz * ny, nzl * nyl * nx
    count = nzl * nyl
    tokens, width = attention_input.shape
    columns = query_cotangent.shape[1]
    heads = gate_cotangent.shape[0]
    own, rank = projector.shape
    block = rank // nx
    norming = 1.0 / (tokens * far * near) ** 0.5
    shape = jax.ShapeDtypeStruct

    wide = nzl * ny * nyl * own
    first = pl.pallas_call(
        functools.partial(first_kernel, (nz, nzl, ny, nyl, nx, own)),
        out_shape=shape((near, far * own + heads, LANES), BF),
        in_specs=[ANY] * 4,
        out_specs=ANY,
        scratch_shapes=[
            pltpu.VMEM((nz, tokens, wide), BF),
            pltpu.VMEM((tokens, columns), BF),
            pltpu.VMEM((heads, tokens), F32),
            pltpu.VMEM((heads, tokens), F32),
            pltpu.VMEM((nz, near, ny * own, LANES), BF),
            pltpu.VMEM((near, heads, LANES), BF),
            pltpu.SemaphoreType.DMA((nz,)),
            pltpu.SemaphoreType.DMA,
            pltpu.SemaphoreType.DMA((2,)),
            pltpu.SemaphoreType.DMA((nz + 1,)),
        ],
        name="first",
    )(attention_input, query_cotangent, gate_cotangent, gate_totals)
    first = swap(first, NEAR)
    pieces = pl.pallas_call(
        moment_kernel,
        out_shape=shape((nx, own, LANES), F32),
        in_specs=[VMEM, VMEM],
        out_specs=VMEM,
        name="pieces",
    )(lowrank_mean, lowrank_square)
    moments = jnp.stack([pieces[0], *(shifted(pieces[s], "x", s) for s in range(1, nx))])
    neighbours = [lax.ppermute(projector, CLOSE, [(i, i ^ e) for i in range(count)]) for e in range(1, count)]
    factors = jnp.stack([projector, *neighbours])
    first, moments, factors = lax.optimization_barrier((first, moments, factors))

    second = pl.pallas_call(
        functools.partial(second_kernel, own),
        out_shape=pltpu.VMEM((far, own + heads, LANES), BF),
        in_specs=[VMEM],
        out_specs=VMEM,
        name="second",
    )(near_memory(first))
    second = swap(second, FAR)

    gradient, third, gates = pl.pallas_call(
        functools.partial(third_kernel, norming),
        out_shape=(
            pltpu.VMEM((own, LANES), F32),
            pltpu.VMEM((far, block, LANES), BF),
            pltpu.VMEM((heads, LANES), F32),
        ),
        in_specs=[VMEM, VMEM],
        out_specs=(VMEM, VMEM, VMEM),
        name="third",
    )(near_memory(second), near_memory(factors))
    third = swap(third, FAR)

    fourth = pl.pallas_call(
        functools.partial(fourth_kernel, (nx, nc)),
        out_shape=pltpu.VMEM((count * nx * nc, own + own // 2 + 16, LANES), BF),
        in_specs=[VMEM, VMEM, VMEM, VMEM, VMEM],
        out_specs=VMEM,
        name="fourth",
    )(
        near_memory(third),
        near_memory(moments),
        near_memory(factors),
        near_memory(gradient),
        near_memory(gates),
    )
    fourth = swap(fourth, LAST)

    return pl.pallas_call(
        functools.partial(last_kernel, (count, nx, nc)),
        out_shape=(
            shape((own, columns), F32),
            shape((own, columns), F32),
            shape((own, columns), BF),
            shape((block, columns), F32),
            shape((block, columns), F32),
            shape((heads, width), F32),
            shape((heads, width), F32),
            shape((heads, width), F32),
        ),
        in_specs=[VMEM] * 6,
        out_specs=(VMEM,) * 8,
        name="last",
    )(
        near_memory(fourth),
        near_memory(query_master),
        near_memory(lowrank_mean),
        near_memory(lowrank_square),
        near_memory(gating_mean),
        near_memory(gating_square),
    )


def solution(mesh):
    split = Mesh(
        mesh.devices.reshape(4, 2, 4, 2, mesh.shape["rep"], mesh.shape["tp"]),
        ("zh", "zl", "yh", "yl", "x", "c"),
    )
    in_specs = (
        P((*FS, "x"), None),
        P((*FS, "x"), "c"),
        P("c", (*FS, "x")),
        P("c", (*FS, "x")),
        P(FS, None),
        P(FS, "c"),
        P("x", "c"),
        P("x", "c"),
        P("c", None),
        P("c", None),
    )
    out_specs = (
        P(FS, "c"),
        P(FS, "c"),
        P(FS, "c"),
        P("x", "c"),
        P("x", "c"),
        P("c", None),
        P("c", None),
        P("c", None),
    )
    return jax.shard_map(
        per_device, mesh=split, in_specs=in_specs, out_specs=out_specs, check_vma=False
    )
```

```python
import functools

import jax
import jax.numpy as jnp
from jax import lax
from jax.experimental import pallas as pl
from jax.experimental.pallas import tpu as pltpu
from jax.sharding import Mesh
from jax.sharding import PartitionSpec as P

FS = ("zh", "zl", "yh", "yl")
NEAR = ("zl", "yl", "x")
FAR = ("zh", "yh")
CLOSE = ("zl", "yl")
LAST = ("zl", "yl", "x", "c")


BETA_ONE = 0.9
BETA_TWO = 0.95
STEP_RATE = 0.01
EPSILON = 1e-08
NORM_FLOOR = 1e-06
BF = jnp.bfloat16
F32 = jnp.float32
FIRST = (((0,), (0,)), ((), ()))
LANES = 128
PART = 32
VMEM = pl.BlockSpec(memory_space=pltpu.VMEM)
ANY = pl.BlockSpec(memory_space=pltpu.HBM)


def swap(pieces, axes):
    return lax.all_to_all(pieces, axes, 0, 0, tiled=True)


def shifted(value, axis, step):
    length = lax.axis_size(axis)
    return lax.ppermute(value, axis, [(i, (i + step) % length) for i in range(length)])


def split_two(v):
    high = v.astype(BF)
    return high, (v - high.astype(F32)).astype(BF)


def dot(a, b, dims=(((1,), (0,)), ((), ()))):
    return lax.dot_general(a, b, dims, preferred_element_type=F32)


def one_less_exp(v):
    series = 1.0 + v * 0.125
    for k in range(7, 1, -1):
        series = 1.0 + v * (1.0 / k) * series
    return jnp.where(v > -0.3, -v * series, 1.0 - jnp.exp(v))


def gate_signals(cot, totals):
    heads, tokens = cot.shape
    later = lax.broadcasted_iota(jnp.int32, (tokens, tokens), 0) >= lax.broadcasted_iota(
        jnp.int32, (tokens, tokens), 1
    )
    later = jnp.where(later, 1.0, 0.0).astype(BF)
    one = cot.astype(BF).astype(F32)
    rest = cot - one
    two = rest.astype(BF).astype(F32)
    parts = jnp.concatenate([one, two, rest - two, jnp.zeros_like(one)], axis=0).astype(BF)
    trailing = dot(parts, later)
    trailing = trailing[2 * heads : 3 * heads] + trailing[heads : 2 * heads] + trailing[:heads]
    lane = lax.broadcasted_iota(jnp.int32, totals.shape, 1)
    gate = totals - jnp.where(lane == 0, 0.0, pltpu.roll(totals, 1, 1))
    return (trailing * one_less_exp(gate)).astype(BF)


def lane_blocks(shape):
    return lax.broadcasted_iota(jnp.int32, shape, len(shape) - 1) // PART


def turn(value, blocks):
    blocks = blocks % (LANES // PART)
    return pltpu.roll(value, blocks * PART, 1) if blocks else value


def turn_by(value, blocks):
    count = LANES // PART
    return pltpu.roll(value, lax.rem(blocks + 2 * count, count) * PART, 1)


def first_kernel(
    sizes,
    x_ref,
    q_ref,
    cot_ref,
    tot_ref,
    out_ref,
    x_held,
    q_held,
    cot_held,
    tot_held,
    out_held,
    gate_held,
    x_sem,
    q_sem,
    small_sem,
    out_sem,
):
    nz, nzl, ny, nyl, nx, own = sizes
    wide = x_held.shape[2]
    heads = gate_held.shape[1]
    small = [
        pltpu.make_async_copy(cot_ref, cot_held, small_sem.at[0]),
        pltpu.make_async_copy(tot_ref, tot_held, small_sem.at[1]),
    ]
    q_copy = pltpu.make_async_copy(q_ref, q_held, q_sem)
    loads = [
        pltpu.make_async_copy(x_ref.at[:, z * wide : (z + 1) * wide], x_held.at[z], x_sem.at[z])
        for z in range(nz)
    ]
    for copy in (*small, q_copy, loads[0]):
        copy.start()
    for copy in small:
        copy.wait()
    for copy in loads[1:]:
        copy.start()
    signal = gate_signals(cot_held[...], tot_held[...])
    lane = lane_blocks((own, LANES))
    q_copy.wait()

    def send_of(z):
        rows = pl.ds(pl.multiple_of(z * ny * own, ny * own), ny * own)
        return pltpu.make_async_copy(out_held.at[z], out_ref.at[:, rows, :], out_sem.at[z])

    def step(z, carry):
        columns = pl.ds(pl.multiple_of(z * wide, wide), wide)
        pltpu.make_async_copy(x_ref.at[:, columns], x_held.at[z], x_sem.at[z]).wait()
        block = x_held[z]
        part = dot(block, q_held[...], FIRST)
        for yh in range(ny):
            to = slice(yh * own, (yh + 1) * own)
            for q in range(nx):
                turned = []
                for j in range(nzl * nyl):
                    row = ((j // nyl * ny + yh) * nyl + j % nyl) * own
                    turned.append(turn(part[row : row + own, q * LANES : (q + 1) * LANES], j))
                for t in range(nzl * nyl):
                    piece = turned[0]
                    for j in range(1, nzl * nyl):
                        piece = jnp.where(lane == (t + j) % (nzl * nyl), turned[j], piece)
                    out_held[z, t * nx + q, to, :] = piece.astype(BF)
        send_of(z).start()
        gates = dot(signal, block).astype(BF)
        for k in range(wide // LANES):
            gate_held[z * (wide // LANES) + k] = gates[:, k * LANES : (k + 1) * LANES]
        return carry

    lax.fori_loop(0, nz, step, 0)
    target = out_ref.at[:, nz * ny * own : nz * ny * own + heads, :]
    gate_send = pltpu.make_async_copy(gate_held, target, out_sem.at[nz])
    gate_send.start()
    for z in range(nz):
        send_of(z).wait()
    gate_send.wait()


def second_kernel(own, in_ref, out_ref):
    far = out_ref.shape[0]

    def total(rows):
        summed = in_ref[0, rows].astype(F32)
        for i in range(1, in_ref.shape[0]):
            summed = summed + in_ref[i, rows].astype(F32)
        return summed

    def step(k, carry):
        high, low = split_two(total(pl.ds(pl.multiple_of(k * own, own), own)))
        out_ref[k, :own, :] = high
        out_ref[k, own : 2 * own, :] = low
        return carry

    lax.fori_loop(0, far, step, 0)
    gates = total(slice(far * own, in_ref.shape[1])).astype(BF)
    for k in range(far):
        out_ref[k, 2 * own :, :] = gates


def four_factors(p_ref, t):
    return jnp.concatenate([p_ref[j ^ t] for j in range(p_ref.shape[0])], axis=0)


def third_kernel(norming, in_ref, p_ref, gradient_ref, out_ref, gate_ref):
    own = p_ref.shape[1]
    count = p_ref.shape[0]
    summed = in_ref[0].astype(F32)
    for k in range(1, in_ref.shape[0]):
        summed = summed + in_ref[k].astype(F32)
    summed = summed * norming
    gate_ref[...] = summed[2 * own :]
    gradient = turn_by(summed[:own] + summed[own : 2 * own], -lax.axis_index(CLOSE))
    gradient_ref[...] = gradient
    factor = four_factors(p_ref, lax.axis_index(CLOSE))
    high, low = split_two(jnp.concatenate([turn(gradient, -j) for j in range(count)], axis=0))
    rank = dot(factor, high, FIRST) + dot(factor, low, FIRST)
    block = rank.shape[0] // count
    lane = lane_blocks((block, LANES))
    packed = rank[:block]
    for u in range(1, count):
        packed = jnp.where(lane == u, turn(rank[u * block : (u + 1) * block], u), packed)
    high, low = split_two(packed)
    for k in range(out_ref.shape[0]):
        out_ref[k, :block] = high
        out_ref[k, block:] = low


def moment_kernel(mean_ref, square_ref, out_ref):
    own = out_ref.shape[1]
    lane = lane_blocks((own, LANES))
    count = out_ref.shape[0]
    for s in range(count):
        cut = pl.ds(pl.multiple_of(lax.rem(lax.axis_index("x") + s, count) * LANES, LANES), LANES)
        mean, square = mean_ref[:, cut], square_ref[:, cut]
        piece = None
        for k, rows in enumerate((mean[:own], mean[own:], square[:own], square[own:])):
            rows = turn_by(rows, k - lax.axis_index(CLOSE))
            piece = rows if k == 0 else jnp.where(lane == k, rows, piece)
        out_ref[s] = piece


def fourth_kernel(sizes, in_ref, moments_ref, p_ref, gradient_ref, gates_ref, out_ref):
    nx, nc = sizes
    count, own = p_ref.shape[:2]
    projected = in_ref[0].astype(F32)
    for k in range(1, in_ref.shape[0]):
        projected = projected + in_ref[k].astype(F32)
    block = projected.shape[0] // 2
    projected = projected[:block] + projected[block:]
    lane = lane_blocks((own, LANES))
    moments = [moments_ref[0]] * 4
    for s in range(nx):
        u = lax.rem(lax.axis_index("x") + nx - s, nx)
        piece = moments_ref[s]
        moments = [jnp.where(lane == u, turn_by(piece, u - k), moments[k]) for k in range(4)]
    mean = jnp.concatenate(moments[:2], axis=0)
    square = jnp.concatenate(moments[2:], axis=0)
    mean = BETA_ONE * mean + (1.0 - BETA_ONE) * projected
    square = BETA_TWO * square + (1.0 - BETA_TWO) * projected * projected
    direction = mean / (jnp.sqrt(square) + EPSILON)
    sums = [
        jnp.sum(direction * direction, axis=0, keepdims=True),
        jnp.sum(projected * projected, axis=0, keepdims=True),
    ]
    sums = jnp.concatenate(sums, axis=0)
    one = sums.astype(BF).astype(F32)
    two = (sums - one).astype(BF).astype(F32)
    sums = jnp.concatenate([one, two, sums - one - two, jnp.zeros((2, LANES), F32)], axis=0).astype(BF)
    lane = lane_blocks((block, LANES))
    both = [jnp.where(lane == 0, turn(direction, -u), turn(projected, 1 - u)) for u in range(count)]
    high, low = split_two(jnp.concatenate(both, axis=0))
    factor = four_factors(p_ref, lax.axis_index(CLOSE))
    lifted = dot(factor, high) + dot(factor, low)
    lane = lane_blocks((own, LANES))
    gates = gates_ref[...].astype(BF)
    gradient = gradient_ref[...]
    for x in range(nx):
        tail = jnp.where(lane == 2, turn(projected[:own], 2 - x), turn(projected[own:], 3 - x))
        for j in range(count):
            piece = lifted[j * own : (j + 1) * own]
            piece = jnp.where(lane == 1, piece - turn(gradient, 1 - j), piece)
            low = piece - piece.astype(BF).astype(F32)
            low = jnp.where(lane[: own // 2] < 2, low[: own // 2], turn(low[own // 2 :], 2)).astype(BF)
            piece = jnp.where(lane < 2, piece, tail).astype(BF)
            for c in range(nc):
                k = (j * nx + x) * nc + c
                out_ref[k, :own] = piece
                out_ref[k, own : own + own // 2] = low
                out_ref[k, own + own // 2 : own + own // 2 + 8] = gates
                out_ref[k, own + own // 2 + 8 :] = sums


def last_kernel(
    sizes,
    in_ref,
    master_ref,
    mean_ref,
    square_ref,
    gate_mean_ref,
    gate_square_ref,
    update_ref,
    new_ref,
    copy_ref,
    mean_out,
    square_out,
    gate_update_ref,
    average_ref,
    energy_ref,
):
    count, nx, nc = sizes
    own = master_ref.shape[0]
    after = own + own // 2
    sums = in_ref[0, after + 8 :].astype(F32)
    for k in range(1, in_ref.shape[0]):
        sums = sums + in_ref[k, after + 8 :].astype(F32)
    sums = sums[0:2] + sums[2:4] + sums[4:6]
    direction_squares = jnp.sum(sums[0:1], axis=1, keepdims=True)
    projected_squares = jnp.sum(sums[1:2], axis=1, keepdims=True)
    balance = jnp.sqrt(direction_squares / (projected_squares + NORM_FLOOR))
    lane = lane_blocks((own, LANES))
    for x in range(nx):
        update, upper, lower = None, None, None
        for t in range(count):
            k = (t * nx + x) * nc + lax.axis_index("c")
            piece = in_ref[k, :own].astype(F32)
            low = in_ref[k, own:after].astype(F32)
            full = piece + jnp.concatenate([low, turn(low, -2)], axis=0)
            term = turn(full - balance * turn(full, -1), t)
            above, below = turn(piece, t - 2), turn(piece, t - 3)
            update = term if t == 0 else jnp.where(lane == t, term, update)
            upper = above if t == 0 else jnp.where(lane == t, above, upper)
            lower = below if t == 0 else jnp.where(lane == t, below, lower)
            g = in_ref[k, after : after + 8].astype(F32)
            place = slice((t * nx + x) * LANES, (t * nx + x + 1) * LANES)
            average = BETA_ONE * gate_mean_ref[:, place] + (1.0 - BETA_ONE) * g
            energy = BETA_TWO * gate_square_ref[:, place] + (1.0 - BETA_TWO) * g * g
            average_ref[:, place] = average
            energy_ref[:, place] = energy
            gate_update_ref[:, place] = average / (jnp.sqrt(energy) + EPSILON)
        cut = slice(x * LANES, (x + 1) * LANES)
        update_ref[:, cut] = update
        new = master_ref[:, cut] - STEP_RATE * update
        new_ref[:, cut] = new
        copy_ref[:, cut] = new.astype(BF)
        p = jnp.concatenate([upper, lower], axis=0)
        mean_out[:, cut] = BETA_ONE * mean_ref[:, cut] + (1.0 - BETA_ONE) * p
        square_out[:, cut] = BETA_TWO * square_ref[:, cut] + (1.0 - BETA_TWO) * p * p


def near_memory(value):
    return pltpu.with_memory_space_constraint(value, pltpu.VMEM)


def per_device(
    attention_input,
    query_cotangent,
    gate_cotangent,
    gate_totals,
    projector,
    query_master,
    lowrank_mean,
    lowrank_square,
    gating_mean,
    gating_square,
):
    nz, ny, nzl, nyl, nx, nc = (lax.axis_size(a) for a in ("zh", "yh", "zl", "yl", "x", "c"))
    far, near = nz * ny, nzl * nyl * nx
    count = nzl * nyl
    tokens, width = attention_input.shape
    columns = query_cotangent.shape[1]
    heads = gate_cotangent.shape[0]
    own, rank = projector.shape
    block = rank // nx
    norming = 1.0 / (tokens * far * near) ** 0.5
    shape = jax.ShapeDtypeStruct

    wide = nzl * ny * nyl * own
    first = pl.pallas_call(
        functools.partial(first_kernel, (nz, nzl, ny, nyl, nx, own)),
        out_shape=shape((near, far * own + heads, LANES), BF),
        in_specs=[ANY] * 4,
        out_specs=ANY,
        scratch_shapes=[
            pltpu.VMEM((nz, tokens, wide), BF),
            pltpu.VMEM((tokens, columns), BF),
            pltpu.VMEM((heads, tokens), F32),
            pltpu.VMEM((heads, tokens), F32),
            pltpu.VMEM((nz, near, ny * own, LANES), BF),
            pltpu.VMEM((near, heads, LANES), BF),
            pltpu.SemaphoreType.DMA((nz,)),
            pltpu.SemaphoreType.DMA,
            pltpu.SemaphoreType.DMA((2,)),
            pltpu.SemaphoreType.DMA((nz + 1,)),
        ],
        name="first",
    )(attention_input, query_cotangent, gate_cotangent, gate_totals)
    first = swap(first, NEAR)
    pieces = pl.pallas_call(
        moment_kernel,
        out_shape=shape((nx, own, LANES), F32),
        in_specs=[VMEM, VMEM],
        out_specs=VMEM,
        name="pieces",
    )(lowrank_mean, lowrank_square)
    moments = jnp.stack([pieces[0], *(shifted(pieces[s], "x", s) for s in range(1, nx))])
    neighbours = [lax.ppermute(projector, CLOSE, [(i, i ^ e) for i in range(count)]) for e in range(1, count)]
    factors = jnp.stack([projector, *neighbours])
    first, moments, factors = lax.optimization_barrier((first, moments, factors))

    second = pl.pallas_call(
        functools.partial(second_kernel, own),
        out_shape=pltpu.VMEM((far, 2 * own + heads, LANES), BF),
        in_specs=[VMEM],
        out_specs=VMEM,
        name="second",
    )(near_memory(first))
    second = swap(second, FAR)

    gradient, third, gates = pl.pallas_call(
        functools.partial(third_kernel, norming),
        out_shape=(
            pltpu.VMEM((own, LANES), F32),
            pltpu.VMEM((far, 2 * block, LANES), BF),
            pltpu.VMEM((heads, LANES), F32),
        ),
        in_specs=[VMEM, VMEM],
        out_specs=(VMEM, VMEM, VMEM),
        name="third",
    )(near_memory(second), near_memory(factors))
    third = swap(third, FAR)

    fourth = pl.pallas_call(
        functools.partial(fourth_kernel, (nx, nc)),
        out_shape=pltpu.VMEM((count * nx * nc, own + own // 2 + 16, LANES), BF),
        in_specs=[VMEM, VMEM, VMEM, VMEM, VMEM],
        out_specs=VMEM,
        name="fourth",
    )(
        near_memory(third),
        near_memory(moments),
        near_memory(factors),
        near_memory(gradient),
        near_memory(gates),
    )
    fourth = swap(fourth, LAST)

    return pl.pallas_call(
        functools.partial(last_kernel, (count, nx, nc)),
        out_shape=(
            shape((own, columns), F32),
            shape((own, columns), F32),
            shape((own, columns), BF),
            shape((block, columns), F32),
            shape((block, columns), F32),
            shape((heads, width), F32),
            shape((heads, width), F32),
            shape((heads, width), F32),
        ),
        in_specs=[VMEM] * 6,
        out_specs=(VMEM,) * 8,
        name="last",
    )(
        near_memory(fourth),
        near_memory(query_master),
        near_memory(lowrank_mean),
        near_memory(lowrank_square),
        near_memory(gating_mean),
        near_memory(gating_square),
    )


def solution(mesh):
    split = Mesh(
        mesh.devices.reshape(4, 2, 4, 2, mesh.shape["rep"], mesh.shape["tp"]),
        ("zh", "zl", "yh", "yl", "x", "c"),
    )
    in_specs = (
        P((*FS, "x"), None),
        P((*FS, "x"), "c"),
        P("c", (*FS, "x")),
        P("c", (*FS, "x")),
        P(FS, None),
        P(FS, "c"),
        P("x", "c"),
        P("x", "c"),
        P("c", None),
        P("c", None),
    )
    out_specs = (
        P(FS, "c"),
        P(FS, "c"),
        P(FS, "c"),
        P("x", "c"),
        P("x", "c"),
        P("c", None),
        P("c", None),
        P("c", None),
    )
    return jax.shard_map(
        per_device, mesh=split, in_specs=in_specs, out_specs=out_specs, check_vma=False
    )
```

```python
import functools

import jax
import jax.numpy as jnp
from jax import lax
from jax.experimental import pallas as pl
from jax.experimental.pallas import tpu as pltpu
from jax.sharding import Mesh
from jax.sharding import PartitionSpec as P

FS = ("zh", "zl", "yh", "yl")
NEAR = ("zl", "yl", "x")
FAR = ("zh", "yh")
CLOSE = ("zl", "yl")
LAST = ("zl", "yl", "x", "c")


BETA_ONE = 0.9
BETA_TWO = 0.95
STEP_RATE = 0.01
EPSILON = 1e-08
NORM_FLOOR = 1e-06
BF = jnp.bfloat16
F32 = jnp.float32
FIRST = (((0,), (0,)), ((), ()))
LANES = 128
PART = 32
VMEM = pl.BlockSpec(memory_space=pltpu.VMEM)
ANY = pl.BlockSpec(memory_space=pltpu.HBM)


def swap(pieces, axes):
    return lax.all_to_all(pieces, axes, 0, 0, tiled=True)


def shifted(value, axis, step):
    length = lax.axis_size(axis)
    return lax.ppermute(value, axis, [(i, (i + step) % length) for i in range(length)])


def split_two(v):
    high = v.astype(BF)
    return high, (v - high.astype(F32)).astype(BF)


def dot(a, b, dims=(((1,), (0,)), ((), ()))):
    return lax.dot_general(a, b, dims, preferred_element_type=F32)


def one_less_exp(v):
    series = 1.0 + v * 0.125
    for k in range(7, 1, -1):
        series = 1.0 + v * (1.0 / k) * series
    return jnp.where(v > -0.3, -v * series, 1.0 - jnp.exp(v))


def gate_signals(cot, totals):
    heads, tokens = cot.shape
    later = lax.broadcasted_iota(jnp.int32, (tokens, tokens), 0) >= lax.broadcasted_iota(
        jnp.int32, (tokens, tokens), 1
    )
    later = jnp.where(later, 1.0, 0.0).astype(BF)
    one = cot.astype(BF).astype(F32)
    rest = cot - one
    two = rest.astype(BF).astype(F32)
    parts = jnp.concatenate([one, two, rest - two, jnp.zeros_like(one)], axis=0).astype(BF)
    trailing = dot(parts, later)
    trailing = trailing[2 * heads : 3 * heads] + trailing[heads : 2 * heads] + trailing[:heads]
    lane = lax.broadcasted_iota(jnp.int32, totals.shape, 1)
    gate = totals - jnp.where(lane == 0, 0.0, pltpu.roll(totals, 1, 1))
    return (trailing * one_less_exp(gate)).astype(BF)


def lane_blocks(shape):
    return lax.broadcasted_iota(jnp.int32, shape, len(shape) - 1) // PART


def turn(value, blocks):
    blocks = blocks % (LANES // PART)
    return pltpu.roll(value, blocks * PART, 1) if blocks else value


def turn_by(value, blocks):
    count = LANES // PART
    return pltpu.roll(value, lax.rem(blocks + 2 * count, count) * PART, 1)


def first_kernel(
    sizes,
    x_ref,
    q_ref,
    cot_ref,
    tot_ref,
    out_ref,
    x_held,
    q_held,
    cot_held,
    tot_held,
    out_held,
    gate_held,
    x_sem,
    q_sem,
    small_sem,
    out_sem,
):
    nz, nzl, ny, nyl, nx, own = sizes
    wide = x_held.shape[2]
    heads = gate_held.shape[1]
    small = [
        pltpu.make_async_copy(cot_ref, cot_held, small_sem.at[0]),
        pltpu.make_async_copy(tot_ref, tot_held, small_sem.at[1]),
    ]
    q_copy = pltpu.make_async_copy(q_ref, q_held, q_sem)
    loads = [
        pltpu.make_async_copy(x_ref.at[:, z * wide : (z + 1) * wide], x_held.at[z], x_sem.at[z])
        for z in range(nz)
    ]
    for copy in (*small, q_copy, loads[0]):
        copy.start()
    for copy in small:
        copy.wait()
    for copy in loads[1:]:
        copy.start()
    signal = gate_signals(cot_held[...], tot_held[...])
    lane = lane_blocks((own, LANES))
    q_copy.wait()

    def send_of(z):
        rows = pl.ds(pl.multiple_of(z * ny * own, ny * own), ny * own)
        return pltpu.make_async_copy(out_held.at[z], out_ref.at[:, rows, :], out_sem.at[z])

    def step(z, carry):
        columns = pl.ds(pl.multiple_of(z * wide, wide), wide)
        pltpu.make_async_copy(x_ref.at[:, columns], x_held.at[z], x_sem.at[z]).wait()
        block = x_held[z]
        part = dot(block, q_held[...], FIRST)
        for yh in range(ny):
            to = slice(yh * own, (yh + 1) * own)
            for q in range(nx):
                turned = []
                for j in range(nzl * nyl):
                    row = ((j // nyl * ny + yh) * nyl + j % nyl) * own
                    turned.append(turn(part[row : row + own, q * LANES : (q + 1) * LANES], j))
                for t in range(nzl * nyl):
                    piece = turned[0]
                    for j in range(1, nzl * nyl):
                        piece = jnp.where(lane == (t + j) % (nzl * nyl), turned[j], piece)
                    out_held[z, t * nx + q, to, :] = piece.astype(BF)
        send_of(z).start()
        gates = dot(signal, block).astype(BF)
        for k in range(wide // LANES):
            gate_held[z * (wide // LANES) + k] = gates[:, k * LANES : (k + 1) * LANES]
        return carry

    lax.fori_loop(0, nz, step, 0)
    target = out_ref.at[:, nz * ny * own : nz * ny * own + heads, :]
    gate_send = pltpu.make_async_copy(gate_held, target, out_sem.at[nz])
    gate_send.start()
    for z in range(nz):
        send_of(z).wait()
    gate_send.wait()


def second_kernel(own, in_ref, out_ref):
    far = out_ref.shape[0]

    def total(rows):
        summed = in_ref[0, rows].astype(F32)
        for i in range(1, in_ref.shape[0]):
            summed = summed + in_ref[i, rows].astype(F32)
        return summed

    def step(k, carry):
        high, low = split_two(total(pl.ds(pl.multiple_of(k * own, own), own)))
        out_ref[k, :own, :] = high
        out_ref[k, own : 2 * own, :] = low
        return carry

    lax.fori_loop(0, far, step, 0)
    gates = total(slice(far * own, in_ref.shape[1])).astype(BF)
    for k in range(far):
        out_ref[k, 2 * own :, :] = gates


def four_factors(p_ref, t):
    return jnp.concatenate([p_ref[j ^ t] for j in range(p_ref.shape[0])], axis=0)


def third_kernel(norming, in_ref, p_ref, gradient_ref, out_ref, gate_ref):
    own = p_ref.shape[1]
    count = p_ref.shape[0]
    summed = in_ref[0].astype(F32)
    for k in range(1, in_ref.shape[0]):
        summed = summed + in_ref[k].astype(F32)
    summed = summed * norming
    gate_ref[...] = summed[2 * own :]
    gradient = turn_by(summed[:own] + summed[own : 2 * own], -lax.axis_index(CLOSE))
    gradient_ref[...] = gradient
    factor = four_factors(p_ref, lax.axis_index(CLOSE))
    high, low = split_two(jnp.concatenate([turn(gradient, -j) for j in range(count)], axis=0))
    rank = dot(factor, high, FIRST) + dot(factor, low, FIRST)
    block = rank.shape[0] // count
    lane = lane_blocks((block, LANES))
    packed = rank[:block]
    for u in range(1, count):
        packed = jnp.where(lane == u, turn(rank[u * block : (u + 1) * block], u), packed)
    packed = packed.astype(BF)
    for k in range(out_ref.shape[0]):
        out_ref[k] = packed


def moment_kernel(mean_ref, square_ref, out_ref):
    own = out_ref.shape[1]
    lane = lane_blocks((own, LANES))
    count = out_ref.shape[0]
    for s in range(count):
        cut = pl.ds(pl.multiple_of(lax.rem(lax.axis_index("x") + s, count) * LANES, LANES), LANES)
        mean, square = mean_ref[:, cut], square_ref[:, cut]
        piece = None
        for k, rows in enumerate((mean[:own], mean[own:], square[:own], square[own:])):
            rows = turn_by(rows, k - lax.axis_index(CLOSE))
            piece = rows if k == 0 else jnp.where(lane == k, rows, piece)
        out_ref[s] = piece


def fourth_kernel(sizes, in_ref, moments_ref, p_ref, gradient_ref, gates_ref, out_ref):
    nx, nc = sizes
    count, own = p_ref.shape[:2]
    projected = in_ref[0].astype(F32)
    for k in range(1, in_ref.shape[0]):
        projected = projected + in_ref[k].astype(F32)
    block = projected.shape[0]
    lane = lane_blocks((own, LANES))
    moments = [moments_ref[0]] * 4
    for s in range(nx):
        u = lax.rem(lax.axis_index("x") + nx - s, nx)
        piece = moments_ref[s]
        moments = [jnp.where(lane == u, turn_by(piece, u - k), moments[k]) for k in range(4)]
    mean = jnp.concatenate(moments[:2], axis=0)
    square = jnp.concatenate(moments[2:], axis=0)
    mean = BETA_ONE * mean + (1.0 - BETA_ONE) * projected
    square = BETA_TWO * square + (1.0 - BETA_TWO) * projected * projected
    direction = mean / (jnp.sqrt(square) + EPSILON)
    sums = [
        jnp.sum(direction * direction, axis=0, keepdims=True),
        jnp.sum(projected * projected, axis=0, keepdims=True),
    ]
    sums = jnp.concatenate(sums, axis=0)
    one = sums.astype(BF).astype(F32)
    two = (sums - one).astype(BF).astype(F32)
    sums = jnp.concatenate([one, two, sums - one - two, jnp.zeros((2, LANES), F32)], axis=0).astype(BF)
    lane = lane_blocks((block, LANES))
    both = [jnp.where(lane == 0, turn(direction, -u), turn(projected, 1 - u)) for u in range(count)]
    high, low = split_two(jnp.concatenate(both, axis=0))
    factor = four_factors(p_ref, lax.axis_index(CLOSE))
    lifted = dot(factor, high) + dot(factor, low)
    lane = lane_blocks((own, LANES))
    gates = gates_ref[...].astype(BF)
    gradient = gradient_ref[...]
    for x in range(nx):
        tail = jnp.where(lane == 2, turn(projected[:own], 2 - x), turn(projected[own:], 3 - x))
        for j in range(count):
            piece = lifted[j * own : (j + 1) * own]
            piece = jnp.where(lane == 1, piece - turn(gradient, 1 - j), piece)
            piece = jnp.where(lane < 2, piece, tail).astype(BF)
            for c in range(nc):
                k = (j * nx + x) * nc + c
                out_ref[k, :own] = piece
                out_ref[k, own : own + 8] = gates
                out_ref[k, own + 8 :] = sums


def last_kernel(
    sizes,
    in_ref,
    master_ref,
    mean_ref,
    square_ref,
    gate_mean_ref,
    gate_square_ref,
    update_ref,
    new_ref,
    copy_ref,
    mean_out,
    square_out,
    gate_update_ref,
    average_ref,
    energy_ref,
):
    count, nx, nc = sizes
    own = master_ref.shape[0]
    sums = in_ref[0, own + 8 :].astype(F32)
    for k in range(1, in_ref.shape[0]):
        sums = sums + in_ref[k, own + 8 :].astype(F32)
    sums = sums[0:2] + sums[2:4] + sums[4:6]
    direction_squares = jnp.sum(sums[0:1], axis=1, keepdims=True)
    projected_squares = jnp.sum(sums[1:2], axis=1, keepdims=True)
    balance = jnp.sqrt(direction_squares / (projected_squares + NORM_FLOOR))
    lane = lane_blocks((own, LANES))
    for x in range(nx):
        update, upper, lower = None, None, None
        for t in range(count):
            k = (t * nx + x) * nc + lax.axis_index("c")
            piece = in_ref[k, :own].astype(F32)
            term = turn(piece - balance * turn(piece, -1), t)
            above, below = turn(piece, t - 2), turn(piece, t - 3)
            update = term if t == 0 else jnp.where(lane == t, term, update)
            upper = above if t == 0 else jnp.where(lane == t, above, upper)
            lower = below if t == 0 else jnp.where(lane == t, below, lower)
            g = in_ref[k, own : own + 8].astype(F32)
            place = slice((t * nx + x) * LANES, (t * nx + x + 1) * LANES)
            average = BETA_ONE * gate_mean_ref[:, place] + (1.0 - BETA_ONE) * g
            energy = BETA_TWO * gate_square_ref[:, place] + (1.0 - BETA_TWO) * g * g
            average_ref[:, place] = average
            energy_ref[:, place] = energy
            gate_update_ref[:, place] = average / (jnp.sqrt(energy) + EPSILON)
        cut = slice(x * LANES, (x + 1) * LANES)
        update_ref[:, cut] = update
        new = master_ref[:, cut] - STEP_RATE * update
        new_ref[:, cut] = new
        copy_ref[:, cut] = new.astype(BF)
        p = jnp.concatenate([upper, lower], axis=0)
        mean_out[:, cut] = BETA_ONE * mean_ref[:, cut] + (1.0 - BETA_ONE) * p
        square_out[:, cut] = BETA_TWO * square_ref[:, cut] + (1.0 - BETA_TWO) * p * p


def near_memory(value):
    return pltpu.with_memory_space_constraint(value, pltpu.VMEM)


def per_device(
    attention_input,
    query_cotangent,
    gate_cotangent,
    gate_totals,
    projector,
    query_master,
    lowrank_mean,
    lowrank_square,
    gating_mean,
    gating_square,
):
    nz, ny, nzl, nyl, nx, nc = (lax.axis_size(a) for a in ("zh", "yh", "zl", "yl", "x", "c"))
    far, near = nz * ny, nzl * nyl * nx
    count = nzl * nyl
    tokens, width = attention_input.shape
    columns = query_cotangent.shape[1]
    heads = gate_cotangent.shape[0]
    own, rank = projector.shape
    block = rank // nx
    norming = 1.0 / (tokens * far * near) ** 0.5
    shape = jax.ShapeDtypeStruct

    wide = nzl * ny * nyl * own
    first = pl.pallas_call(
        functools.partial(first_kernel, (nz, nzl, ny, nyl, nx, own)),
        out_shape=shape((near, far * own + heads, LANES), BF),
        in_specs=[ANY] * 4,
        out_specs=ANY,
        scratch_shapes=[
            pltpu.VMEM((nz, tokens, wide), BF),
            pltpu.VMEM((tokens, columns), BF),
            pltpu.VMEM((heads, tokens), F32),
            pltpu.VMEM((heads, tokens), F32),
            pltpu.VMEM((nz, near, ny * own, LANES), BF),
            pltpu.VMEM((near, heads, LANES), BF),
            pltpu.SemaphoreType.DMA((nz,)),
            pltpu.SemaphoreType.DMA,
            pltpu.SemaphoreType.DMA((2,)),
            pltpu.SemaphoreType.DMA((nz + 1,)),
        ],
        name="first",
    )(attention_input, query_cotangent, gate_cotangent, gate_totals)
    first = swap(first, NEAR)
    pieces = pl.pallas_call(
        moment_kernel,
        out_shape=shape((nx, own, LANES), F32),
        in_specs=[VMEM, VMEM],
        out_specs=VMEM,
        name="pieces",
    )(lowrank_mean, lowrank_square)
    moments = jnp.stack([pieces[0], *(shifted(pieces[s], "x", s) for s in range(1, nx))])
    neighbours = [lax.ppermute(projector, CLOSE, [(i, i ^ e) for i in range(count)]) for e in range(1, count)]
    factors = jnp.stack([projector, *neighbours])
    first, moments, factors = lax.optimization_barrier((first, moments, factors))

    second = pl.pallas_call(
        functools.partial(second_kernel, own),
        out_shape=pltpu.VMEM((far, 2 * own + heads, LANES), BF),
        in_specs=[VMEM],
        out_specs=VMEM,
        name="second",
    )(near_memory(first))
    second = swap(second, FAR)

    gradient, third, gates = pl.pallas_call(
        functools.partial(third_kernel, norming),
        out_shape=(
            pltpu.VMEM((own, LANES), F32),
            pltpu.VMEM((far, block, LANES), BF),
            pltpu.VMEM((heads, LANES), F32),
        ),
        in_specs=[VMEM, VMEM],
        out_specs=(VMEM, VMEM, VMEM),
        name="third",
    )(near_memory(second), near_memory(factors))
    third = swap(third, FAR)

    fourth = pl.pallas_call(
        functools.partial(fourth_kernel, (nx, nc)),
        out_shape=pltpu.VMEM((count * nx * nc, own + 16, LANES), BF),
        in_specs=[VMEM, VMEM, VMEM, VMEM, VMEM],
        out_specs=VMEM,
        name="fourth",
    )(
        near_memory(third),
        near_memory(moments),
        near_memory(factors),
        near_memory(gradient),
        near_memory(gates),
    )
    fourth = swap(fourth, LAST)

    return pl.pallas_call(
        functools.partial(last_kernel, (count, nx, nc)),
        out_shape=(
            shape((own, columns), F32),
            shape((own, columns), F32),
            shape((own, columns), BF),
            shape((block, columns), F32),
            shape((block, columns), F32),
            shape((heads, width), F32),
            shape((heads, width), F32),
            shape((heads, width), F32),
        ),
        in_specs=[VMEM] * 6,
        out_specs=(VMEM,) * 8,
        name="last",
    )(
        near_memory(fourth),
        near_memory(query_master),
        near_memory(lowrank_mean),
        near_memory(lowrank_square),
        near_memory(gating_mean),
        near_memory(gating_square),
    )


def solution(mesh):
    split = Mesh(
        mesh.devices.reshape(4, 2, 4, 2, mesh.shape["rep"], mesh.shape["tp"]),
        ("zh", "zl", "yh", "yl", "x", "c"),
    )
    in_specs = (
        P((*FS, "x"), None),
        P((*FS, "x"), "c"),
        P("c", (*FS, "x")),
        P("c", (*FS, "x")),
        P(FS, None),
        P(FS, "c"),
        P("x", "c"),
        P("x", "c"),
        P("c", None),
        P("c", None),
    )
    out_specs = (
        P(FS, "c"),
        P(FS, "c"),
        P(FS, "c"),
        P("x", "c"),
        P("x", "c"),
        P("c", None),
        P("c", None),
        P("c", None),
    )
    return jax.shard_map(
        per_device, mesh=split, in_specs=in_specs, out_specs=out_specs, check_vma=False
    )
```

```python
import functools

import jax
import jax.numpy as jnp
from jax import lax
from jax.experimental import pallas as pl
from jax.experimental.pallas import tpu as pltpu
from jax.sharding import Mesh
from jax.sharding import PartitionSpec as P

FS = ("zh", "zl", "yh", "yl")
NEAR = ("zl", "yl", "x")
FAR = ("zh", "yh")
CLOSE = ("zl", "yl")
LAST = ("zl", "yl", "x", "c")


BETA_ONE = 0.9
BETA_TWO = 0.95
STEP_RATE = 0.01
EPSILON = 1e-08
NORM_FLOOR = 1e-06
BF = jnp.bfloat16
F32 = jnp.float32
FIRST = (((0,), (0,)), ((), ()))
LANES = 128
PART = 32
VMEM = pl.BlockSpec(memory_space=pltpu.VMEM)
ANY = pl.BlockSpec(memory_space=pltpu.HBM)


def swap(pieces, axes):
    return lax.all_to_all(pieces, axes, 0, 0, tiled=True)


def shifted(value, axis, step):
    length = lax.axis_size(axis)
    return lax.ppermute(value, axis, [(i, (i + step) % length) for i in range(length)])


def split_two(v):
    high = v.astype(BF)
    return high, (v - high.astype(F32)).astype(BF)


def dot(a, b, dims=(((1,), (0,)), ((), ()))):
    return lax.dot_general(a, b, dims, preferred_element_type=F32)


def one_less_exp(v):
    series = 1.0 + v * 0.125
    for k in range(7, 1, -1):
        series = 1.0 + v * (1.0 / k) * series
    return jnp.where(v > -0.3, -v * series, 1.0 - jnp.exp(v))


def gate_signals(cot, totals):
    heads, tokens = cot.shape
    later = lax.broadcasted_iota(jnp.int32, (tokens, tokens), 0) >= lax.broadcasted_iota(
        jnp.int32, (tokens, tokens), 1
    )
    later = jnp.where(later, 1.0, 0.0).astype(BF)
    one = cot.astype(BF).astype(F32)
    rest = cot - one
    two = rest.astype(BF).astype(F32)
    parts = jnp.concatenate([one, two, rest - two, jnp.zeros_like(one)], axis=0).astype(BF)
    trailing = dot(parts, later)
    trailing = trailing[2 * heads : 3 * heads] + trailing[heads : 2 * heads] + trailing[:heads]
    lane = lax.broadcasted_iota(jnp.int32, totals.shape, 1)
    gate = totals - jnp.where(lane == 0, 0.0, pltpu.roll(totals, 1, 1))
    return (trailing * one_less_exp(gate)).astype(BF)


def lane_blocks(shape):
    return lax.broadcasted_iota(jnp.int32, shape, len(shape) - 1) // PART


def turn(value, blocks):
    blocks = blocks % (LANES // PART)
    return pltpu.roll(value, blocks * PART, 1) if blocks else value


def turn_by(value, blocks):
    count = LANES // PART
    return pltpu.roll(value, lax.rem(blocks + 2 * count, count) * PART, 1)


def first_kernel(
    sizes,
    x_ref,
    q_ref,
    cot_ref,
    tot_ref,
    out_ref,
    x_held,
    q_held,
    cot_held,
    tot_held,
    out_held,
    gate_held,
    x_sem,
    q_sem,
    small_sem,
    out_sem,
):
    nz, nzl, ny, nyl, nx, own = sizes
    wide = x_held.shape[2]
    heads = gate_held.shape[1]
    small = [
        pltpu.make_async_copy(cot_ref, cot_held, small_sem.at[0]),
        pltpu.make_async_copy(tot_ref, tot_held, small_sem.at[1]),
    ]
    q_copy = pltpu.make_async_copy(q_ref, q_held, q_sem)
    loads = [
        pltpu.make_async_copy(x_ref.at[:, z * wide : (z + 1) * wide], x_held.at[z], x_sem.at[z])
        for z in range(nz)
    ]
    for copy in (*small, q_copy, loads[0]):
        copy.start()
    for copy in small:
        copy.wait()
    for copy in loads[1:]:
        copy.start()
    signal = gate_signals(cot_held[...], tot_held[...])
    lane = lane_blocks((own, LANES))
    q_copy.wait()

    def send_of(z):
        rows = pl.ds(pl.multiple_of(z * ny * own, ny * own), ny * own)
        return pltpu.make_async_copy(out_held.at[z], out_ref.at[:, rows, :], out_sem.at[z])

    def step(z, carry):
        columns = pl.ds(pl.multiple_of(z * wide, wide), wide)
        pltpu.make_async_copy(x_ref.at[:, columns], x_held.at[z], x_sem.at[z]).wait()
        block = x_held[z]
        part = dot(block, q_held[...], FIRST)
        for yh in range(ny):
            to = slice(yh * own, (yh + 1) * own)
            for q in range(nx):
                turned = []
                for j in range(nzl * nyl):
                    row = ((j // nyl * ny + yh) * nyl + j % nyl) * own
                    turned.append(turn(part[row : row + own, q * LANES : (q + 1) * LANES], j))
                for t in range(nzl * nyl):
                    piece = turned[0]
                    for j in range(1, nzl * nyl):
                        piece = jnp.where(lane == (t + j) % (nzl * nyl), turned[j], piece)
                    out_held[z, t * nx + q, to, :] = piece.astype(BF)
        send_of(z).start()
        gates = dot(signal, block).astype(BF)
        for k in range(wide // LANES):
            gate_held[z * (wide // LANES) + k] = gates[:, k * LANES : (k + 1) * LANES]
        return carry

    lax.fori_loop(0, nz, step, 0)
    target = out_ref.at[:, nz * ny * own : nz * ny * own + heads, :]
    gate_send = pltpu.make_async_copy(gate_held, target, out_sem.at[nz])
    gate_send.start()
    for z in range(nz):
        send_of(z).wait()
    gate_send.wait()


def second_kernel(own, in_ref, out_ref):
    far = out_ref.shape[0]

    def total(rows):
        summed = in_ref[0, rows].astype(F32)
        for i in range(1, in_ref.shape[0]):
            summed = summed + in_ref[i, rows].astype(F32)
        return summed.astype(BF)

    def step(k, carry):
        out_ref[k, :own, :] = total(pl.ds(pl.multiple_of(k * own, own), own))
        return carry

    lax.fori_loop(0, far, step, 0)
    gates = total(slice(far * own, in_ref.shape[1]))
    for k in range(far):
        out_ref[k, own:, :] = gates


def four_factors(p_ref, t):
    return jnp.concatenate([p_ref[j ^ t] for j in range(p_ref.shape[0])], axis=0)


def third_kernel(norming, in_ref, p_ref, gradient_ref, out_ref, gate_ref):
    own = p_ref.shape[1]
    count = p_ref.shape[0]
    summed = in_ref[0].astype(F32)
    for k in range(1, in_ref.shape[0]):
        summed = summed + in_ref[k].astype(F32)
    summed = summed * norming
    gate_ref[...] = summed[own:]
    gradient = turn_by(summed[:own], -lax.axis_index(CLOSE))
    gradient_ref[...] = gradient
    factor = four_factors(p_ref, lax.axis_index(CLOSE))
    high, low = split_two(jnp.concatenate([turn(gradient, -j) for j in range(count)], axis=0))
    rank = dot(factor, high, FIRST) + dot(factor, low, FIRST)
    block = rank.shape[0] // count
    lane = lane_blocks((block, LANES))
    packed = rank[:block]
    for u in range(1, count):
        packed = jnp.where(lane == u, turn(rank[u * block : (u + 1) * block], u), packed)
    packed = packed.astype(BF)
    for k in range(out_ref.shape[0]):
        out_ref[k] = packed


def moment_kernel(mean_ref, square_ref, out_ref):
    own = out_ref.shape[1]
    lane = lane_blocks((own, LANES))
    count = out_ref.shape[0]
    for s in range(count):
        cut = pl.ds(pl.multiple_of(lax.rem(lax.axis_index("x") + s, count) * LANES, LANES), LANES)
        mean, square = mean_ref[:, cut], square_ref[:, cut]
        piece = None
        for k, rows in enumerate((mean[:own], mean[own:], square[:own], square[own:])):
            rows = turn_by(rows, k - lax.axis_index(CLOSE))
            piece = rows if k == 0 else jnp.where(lane == k, rows, piece)
        out_ref[s] = piece


def fourth_kernel(sizes, in_ref, moments_ref, p_ref, gradient_ref, gates_ref, out_ref):
    nx, nc = sizes
    count, own = p_ref.shape[:2]
    projected = in_ref[0].astype(F32)
    for k in range(1, in_ref.shape[0]):
        projected = projected + in_ref[k].astype(F32)
    block = projected.shape[0]
    lane = lane_blocks((own, LANES))
    moments = [moments_ref[0]] * 4
    for s in range(nx):
        u = lax.rem(lax.axis_index("x") + nx - s, nx)
        piece = moments_ref[s]
        moments = [jnp.where(lane == u, turn_by(piece, u - k), moments[k]) for k in range(4)]
    mean = jnp.concatenate(moments[:2], axis=0)
    square = jnp.concatenate(moments[2:], axis=0)
    mean = BETA_ONE * mean + (1.0 - BETA_ONE) * projected
    square = BETA_TWO * square + (1.0 - BETA_TWO) * projected * projected
    direction = mean / (jnp.sqrt(square) + EPSILON)
    sums = [
        jnp.sum(direction * direction, axis=0, keepdims=True),
        jnp.sum(projected * projected, axis=0, keepdims=True),
    ]
    sums = jnp.concatenate(sums, axis=0)
    one = sums.astype(BF).astype(F32)
    two = (sums - one).astype(BF).astype(F32)
    sums = jnp.concatenate([one, two, sums - one - two, jnp.zeros((2, LANES), F32)], axis=0).astype(BF)
    lane = lane_blocks((block, LANES))
    both = [jnp.where(lane == 0, turn(direction, -u), turn(projected, 1 - u)) for u in range(count)]
    high, low = split_two(jnp.concatenate(both, axis=0))
    factor = four_factors(p_ref, lax.axis_index(CLOSE))
    lifted = dot(factor, high) + dot(factor, low)
    lane = lane_blocks((own, LANES))
    gates = gates_ref[...].astype(BF)
    gradient = gradient_ref[...]
    for x in range(nx):
        tail = jnp.where(lane == 2, turn(projected[:own], 2 - x), turn(projected[own:], 3 - x))
        for j in range(count):
            piece = lifted[j * own : (j + 1) * own]
            piece = jnp.where(lane == 1, piece - turn(gradient, 1 - j), piece)
            low = piece - piece.astype(BF).astype(F32)
            low = jnp.where(lane[: own // 2] < 2, low[: own // 2], turn(low[own // 2 :], 2)).astype(BF)
            piece = jnp.where(lane < 2, piece, tail).astype(BF)
            for c in range(nc):
                k = (j * nx + x) * nc + c
                out_ref[k, :own] = piece
                out_ref[k, own : own + own // 2] = low
                out_ref[k, own + own // 2 : own + own // 2 + 8] = gates
                out_ref[k, own + own // 2 + 8 :] = sums


def last_kernel(
    sizes,
    in_ref,
    master_ref,
    mean_ref,
    square_ref,
    gate_mean_ref,
    gate_square_ref,
    update_ref,
    new_ref,
    copy_ref,
    mean_out,
    square_out,
    gate_update_ref,
    average_ref,
    energy_ref,
):
    count, nx, nc = sizes
    own = master_ref.shape[0]
    after = own + own // 2
    sums = in_ref[0, after + 8 :].astype(F32)
    for k in range(1, in_ref.shape[0]):
        sums = sums + in_ref[k, after + 8 :].astype(F32)
    sums = sums[0:2] + sums[2:4] + sums[4:6]
    direction_squares = jnp.sum(sums[0:1], axis=1, keepdims=True)
    projected_squares = jnp.sum(sums[1:2], axis=1, keepdims=True)
    balance = jnp.sqrt(direction_squares / (projected_squares + NORM_FLOOR))
    lane = lane_blocks((own, LANES))
    for x in range(nx):
        update, upper, lower = None, None, None
        for t in range(count):
            k = (t * nx + x) * nc + lax.axis_index("c")
            piece = in_ref[k, :own].astype(F32)
            low = in_ref[k, own:after].astype(F32)
            full = piece + jnp.concatenate([low, turn(low, -2)], axis=0)
            term = turn(full - balance * turn(full, -1), t)
            above, below = turn(piece, t - 2), turn(piece, t - 3)
            update = term if t == 0 else jnp.where(lane == t, term, update)
            upper = above if t == 0 else jnp.where(lane == t, above, upper)
            lower = below if t == 0 else jnp.where(lane == t, below, lower)
            g = in_ref[k, after : after + 8].astype(F32)
            place = slice((t * nx + x) * LANES, (t * nx + x + 1) * LANES)
            average = BETA_ONE * gate_mean_ref[:, place] + (1.0 - BETA_ONE) * g
            energy = BETA_TWO * gate_square_ref[:, place] + (1.0 - BETA_TWO) * g * g
            average_ref[:, place] = average
            energy_ref[:, place] = energy
            gate_update_ref[:, place] = average / (jnp.sqrt(energy) + EPSILON)
        cut = slice(x * LANES, (x + 1) * LANES)
        update_ref[:, cut] = update
        new = master_ref[:, cut] - STEP_RATE * update
        new_ref[:, cut] = new
        copy_ref[:, cut] = new.astype(BF)
        p = jnp.concatenate([upper, lower], axis=0)
        mean_out[:, cut] = BETA_ONE * mean_ref[:, cut] + (1.0 - BETA_ONE) * p
        square_out[:, cut] = BETA_TWO * square_ref[:, cut] + (1.0 - BETA_TWO) * p * p


def near_memory(value):
    return pltpu.with_memory_space_constraint(value, pltpu.VMEM)


def per_device(
    attention_input,
    query_cotangent,
    gate_cotangent,
    gate_totals,
    projector,
    query_master,
    lowrank_mean,
    lowrank_square,
    gating_mean,
    gating_square,
):
    nz, ny, nzl, nyl, nx, nc = (lax.axis_size(a) for a in ("zh", "yh", "zl", "yl", "x", "c"))
    far, near = nz * ny, nzl * nyl * nx
    count = nzl * nyl
    tokens, width = attention_input.shape
    columns = query_cotangent.shape[1]
    heads = gate_cotangent.shape[0]
    own, rank = projector.shape
    block = rank // nx
    norming = 1.0 / (tokens * far * near) ** 0.5
    shape = jax.ShapeDtypeStruct

    wide = nzl * ny * nyl * own
    first = pl.pallas_call(
        functools.partial(first_kernel, (nz, nzl, ny, nyl, nx, own)),
        out_shape=shape((near, far * own + heads, LANES), BF),
        in_specs=[ANY] * 4,
        out_specs=ANY,
        scratch_shapes=[
            pltpu.VMEM((nz, tokens, wide), BF),
            pltpu.VMEM((tokens, columns), BF),
            pltpu.VMEM((heads, tokens), F32),
            pltpu.VMEM((heads, tokens), F32),
            pltpu.VMEM((nz, near, ny * own, LANES), BF),
            pltpu.VMEM((near, heads, LANES), BF),
            pltpu.SemaphoreType.DMA((nz,)),
            pltpu.SemaphoreType.DMA,
            pltpu.SemaphoreType.DMA((2,)),
            pltpu.SemaphoreType.DMA((nz + 1,)),
        ],
        name="first",
    )(attention_input, query_cotangent, gate_cotangent, gate_totals)
    first = swap(first, NEAR)
    pieces = pl.pallas_call(
        moment_kernel,
        out_shape=shape((nx, own, LANES), F32),
        in_specs=[VMEM, VMEM],
        out_specs=VMEM,
        name="pieces",
    )(lowrank_mean, lowrank_square)
    moments = jnp.stack([pieces[0], *(shifted(pieces[s], "x", s) for s in range(1, nx))])
    neighbours = [lax.ppermute(projector, CLOSE, [(i, i ^ e) for i in range(count)]) for e in range(1, count)]
    factors = jnp.stack([projector, *neighbours])
    first, moments, factors = lax.optimization_barrier((first, moments, factors))

    second = pl.pallas_call(
        functools.partial(second_kernel, own),
        out_shape=pltpu.VMEM((far, own + heads, LANES), BF),
        in_specs=[VMEM],
        out_specs=VMEM,
        name="second",
    )(near_memory(first))
    second = swap(second, FAR)

    gradient, third, gates = pl.pallas_call(
        functools.partial(third_kernel, norming),
        out_shape=(
            pltpu.VMEM((own, LANES), F32),
            pltpu.VMEM((far, block, LANES), BF),
            pltpu.VMEM((heads, LANES), F32),
        ),
        in_specs=[VMEM, VMEM],
        out_specs=(VMEM, VMEM, VMEM),
        name="third",
    )(near_memory(second), near_memory(factors))
    third = swap(third, FAR)

    fourth = pl.pallas_call(
        functools.partial(fourth_kernel, (nx, nc)),
        out_shape=pltpu.VMEM((count * nx * nc, own + own // 2 + 16, LANES), BF),
        in_specs=[VMEM, VMEM, VMEM, VMEM, VMEM],
        out_specs=VMEM,
        name="fourth",
    )(
        near_memory(third),
        near_memory(moments),
        near_memory(factors),
        near_memory(gradient),
        near_memory(gates),
    )
    fourth = swap(fourth, LAST)

    return pl.pallas_call(
        functools.partial(last_kernel, (count, nx, nc)),
        out_shape=(
            shape((own, columns), F32),
            shape((own, columns), F32),
            shape((own, columns), BF),
            shape((block, columns), F32),
            shape((block, columns), F32),
            shape((heads, width), F32),
            shape((heads, width), F32),
            shape((heads, width), F32),
        ),
        in_specs=[VMEM] * 6,
        out_specs=(VMEM,) * 8,
        name="last",
    )(
        near_memory(fourth),
        near_memory(query_master),
        near_memory(lowrank_mean),
        near_memory(lowrank_square),
        near_memory(gating_mean),
        near_memory(gating_square),
    )


def solution(mesh):
    split = Mesh(
        mesh.devices.reshape(4, 2, 4, 2, mesh.shape["rep"], mesh.shape["tp"]),
        ("zh", "zl", "yh", "yl", "x", "c"),
    )
    in_specs = (
        P((*FS, "x"), None),
        P((*FS, "x"), "c"),
        P("c", (*FS, "x")),
        P("c", (*FS, "x")),
        P(FS, None),
        P(FS, "c"),
        P("x", "c"),
        P("x", "c"),
        P("c", None),
        P("c", None),
    )
    out_specs = (
        P(FS, "c"),
        P(FS, "c"),
        P(FS, "c"),
        P("x", "c"),
        P("x", "c"),
        P("c", None),
        P("c", None),
        P("c", None),
    )
    return jax.shard_map(
        per_device, mesh=split, in_specs=in_specs, out_specs=out_specs, check_vma=False
    )
```

```python
import functools

import jax
import jax.numpy as jnp
from jax import lax
from jax.experimental import pallas as pl
from jax.experimental.pallas import tpu as pltpu
from jax.sharding import Mesh
from jax.sharding import PartitionSpec as P

FS = ("zh", "zl", "yh", "yl")
NEAR = ("zl", "yl", "x")
FAR = ("zh", "yh")
CLOSE = ("zl", "yl")
LAST = ("zl", "yl", "x", "c")


BETA_ONE = 0.9
BETA_TWO = 0.95
STEP_RATE = 0.01
EPSILON = 1e-08
NORM_FLOOR = 1e-06
BF = jnp.bfloat16
F32 = jnp.float32
FIRST = (((0,), (0,)), ((), ()))
LANES = 128
PART = 32
VMEM = pl.BlockSpec(memory_space=pltpu.VMEM)
ANY = pl.BlockSpec(memory_space=pltpu.HBM)


def swap(pieces, axes):
    return lax.all_to_all(pieces, axes, 0, 0, tiled=True)


def shifted(value, axis, step):
    length = lax.axis_size(axis)
    return lax.ppermute(value, axis, [(i, (i + step) % length) for i in range(length)])


def split_two(v):
    high = v.astype(BF)
    return high, (v - high.astype(F32)).astype(BF)


def dot(a, b, dims=(((1,), (0,)), ((), ()))):
    return lax.dot_general(a, b, dims, preferred_element_type=F32)


def one_less_exp(v):
    series = 1.0 + v * 0.125
    for k in range(7, 1, -1):
        series = 1.0 + v * (1.0 / k) * series
    return jnp.where(v > -0.3, -v * series, 1.0 - jnp.exp(v))


def gate_signals(cot, totals):
    heads, tokens = cot.shape
    later = lax.broadcasted_iota(jnp.int32, (tokens, tokens), 0) >= lax.broadcasted_iota(
        jnp.int32, (tokens, tokens), 1
    )
    later = jnp.where(later, 1.0, 0.0).astype(BF)
    one = cot.astype(BF).astype(F32)
    rest = cot - one
    two = rest.astype(BF).astype(F32)
    parts = jnp.concatenate([one, two, rest - two, jnp.zeros_like(one)], axis=0).astype(BF)
    trailing = dot(parts, later)
    trailing = trailing[2 * heads : 3 * heads] + trailing[heads : 2 * heads] + trailing[:heads]
    lane = lax.broadcasted_iota(jnp.int32, totals.shape, 1)
    gate = totals - jnp.where(lane == 0, 0.0, pltpu.roll(totals, 1, 1))
    return (trailing * one_less_exp(gate)).astype(BF)


def lane_blocks(shape):
    return lax.broadcasted_iota(jnp.int32, shape, len(shape) - 1) // PART


def turn(value, blocks):
    blocks = blocks % (LANES // PART)
    return pltpu.roll(value, blocks * PART, 1) if blocks else value


def turn_by(value, blocks):
    count = LANES // PART
    return pltpu.roll(value, lax.rem(blocks + 2 * count, count) * PART, 1)


def first_kernel(
    sizes,
    x_ref,
    q_ref,
    cot_ref,
    tot_ref,
    out_ref,
    x_held,
    q_held,
    cot_held,
    tot_held,
    out_held,
    gate_held,
    x_sem,
    q_sem,
    small_sem,
    out_sem,
):
    nz, nzl, ny, nyl, nx, own = sizes
    wide = x_held.shape[2]
    heads = gate_held.shape[1]
    small = [
        pltpu.make_async_copy(cot_ref, cot_held, small_sem.at[0]),
        pltpu.make_async_copy(tot_ref, tot_held, small_sem.at[1]),
    ]
    q_copy = pltpu.make_async_copy(q_ref, q_held, q_sem)
    loads = [
        pltpu.make_async_copy(x_ref.at[:, z * wide : (z + 1) * wide], x_held.at[z], x_sem.at[z])
        for z in range(nz)
    ]
    for copy in (*small, q_copy, loads[0]):
        copy.start()
    for copy in small:
        copy.wait()
    for copy in loads[1:]:
        copy.start()
    signal = gate_signals(cot_held[...], tot_held[...])
    lane = lane_blocks((own, LANES))
    q_copy.wait()

    def send_of(z):
        rows = pl.ds(pl.multiple_of(z * ny * own, ny * own), ny * own)
        return pltpu.make_async_copy(out_held.at[z], out_ref.at[:, rows, :], out_sem.at[z])

    def step(z, carry):
        columns = pl.ds(pl.multiple_of(z * wide, wide), wide)
        pltpu.make_async_copy(x_ref.at[:, columns], x_held.at[z], x_sem.at[z]).wait()
        block = x_held[z]
        part = dot(block, q_held[...], FIRST)
        for yh in range(ny):
            to = slice(yh * own, (yh + 1) * own)
            for q in range(nx):
                turned = []
                for j in range(nzl * nyl):
                    row = ((j // nyl * ny + yh) * nyl + j % nyl) * own
                    turned.append(turn(part[row : row + own, q * LANES : (q + 1) * LANES], j))
                for t in range(nzl * nyl):
                    piece = turned[0]
                    for j in range(1, nzl * nyl):
                        piece = jnp.where(lane == (t + j) % (nzl * nyl), turned[j], piece)
                    out_held[z, t * nx + q, to, :] = piece.astype(BF)
        send_of(z).start()
        gates = dot(signal, block).astype(BF)
        for k in range(wide // LANES):
            gate_held[z * (wide // LANES) + k] = gates[:, k * LANES : (k + 1) * LANES]
        return carry

    lax.fori_loop(0, nz, step, 0, unroll=2)
    target = out_ref.at[:, nz * ny * own : nz * ny * own + heads, :]
    gate_send = pltpu.make_async_copy(gate_held, target, out_sem.at[nz])
    gate_send.start()
    for z in range(nz):
        send_of(z).wait()
    gate_send.wait()


def second_kernel(own, in_ref, out_ref):
    far = out_ref.shape[0]

    def total(rows):
        summed = in_ref[0, rows].astype(F32)
        for i in range(1, in_ref.shape[0]):
            summed = summed + in_ref[i, rows].astype(F32)
        return summed.astype(BF)

    def step(k, carry):
        out_ref[k, :own, :] = total(pl.ds(pl.multiple_of(k * own, own), own))
        return carry

    lax.fori_loop(0, far, step, 0)
    gates = total(slice(far * own, in_ref.shape[1]))
    for k in range(far):
        out_ref[k, own:, :] = gates


def four_factors(p_ref, t):
    return jnp.concatenate([p_ref[j ^ t] for j in range(p_ref.shape[0])], axis=0)


def third_kernel(norming, in_ref, p_ref, gradient_ref, out_ref, gate_ref):
    own = p_ref.shape[1]
    count = p_ref.shape[0]
    summed = in_ref[0].astype(F32)
    for k in range(1, in_ref.shape[0]):
        summed = summed + in_ref[k].astype(F32)
    summed = summed * norming
    gate_ref[...] = summed[own:]
    gradient = turn_by(summed[:own], -lax.axis_index(CLOSE))
    gradient_ref[...] = gradient
    factor = four_factors(p_ref, lax.axis_index(CLOSE))
    high, low = split_two(jnp.concatenate([turn(gradient, -j) for j in range(count)], axis=0))
    rank = dot(factor, high, FIRST) + dot(factor, low, FIRST)
    block = rank.shape[0] // count
    lane = lane_blocks((block, LANES))
    packed = rank[:block]
    for u in range(1, count):
        packed = jnp.where(lane == u, turn(rank[u * block : (u + 1) * block], u), packed)
    packed = packed.astype(BF)
    for k in range(out_ref.shape[0]):
        out_ref[k] = packed


def moment_kernel(mean_ref, square_ref, out_ref):
    own = out_ref.shape[1]
    lane = lane_blocks((own, LANES))
    count = out_ref.shape[0]
    for s in range(count):
        cut = pl.ds(pl.multiple_of(lax.rem(lax.axis_index("x") + s, count) * LANES, LANES), LANES)
        mean, square = mean_ref[:, cut], square_ref[:, cut]
        piece = None
        for k, rows in enumerate((mean[:own], mean[own:], square[:own], square[own:])):
            rows = turn_by(rows, k - lax.axis_index(CLOSE))
            piece = rows if k == 0 else jnp.where(lane == k, rows, piece)
        out_ref[s] = piece


def fourth_kernel(sizes, in_ref, moments_ref, p_ref, gradient_ref, gates_ref, out_ref):
    nx, nc = sizes
    count, own = p_ref.shape[:2]
    projected = in_ref[0].astype(F32)
    for k in range(1, in_ref.shape[0]):
        projected = projected + in_ref[k].astype(F32)
    block = projected.shape[0]
    lane = lane_blocks((own, LANES))
    moments = [moments_ref[0]] * 4
    for s in range(nx):
        u = lax.rem(lax.axis_index("x") + nx - s, nx)
        piece = moments_ref[s]
        moments = [jnp.where(lane == u, turn_by(piece, u - k), moments[k]) for k in range(4)]
    mean = jnp.concatenate(moments[:2], axis=0)
    square = jnp.concatenate(moments[2:], axis=0)
    mean = BETA_ONE * mean + (1.0 - BETA_ONE) * projected
    square = BETA_TWO * square + (1.0 - BETA_TWO) * projected * projected
    direction = mean / (jnp.sqrt(square) + EPSILON)
    sums = [
        jnp.sum(direction * direction, axis=0, keepdims=True),
        jnp.sum(projected * projected, axis=0, keepdims=True),
    ]
    sums = jnp.concatenate(sums, axis=0)
    one = sums.astype(BF).astype(F32)
    two = (sums - one).astype(BF).astype(F32)
    sums = jnp.concatenate([one, two, sums - one - two, jnp.zeros((2, LANES), F32)], axis=0).astype(BF)
    lane = lane_blocks((block, LANES))
    both = [jnp.where(lane == 0, turn(direction, -u), turn(projected, 1 - u)) for u in range(count)]
    high, low = split_two(jnp.concatenate(both, axis=0))
    factor = four_factors(p_ref, lax.axis_index(CLOSE))
    lifted = dot(factor, high) + dot(factor, low)
    lane = lane_blocks((own, LANES))
    gates = gates_ref[...].astype(BF)
    gradient = gradient_ref[...]
    for x in range(nx):
        tail = jnp.where(lane == 2, turn(projected[:own], 2 - x), turn(projected[own:], 3 - x))
        for j in range(count):
            piece = lifted[j * own : (j + 1) * own]
            piece = jnp.where(lane == 1, piece - turn(gradient, 1 - j), piece)
            low = piece - piece.astype(BF).astype(F32)
            low = jnp.where(lane[: own // 2] < 2, low[: own // 2], turn(low[own // 2 :], 2)).astype(BF)
            piece = jnp.where(lane < 2, piece, tail).astype(BF)
            for c in range(nc):
                k = (j * nx + x) * nc + c
                out_ref[k, :own] = piece
                out_ref[k, own : own + own // 2] = low
                out_ref[k, own + own // 2 : own + own // 2 + 8] = gates
                out_ref[k, own + own // 2 + 8 :] = sums


def last_kernel(
    sizes,
    in_ref,
    master_ref,
    mean_ref,
    square_ref,
    gate_mean_ref,
    gate_square_ref,
    update_ref,
    new_ref,
    copy_ref,
    mean_out,
    square_out,
    gate_update_ref,
    average_ref,
    energy_ref,
):
    count, nx, nc = sizes
    own = master_ref.shape[0]
    after = own + own // 2
    sums = in_ref[0, after + 8 :].astype(F32)
    for k in range(1, in_ref.shape[0]):
        sums = sums + in_ref[k, after + 8 :].astype(F32)
    sums = sums[0:2] + sums[2:4] + sums[4:6]
    direction_squares = jnp.sum(sums[0:1], axis=1, keepdims=True)
    projected_squares = jnp.sum(sums[1:2], axis=1, keepdims=True)
    balance = jnp.sqrt(direction_squares / (projected_squares + NORM_FLOOR))
    lane = lane_blocks((own, LANES))
    for x in range(nx):
        update, upper, lower = None, None, None
        for t in range(count):
            k = (t * nx + x) * nc + lax.axis_index("c")
            piece = in_ref[k, :own].astype(F32)
            low = in_ref[k, own:after].astype(F32)
            full = piece + jnp.concatenate([low, turn(low, -2)], axis=0)
            term = turn(full - balance * turn(full, -1), t)
            above, below = turn(piece, t - 2), turn(piece, t - 3)
            update = term if t == 0 else jnp.where(lane == t, term, update)
            upper = above if t == 0 else jnp.where(lane == t, above, upper)
            lower = below if t == 0 else jnp.where(lane == t, below, lower)
            g = in_ref[k, after : after + 8].astype(F32)
            place = slice((t * nx + x) * LANES, (t * nx + x + 1) * LANES)
            average = BETA_ONE * gate_mean_ref[:, place] + (1.0 - BETA_ONE) * g
            energy = BETA_TWO * gate_square_ref[:, place] + (1.0 - BETA_TWO) * g * g
            average_ref[:, place] = average
            energy_ref[:, place] = energy
            gate_update_ref[:, place] = average / (jnp.sqrt(energy) + EPSILON)
        cut = slice(x * LANES, (x + 1) * LANES)
        update_ref[:, cut] = update
        new = master_ref[:, cut] - STEP_RATE * update
        new_ref[:, cut] = new
        copy_ref[:, cut] = new.astype(BF)
        p = jnp.concatenate([upper, lower], axis=0)
        mean_out[:, cut] = BETA_ONE * mean_ref[:, cut] + (1.0 - BETA_ONE) * p
        square_out[:, cut] = BETA_TWO * square_ref[:, cut] + (1.0 - BETA_TWO) * p * p


def near_memory(value):
    return pltpu.with_memory_space_constraint(value, pltpu.VMEM)


def per_device(
    attention_input,
    query_cotangent,
    gate_cotangent,
    gate_totals,
    projector,
    query_master,
    lowrank_mean,
    lowrank_square,
    gating_mean,
    gating_square,
):
    nz, ny, nzl, nyl, nx, nc = (lax.axis_size(a) for a in ("zh", "yh", "zl", "yl", "x", "c"))
    far, near = nz * ny, nzl * nyl * nx
    count = nzl * nyl
    tokens, width = attention_input.shape
    columns = query_cotangent.shape[1]
    heads = gate_cotangent.shape[0]
    own, rank = projector.shape
    block = rank // nx
    norming = 1.0 / (tokens * far * near) ** 0.5
    shape = jax.ShapeDtypeStruct

    wide = nzl * ny * nyl * own
    first = pl.pallas_call(
        functools.partial(first_kernel, (nz, nzl, ny, nyl, nx, own)),
        out_shape=shape((near, far * own + heads, LANES), BF),
        in_specs=[ANY] * 4,
        out_specs=ANY,
        scratch_shapes=[
            pltpu.VMEM((nz, tokens, wide), BF),
            pltpu.VMEM((tokens, columns), BF),
            pltpu.VMEM((heads, tokens), F32),
            pltpu.VMEM((heads, tokens), F32),
            pltpu.VMEM((nz, near, ny * own, LANES), BF),
            pltpu.VMEM((near, heads, LANES), BF),
            pltpu.SemaphoreType.DMA((nz,)),
            pltpu.SemaphoreType.DMA,
            pltpu.SemaphoreType.DMA((2,)),
            pltpu.SemaphoreType.DMA((nz + 1,)),
        ],
        name="first",
    )(attention_input, query_cotangent, gate_cotangent, gate_totals)
    first = swap(first, NEAR)
    pieces = pl.pallas_call(
        moment_kernel,
        out_shape=shape((nx, own, LANES), F32),
        in_specs=[VMEM, VMEM],
        out_specs=VMEM,
        name="pieces",
    )(lowrank_mean, lowrank_square)
    moments = jnp.stack([pieces[0], *(shifted(pieces[s], "x", s) for s in range(1, nx))])
    neighbours = [lax.ppermute(projector, CLOSE, [(i, i ^ e) for i in range(count)]) for e in range(1, count)]
    factors = jnp.stack([projector, *neighbours])
    first, moments, factors = lax.optimization_barrier((first, moments, factors))

    second = pl.pallas_call(
        functools.partial(second_kernel, own),
        out_shape=pltpu.VMEM((far, own + heads, LANES), BF),
        in_specs=[VMEM],
        out_specs=VMEM,
        name="second",
    )(near_memory(first))
    second = swap(second, FAR)

    gradient, third, gates = pl.pallas_call(
        functools.partial(third_kernel, norming),
        out_shape=(
            pltpu.VMEM((own, LANES), F32),
            pltpu.VMEM((far, block, LANES), BF),
            pltpu.VMEM((heads, LANES), F32),
        ),
        in_specs=[VMEM, VMEM],
        out_specs=(VMEM, VMEM, VMEM),
        name="third",
    )(near_memory(second), near_memory(factors))
    third = swap(third, FAR)

    fourth = pl.pallas_call(
        functools.partial(fourth_kernel, (nx, nc)),
        out_shape=pltpu.VMEM((count * nx * nc, own + own // 2 + 16, LANES), BF),
        in_specs=[VMEM, VMEM, VMEM, VMEM, VMEM],
        out_specs=VMEM,
        name="fourth",
    )(
        near_memory(third),
        near_memory(moments),
        near_memory(factors),
        near_memory(gradient),
        near_memory(gates),
    )
    fourth = swap(fourth, LAST)

    return pl.pallas_call(
        functools.partial(last_kernel, (count, nx, nc)),
        out_shape=(
            shape((own, columns), F32),
            shape((own, columns), F32),
            shape((own, columns), BF),
            shape((block, columns), F32),
            shape((block, columns), F32),
            shape((heads, width), F32),
            shape((heads, width), F32),
            shape((heads, width), F32),
        ),
        in_specs=[VMEM] * 6,
        out_specs=(VMEM,) * 8,
        name="last",
    )(
        near_memory(fourth),
        near_memory(query_master),
        near_memory(lowrank_mean),
        near_memory(lowrank_square),
        near_memory(gating_mean),
        near_memory(gating_square),
    )


def solution(mesh):
    split = Mesh(
        mesh.devices.reshape(4, 2, 4, 2, mesh.shape["rep"], mesh.shape["tp"]),
        ("zh", "zl", "yh", "yl", "x", "c"),
    )
    in_specs = (
        P((*FS, "x"), None),
        P((*FS, "x"), "c"),
        P("c", (*FS, "x")),
        P("c", (*FS, "x")),
        P(FS, None),
        P(FS, "c"),
        P("x", "c"),
        P("x", "c"),
        P("c", None),
        P("c", None),
    )
    out_specs = (
        P(FS, "c"),
        P(FS, "c"),
        P(FS, "c"),
        P("x", "c"),
        P("x", "c"),
        P("c", None),
        P("c", None),
        P("c", None),
    )
    return jax.shard_map(
        per_device, mesh=split, in_specs=in_specs, out_specs=out_specs, check_vma=False
    )
```
